32 devices in a mesh: sp: 8 (over z, y), tp: 4 (over x, core).
Axes of the slice: x: 2, y: 2, z: 4, core: 2. Of those that a mesh axis runs over, the one named last changes fastest.
Arguments:
- tokens_in: bfloat16 [2048, 2048], P('sp'), may hold values from -3 to 3
- queries: bfloat16 [2048, 1024], P('sp', 'tp'), may hold values from -6 to 6
- keys: bfloat16 [2048, 256], P('sp', 'tp'), may hold values from -6 to 6
- values: bfloat16 [2048, 256], P('sp', 'tp'), may hold values from -12 to 12
- doc_ids: int32 [2048], P('sp'), may hold values from 0 to 1, never falling along the last dimension, each value on 1 to 1280 neighbouring positions
- query_gain: float32 [64], replicated, may hold values from 2.5 to 6
- key_norm_scale: float32 [64], replicated, may hold values from 2.5 to 6
- out_weight: bfloat16 [1024, 2048], P('tp'), may hold values from -0.1875 to 0.1875
- norm_gain: float32 [2048], replicated, may hold values from 0.1 to 1.9
- gate_weight: bfloat16 [2048, 5632], P('sp', 'tp'), may hold values from -0.125 to 0.125
- up_weight: bfloat16 [2048, 5632], P('sp', 'tp'), may hold values from -0.125 to 0.125
- down_weight: bfloat16 [5632, 2048], P('tp', 'sp'), may hold values from -0.078125 to 0.078125
Outputs:
- layer_out: bfloat16 [2048, 2048], P('sp')
The draws below stay inside these ranges and needn't reach their ends.
Inputs may be any that keep to these rules, and one draw needn't show every extreme that they name: `doc_ids`: document numbers never fall along the sequence; every document has 1 to 1280 positions and one has exactly 1280.
All inputs are finite; a program needn't handle non-finite values.
Results may differ from the reference program's by a relative error of at most 0.014.
The reference program's roundings to bfloat16 on the way (of `weights`, `attended`, `normed` and `hidden`) count: a program that leaves them out, or rounds other values in their place, can miss the bound.
Values may be sent and summed in bfloat16 or wider, within the bound.
A program may use at most 128 MiB of HBM per device.

```python
import math
import jax
import jax.numpy as jnp
import numpy as np
from jax import lax

D = 2048
QUERY_HEADS = 16
KEY_VALUE_HEADS = 4
HEAD_SIZE = 64
FF = 5632
GRID = 64
PACKED_TOKENS = 2048
DOCS = 2
DOC_MOST = 1280
N_TP = 4


def repeated_keys(key):
    sampled_values = jax.random.normal(jax.random.fold_in(key, 11), (PACKED_TOKENS, KEY_VALUE_HEADS * HEAD_SIZE), jnp.float32)
    return jnp.clip(sampled_values, -6.0, 6.0)


def draw_keys(key, part):
    return repeated_keys(key).astype(jnp.bfloat16)


def draw_queries(key, part):
    fresh = jnp.clip(jax.random.normal(jax.random.fold_in(key, 12), (PACKED_TOKENS, QUERY_HEADS * HEAD_SIZE), jnp.float32), -6.0, 6.0)
    return fresh.astype(jnp.bfloat16)


def draw_query_gain(key, part):
    spread = jax.random.uniform(jax.random.fold_in(key, 21), (HEAD_SIZE,), jnp.float32)
    return 2.5 + spread


def draw_key_norm_scale(key, part):
    spread = jax.random.uniform(jax.random.fold_in(key, 22), (HEAD_SIZE,), jnp.float32)
    return 2.5 + spread


def shard_levels(own_key, extent, shards, least, largest):
    def one(dim, parts):
        heights = jax.random.uniform(jax.random.fold_in(jax.random.fold_in(own_key, 6), dim), (parts,), jnp.float32, least / len(shards), largest / len(shards))
        return jnp.repeat(jnp.exp(heights), extent[dim] // parts).reshape((-1,) + (1,) * (len(extent) - dim - 1))

    level = one(*shards[0])
    for cut in shards[1:]:
        level = level * one(*cut)
    return level


def split_up(amount, total, bound, skew):
    loads = [(1 << 20) // math.isqrt(rank ** skew) + 1 for rank in range(2, amount + 1)]
    surplus, counts = total - bound - (amount - 1), [1] * (amount - 1)
    while surplus > 0:
        movable = [i for i in range(amount - 1) if counts[i] < bound]
        mass, remaining = sum([loads[i] for i in movable]), surplus
        for i in movable:
            more = min(bound - counts[i], max(1, remaining * loads[i] // mass), surplus)
            counts[i] = counts[i] + more
            surplus = surplus - more
    return np.array([bound] + counts)


def ragged_sizes(stream_key, amount, total, limit, lean):
    if amount == 2:
        one = jax.random.randint(stream_key, (), max(1, total - limit), min(limit, total - 1) + 1)
        return jnp.stack([one, total - one])
    lengths = jnp.asarray(split_up(amount, total, limit, lean), jnp.int32)
    couples = (amount - 1) // 2
    giver, receiver = lengths[1:1 + 2 * couples:2], lengths[2:2 + 2 * couples:2]
    margin = jnp.minimum(giver - 1, limit - receiver)
    moved = jax.random.randint(jax.random.fold_in(stream_key, 1), (couples,), 0, 1 << 20) % (margin + 1)
    lengths = lengths.at[1:1 + 2 * couples:2].set(giver - moved).at[2:2 + 2 * couples:2].set(receiver + moved)
    return lengths[jax.random.permutation(jax.random.fold_in(stream_key, 2), amount)]


def scatter_about(own_key, dims, width, bound, shards=(), kind=jnp.bfloat16):
    level = shard_levels(own_key, dims, shards, -0.22, 0.18) if shards else 1.0
    drawn = jax.random.normal(own_key, dims, jnp.float32) * width * level
    return jnp.minimum(jnp.maximum(drawn, -bound), bound).astype(kind)


def setup_inputs(seed: int = 0) -> dict:
    key_list = jax.random.split(jax.random.key(seed), 13)
    return {
        "tokens_in": scatter_about(key_list[0], (PACKED_TOKENS, D), 0.5, 3.0, ((0, 8),)),
        "queries": draw_queries(jax.random.fold_in(key_list[12], 71), 0),
        "keys": draw_keys(jax.random.fold_in(key_list[12], 71), 0),
        "values": scatter_about(key_list[3], (PACKED_TOKENS, KEY_VALUE_HEADS * HEAD_SIZE), 2.0, 12.0, ((0, 8), (1, 4))),
        "doc_ids": jnp.searchsorted(jnp.cumsum(ragged_sizes(key_list[4], DOCS, PACKED_TOKENS, DOC_MOST, 1)), jnp.arange(PACKED_TOKENS), side="right").astype(jnp.int32),
        "query_gain": draw_query_gain(jax.random.fold_in(key_list[12], 71), 0),
        "key_norm_scale": draw_key_norm_scale(jax.random.fold_in(key_list[12], 71), 0),
        "out_weight": scatter_about(key_list[7], (QUERY_HEADS * HEAD_SIZE, D), (QUERY_HEADS * HEAD_SIZE) ** -0.5, 0.1875, ((0, 4),)),
        "norm_gain": jnp.clip(1.0 + 0.18 * jax.random.normal(key_list[8], (D,), jnp.float32), 0.1, 1.9),
        "gate_weight": scatter_about(key_list[9], (D, FF), D ** -0.5, 0.125, ((0, 8), (1, 4))),
        "up_weight": scatter_about(key_list[10], (D, FF), D ** -0.5, 0.125, ((0, 8), (1, 4))),
        "down_weight": scatter_about(key_list[11], (FF, D), FF ** -0.5, 0.078125, ((0, 4), (1, 8))),
    }


EPS = 1e-06
THETA = 10000.0
NEG = -1e+30

def rotate_half(block, angle):
    half_dim = block.shape[-1] // 2
    cosine = jnp.cos(angle)[:, None, :]
    sine = jnp.sin(angle)[:, None, :]
    first = block[..., :half_dim]
    second = block[..., half_dim:]
    return jnp.concatenate([first * cosine - second * sine, second * cosine + first * sine], axis=-1)

def normalized_rotated(values_in, gain, heads, lattice_row, lattice_column):
    full = values_in.astype(jnp.float32).reshape(values_in.shape[0], heads, -1)
    full = full * lax.rsqrt(lax.optimization_barrier(jnp.mean(full * full, axis=-1, keepdims=True)) + EPS) * gain
    half_dim = full.shape[-1] // 2
    freqs = THETA ** (-2.0 * jnp.arange(half_dim // 2, dtype=jnp.float32) / half_dim)
    by_row = rotate_half(full[..., :half_dim], lattice_row[:, None] * freqs[None, :])
    by_col = rotate_half(full[..., half_dim:], lattice_column[:, None] * freqs[None, :])
    return jnp.concatenate([by_row, by_col], axis=-1).astype(jnp.bfloat16)

def reference(tokens_in, queries, keys, values, doc_ids, query_gain, key_norm_scale, out_weight, norm_gain, gate_weight, up_weight, down_weight):
    places = jnp.arange(PACKED_TOKENS, dtype=jnp.int32)
    lattice_row = (places // GRID).astype(jnp.float32)
    lattice_column = (places % GRID).astype(jnp.float32)
    q_all = normalized_rotated(queries, query_gain, QUERY_HEADS, lattice_row, lattice_column)
    every_key = normalized_rotated(keys, key_norm_scale, KEY_VALUE_HEADS, lattice_row, lattice_column).astype(jnp.float32)
    every_value = values.reshape(PACKED_TOKENS, KEY_VALUE_HEADS, HEAD_SIZE).astype(jnp.float32)
    query_group = QUERY_HEADS // KEY_VALUE_HEADS
    scale = HEAD_SIZE ** (-0.5)
    rows_per_block = 128

    def attend(start):
        query_tile = lax.dynamic_slice_in_dim(q_all, start, rows_per_block, 0).astype(jnp.float32)
        query_tile = query_tile.reshape(rows_per_block, KEY_VALUE_HEADS, query_group, HEAD_SIZE)
        doc_block = lax.dynamic_slice_in_dim(doc_ids, start, rows_per_block, 0)
        scores = jnp.einsum('qhgd,khd->hgqk', query_tile, every_key) * scale
        same = (doc_block[:, None] == doc_ids[None, :])[None, None]
        scores = jnp.where(same, scores, NEG)
        top = lax.optimization_barrier(jnp.max(scores, axis=-1, keepdims=True))
        weights = jnp.where(same, jnp.exp(scores - top), 0.0)
        total = lax.optimization_barrier(jnp.sum(weights, axis=-1))
        rounded = lax.optimization_barrier(weights.astype(jnp.bfloat16)).astype(jnp.float32)
        blended = jnp.einsum('hgqk,khd->hgqd', rounded, every_value) / total[..., None]
        return blended.transpose(2, 0, 1, 3).reshape(rows_per_block, QUERY_HEADS * HEAD_SIZE).astype(jnp.bfloat16)
    starts = jnp.arange(PACKED_TOKENS // rows_per_block, dtype=jnp.int32) * rows_per_block
    attended = lax.map(attend, starts).reshape(PACKED_TOKENS, QUERY_HEADS * HEAD_SIZE)
    share_cols = QUERY_HEADS * HEAD_SIZE // N_TP
    mixed = jnp.zeros((PACKED_TOKENS, D), jnp.float32)
    for member in range(N_TP):
        part_out = jnp.dot(attended[:, member * share_cols:(member + 1) * share_cols], out_weight[member * share_cols:(member + 1) * share_cols], preferred_element_type=jnp.float32)
        mixed = mixed + part_out.astype(jnp.bfloat16).astype(jnp.float32)
    resid = tokens_in.astype(jnp.float32) + mixed
    normed = (resid * lax.rsqrt(lax.optimization_barrier(jnp.mean(resid * resid, axis=-1, keepdims=True)) + EPS) * norm_gain).astype(jnp.bfloat16)
    gate = jnp.dot(normed, gate_weight, preferred_element_type=jnp.float32)
    up_val = jnp.dot(normed, up_weight, preferred_element_type=jnp.float32)
    hidden = (jax.nn.silu(gate) * up_val).astype(jnp.bfloat16)
    unit_cols = FF // N_TP
    fed = jnp.zeros((PACKED_TOKENS, D), jnp.float32)
    for member in range(N_TP):
        part_out = jnp.dot(hidden[:, member * unit_cols:(member + 1) * unit_cols], down_weight[member * unit_cols:(member + 1) * unit_cols], preferred_element_type=jnp.float32)
        fed = fed + part_out.astype(jnp.bfloat16).astype(jnp.float32)
    return (resid + fed).astype(jnp.bfloat16)
```

```python
import functools

import jax
import jax.numpy as jnp
from jax import lax
from jax.experimental import pallas as pl
from jax.experimental.pallas import tpu as pltpu
from jax.sharding import PartitionSpec as P

GRID = 64


EPS = 1e-06
THETA = 10000.0
NEG = -1e30


def rotate_half(block, angle):
    half_dim = block.shape[-1] // 2
    cosine = jnp.cos(angle)[:, None, :]
    sine = jnp.sin(angle)[:, None, :]
    first = block[..., :half_dim]
    second = block[..., half_dim:]
    return jnp.concatenate(
        [first * cosine - second * sine, second * cosine + first * sine], axis=-1
    )


def normalized_rotated(values_in, gain, heads, lattice_row, lattice_column):
    full = values_in.astype(jnp.float32).reshape(values_in.shape[0], heads, -1)
    full = full * lax.rsqrt(jnp.mean(full * full, axis=-1, keepdims=True) + EPS) * gain
    half_dim = full.shape[-1] // 2
    freqs = THETA ** (-2.0 * jnp.arange(half_dim // 2, dtype=jnp.float32) / half_dim)
    by_row = rotate_half(full[..., :half_dim], lattice_row[:, None] * freqs[None, :])
    by_col = rotate_half(full[..., half_dim:], lattice_column[:, None] * freqs[None, :])
    return jnp.concatenate([by_row, by_col], axis=-1).astype(jnp.bfloat16)


MESH = pl.DeviceIdType.MESH
VM = pl.BlockSpec(memory_space=pltpu.VMEM)


def params(cid):
    return pltpu.CompilerParams(
        collective_id=cid, has_side_effects=True, vmem_limit_bytes=56 * 1024 * 1024
    )


def greet(count, where):
    barrier = pltpu.get_barrier_semaphore()

    @pl.loop(1, count)
    def _(step):
        pl.semaphore_signal(barrier, inc=1, device_id=where(step), device_id_type=MESH)

    pl.semaphore_wait(barrier, count - 1)


def gather_kernel(n, kv_ref, doc_ref, kv_out, doc_out, send, recv, doc_send, doc_recv):
    me = lax.axis_index("sp")

    def where(step):
        return {"sp": lax.rem(me + step, n)}

    def copies(step, slot):
        return (
            pltpu.make_async_remote_copy(
                kv_ref, kv_out.at[slot], send.at[step], recv.at[step], where(step), MESH
            ),
            pltpu.make_async_remote_copy(
                doc_ref, doc_out.at[slot], doc_send.at[step], doc_recv.at[step], where(step), MESH
            ),
        )

    greet(n, where)

    @pl.loop(1, n)
    def _(step):
        for copy in copies(step, me):
            copy.start()

    kv_out[me] = kv_ref[...]
    doc_out[me] = doc_ref[...]

    @pl.loop(1, n)
    def _(step):
        for copy in copies(step, lax.rem(me + n - step, n)):
            copy.wait_recv()
            copy.wait_send()


def gather_sp(n, packed, docs):
    return pl.pallas_call(
        functools.partial(gather_kernel, n),
        out_shape=(
            jax.ShapeDtypeStruct((n,) + packed.shape, packed.dtype),
            jax.ShapeDtypeStruct((n,) + docs.shape, docs.dtype),
        ),
        in_specs=[VM, VM],
        out_specs=(VM, VM),
        scratch_shapes=[pltpu.SemaphoreType.DMA((n,))] * 4,
        compiler_params=params(0),
        name="gather_sp",
    )(packed, docs)


def mid_kernel(
    nt, partial_ref, tokens_ref, gain_ref, normed_out, resid_out, landing, send, recv, send2, recv2
):
    sp, tp = lax.axis_index("sp"), lax.axis_index("tp")
    side = lax.rem(sp, 2)
    base = sp - side
    group = 2 * nt
    me = side * nt + tp
    rows = resid_out.shape[0]

    def where(step):
        other = lax.rem(me + step, group)
        return {"sp": base + other // nt, "tp": lax.rem(other, nt)}

    def part(step):
        peer = lax.rem(tp + step, nt)
        return pltpu.make_async_remote_copy(
            partial_ref.at[peer],
            landing.at[step],
            send.at[step],
            recv.at[step],
            {"sp": sp, "tp": peer},
            MESH,
        )

    def spread(step, slot):
        return pltpu.make_async_remote_copy(
            normed_out.at[slot], normed_out.at[slot], send2.at[step], recv2.at[step], where(step), MESH
        )

    greet(group, where)
    for step in range(1, nt):
        part(step).start()
    for step in range(1, nt):
        part(step).wait_recv()
    chunk = 16

    @pl.loop(0, rows // chunk)
    def _(i):
        at = pl.ds(pl.multiple_of(i * chunk, chunk), chunk)
        mixed = partial_ref[tp, at].astype(jnp.float32)
        for step in range(1, nt):
            mixed = mixed + landing[step, at].astype(jnp.float32)
        resid = tokens_ref[tp, at].astype(jnp.float32) + mixed
        resid_out[at] = resid
        power = jnp.mean(resid * resid, axis=-1, keepdims=True)
        normed_out[me, at] = (resid * lax.rsqrt(power + EPS) * gain_ref[...]).astype(jnp.bfloat16)

    for step in range(1, group):
        spread(step, me).start()
    for step in range(1, group):
        copy = spread(step, lax.rem(me + group - step, group))
        copy.wait_recv()
        copy.wait_send()
    for step in range(1, nt):
        part(step).wait_send()


def mid_stage(nt, part, tokens, gain):
    rows, width = part.shape[0] // nt, part.shape[1]
    return pl.pallas_call(
        functools.partial(mid_kernel, nt),
        out_shape=(
            jax.ShapeDtypeStruct((2 * nt, rows, width), jnp.bfloat16),
            jax.ShapeDtypeStruct((rows, width), jnp.float32),
        ),
        in_specs=[VM, VM, VM],
        out_specs=(VM, VM),
        scratch_shapes=[pltpu.VMEM((nt, rows, width), jnp.bfloat16)]
        + [pltpu.SemaphoreType.DMA((nt,))] * 2
        + [pltpu.SemaphoreType.DMA((2 * nt,))] * 2,
        compiler_params=params(1),
        name="mid_stage",
    )(part.reshape(nt, rows, width), tokens.reshape(nt, rows, width), gain.reshape(1, width))


def last_kernel(nt, fed_ref, resid_ref, out_ref, landing, send, recv, send2, recv2):
    sp, tp = lax.axis_index("sp"), lax.axis_index("tp")
    side = lax.rem(sp, 2)
    base = sp - side
    group = 2 * nt
    me = side * nt + tp
    rows = resid_ref.shape[0]

    def where(step):
        other = lax.rem(me + step, group)
        return {"sp": base + other // nt, "tp": lax.rem(other, nt)}

    def part(step):
        return pltpu.make_async_remote_copy(
            fed_ref.at[lax.rem(me + step, group)],
            landing.at[step],
            send.at[step],
            recv.at[step],
            where(step),
            MESH,
        )

    def spread(step, slot):
        return pltpu.make_async_remote_copy(
            out_ref.at[slot],
            out_ref.at[slot],
            send2.at[step],
            recv2.at[step],
            {"sp": sp, "tp": lax.rem(tp + step, nt)},
            MESH,
        )

    greet(group, where)
    for step in range(1, group):
        part(step).start()
    for step in range(1, group):
        part(step).wait_recv()
    chunk = 16

    @pl.loop(0, rows // chunk)
    def _(i):
        at = pl.ds(pl.multiple_of(i * chunk, chunk), chunk)
        fed = fed_ref[me, at].astype(jnp.float32)
        for step in range(1, group):
            fed = fed + landing[step, at].astype(jnp.float32)
        out_ref[tp, at] = (resid_ref[at] + fed).astype(jnp.bfloat16)

    for step in range(1, nt):
        spread(step, tp).start()
    for step in range(1, nt):
        copy = spread(step, lax.rem(tp + nt - step, nt))
        copy.wait_recv()
        copy.wait_send()
    for step in range(1, group):
        part(step).wait_send()


def last_stage(nt, fed, resid):
    rows, width = resid.shape
    return pl.pallas_call(
        functools.partial(last_kernel, nt),
        out_shape=jax.ShapeDtypeStruct((nt, rows, width), jnp.bfloat16),
        in_specs=[VM, VM],
        out_specs=VM,
        scratch_shapes=[pltpu.VMEM((2 * nt, rows, width), jnp.bfloat16)]
        + [pltpu.SemaphoreType.DMA((2 * nt,))] * 2
        + [pltpu.SemaphoreType.DMA((nt,))] * 2,
        compiler_params=params(2),
        name="last_stage",
    )(fed.reshape(2 * nt, rows, width), resid)


def pair_share(n, arrays, axis, joins):
    side = lax.rem(lax.axis_index("sp"), 2)
    own, away = [], []
    for array in arrays:
        half = array.shape[axis] // 2
        own.append(lax.dynamic_slice_in_dim(array, side * half, half, axis))
        away.append(lax.dynamic_slice_in_dim(array, (1 - side) * half, half, axis))
    own = jnp.concatenate(own, axis=axis)
    away = jnp.concatenate(away, axis=axis)
    came = lax.ppermute(away, "sp", [(i, i ^ 1) for i in range(n)])
    first = jnp.where(side == 0, own, came)
    second = jnp.where(side == 0, came, own)
    return jnp.concatenate([first, second], axis=joins)


SIDES = 2
LANE = 128


def turned(block, gain, table):
    power = jnp.mean(block * block, axis=0, keepdims=True)
    full = block * lax.rsqrt(power + EPS) * gain
    half = block.shape[0] // 2
    quarter = half // 2
    pieces = []
    for part in range(2):
        first = full[part * half : part * half + quarter]
        second = full[part * half + quarter : (part + 1) * half]
        cosine = table[2 * part * quarter : (2 * part + 1) * quarter]
        sine = table[(2 * part + 1) * quarter : (2 * part + 2) * quarter]
        pieces += [first * cosine - second * sine, second * cosine + first * sine]
    return jnp.concatenate(pieces, axis=0)


def fused_kernel(
    n,
    nt,
    wide,
    q_in,
    k_in,
    v_in,
    doc_in,
    table_in,
    q_gain,
    k_gain,
    norm_gain,
    tokens,
    out_weight,
    gate,
    up,
    down,
    out,
    kv,
    q_ref,
    top,
    total,
    acc,
    att_out,
    att,
    ow,
    tok,
    resid,
    act,
    gw,
    uw,
    dw,
    hid,
    keep,
    core_out,
    core_in,
    x_keep,
    x_out,
    x_in,
    z_keep,
    z_out,
    z_in,
    kv_zs,
    kv_ys,
    kv_r,
    w_own,
    w_zs,
    w_ys,
    w_r,
    misc,
    ow_xs,
    ow_cs,
    ow_r,
    att_s,
    att_r,
    act_us,
    act_ds,
    act_xs,
    act_cs,
    act_r,
    rs_cs,
    rs_cr,
    rs_xs,
    rs_xr,
    rs_zs,
    rs_zr,
    ag_xs,
    ag_cs,
    ag_r,
):
    sp, tp = lax.axis_index("sp"), lax.axis_index("tp")
    lanes, xs = n // SIDES, nt // 2
    lane, side = sp // SIDES, sp % SIDES
    xi, core = tp // 2, tp % 2
    rows = q_in.shape[1]
    head_dim = k_in.shape[0]
    heads = q_in.shape[0] // head_dim
    chunk = rows // nt
    blocks = gate.shape[1] // LANE
    width = wide * LANE
    cut = lanes * wide - blocks
    kv_docs = head_dim
    kv_vals = kv.shape[1] - head_dim

    def at_sp(lane_to, side_to):
        return {"sp": lane_to * SIDES + side_to, "tp": tp}

    def at_tp(x_to, core_to):
        return {"sp": sp, "tp": x_to * 2 + core_to}

    def remote(src, dst, send, recv, where):
        return pltpu.make_async_remote_copy(src, dst, send, recv, where, MESH)

    def lane_at(d):
        return (lane + d) % lanes

    def x_at(d):
        return (xi + d) % xs

    other_side = 1 - side
    other_core = 1 - core

    barrier = pltpu.get_barrier_semaphore()
    for d in range(1, lanes):
        pl.semaphore_signal(barrier, inc=1, device_id=at_sp(lane_at(d), side), device_id_type=MESH)
    pl.semaphore_signal(barrier, inc=1, device_id=at_sp(lane, other_side), device_id_type=MESH)
    for d in range(1, nt):
        pl.semaphore_signal(
            barrier, inc=1, device_id={"sp": sp, "tp": (tp + d) % nt}, device_id_type=MESH
        )

    def unit_from(lane_to):
        return pl.multiple_of((lane_to * wide - (lane_to // (lanes - 1)) * cut) * LANE, LANE)

    def weight_block(m, lane_to):
        at = pl.ds(unit_from(lane_to), width)
        if m == 0:
            return gate.at[:, at]
        if m == 1:
            return up.at[:, at]
        return down.at[at, :]

    landed = (gw, uw, dw)

    own_copies = [
        pltpu.make_async_copy(weight_block(m, lane), landed[m].at[sp], w_own.at[m]) for m in range(3)
    ]
    own_copies.append(pltpu.make_async_copy(out_weight, ow.at[tp], misc.at[0]))
    own_copies.append(
        pltpu.make_async_copy(tokens.at[pl.ds(pl.multiple_of(tp * chunk, chunk), chunk)], tok, misc.at[1])
    )
    for copy in own_copies:
        copy.start()

    kv[sp, 0:head_dim, :] = turned(k_in[...].astype(jnp.float32), k_gain[...], table_in[...]).astype(
        jnp.bfloat16
    )
    kv[sp, kv_docs:kv_vals, :] = doc_in[...]
    kv[sp, kv_vals:, :] = v_in[...]

    pl.semaphore_wait(barrier, lanes - 1 + 1 + nt - 1)

    def kv_z(d, slot):
        return remote(kv.at[slot], kv.at[slot], kv_zs.at[d], kv_r.at[slot], at_sp(lane_at(d), side))

    def kv_y(lane_of, side_of):
        slot = lane_of * SIDES + side_of
        return remote(
            kv.at[slot], kv.at[slot], kv_ys.at[lane_of], kv_r.at[slot], at_sp(lane, other_side)
        )

    for d in range(1, lanes):
        kv_z(d, sp).start()
    kv_y(lane, side).start()

    def ow_x(d):
        return remote(out_weight, ow.at[tp], ow_xs.at[d], ow_r.at[tp], at_tp(x_at(d), core))

    def ow_core(x_of, core_of):
        slot = x_of * 2 + core_of
        return remote(ow.at[slot], ow.at[slot], ow_cs.at[x_of], ow_r.at[slot], at_tp(xi, other_core))

    for d in range(1, xs):
        ow_x(d).start()
    own_copies[3].wait()
    ow_core(xi, core).start()

    scale = head_dim ** (-0.5)
    for h in range(heads):
        at = slice(h * head_dim, (h + 1) * head_dim)
        query = turned(q_in[at, :].astype(jnp.float32), q_gain[...], table_in[...])
        q_ref[at, :] = (query.astype(jnp.bfloat16).astype(jnp.float32) * scale).astype(jnp.bfloat16)
    top[...] = jnp.full(top.shape, NEG, jnp.float32)
    total[...] = jnp.zeros(total.shape, jnp.float32)
    acc[...] = jnp.zeros(acc.shape, jnp.float32)

    for d in range(1, lanes):
        slot = lane_at(-d) * SIDES + side
        kv_z(d, slot).wait_recv()
        kv_y(lane_at(-d), side).start()

    def w_z(m, d, slot):
        return remote(
            weight_block(m, lane_at(d)),
            landed[m].at[slot],
            w_zs.at[m, d],
            w_r.at[m, slot],
            at_sp(lane_at(d), side),
        )

    def w_y(m, lane_of, side_of):
        slot = lane_of * SIDES + side_of
        return remote(
            landed[m].at[slot],
            landed[m].at[slot],
            w_ys.at[m, lane_of],
            w_r.at[m, slot],
            at_sp(lane, other_side),
        )

    for m in range(3):
        for d in range(1, lanes):
            w_z(m, d, sp).start()
        own_copies[m].wait()
        w_y(m, lane, side).start()

    eye = (
        lax.broadcasted_iota(jnp.int32, (rows, rows), 0)
        == lax.broadcasted_iota(jnp.int32, (rows, rows), 1)
    ).astype(jnp.bfloat16)
    across = (((1,), (1,)), ((), ()))
    q_doc = doc_in[0:1, :].astype(jnp.float32)

    @pl.loop(0, n)
    def _(k):
        lane_of = (lane + k) % lanes
        side_of = (side + k // lanes) % SIDES
        slot = lane_of * SIDES + side_of

        @pl.when(k >= lanes)
        def _():
            kv_y(lane_of, side_of).wait_recv()

        upright = lax.dot_general(eye, kv[slot, 0:kv_vals, :], across, preferred_element_type=jnp.float32)
        key = upright[:, 0:head_dim].astype(jnp.bfloat16)
        same = upright[:, head_dim : head_dim + 1] == q_doc
        value = kv[slot, kv_vals:, :]
        for h in range(heads):
            at = slice(h * head_dim, (h + 1) * head_dim)
            scores = jnp.dot(key, q_ref[at, :], preferred_element_type=jnp.float32)
            scores = jnp.where(same, scores, NEG)
            before = top[h]
            now = jnp.maximum(before, jnp.max(scores, axis=0, keepdims=True))
            weights = jnp.exp(scores - now)
            shrink = jnp.exp(before - now)
            top[h] = now
            total[h] = total[h] * shrink + jnp.sum(weights, axis=0, keepdims=True)
            acc[at, :] = acc[at, :] * shrink + jnp.dot(
                value, weights.astype(jnp.bfloat16), preferred_element_type=jnp.float32
            )

    pieces = []
    for h in range(heads):
        at = slice(h * head_dim, (h + 1) * head_dim)
        pieces.append((acc[at, :] / total[h]).astype(jnp.bfloat16))
    standing = jnp.concatenate(pieces, axis=0)
    attended = lax.dot_general(eye, standing, across, preferred_element_type=jnp.float32).astype(
        jnp.bfloat16
    )
    for i in range(nt):
        att_out[i] = attended[i * chunk : (i + 1) * chunk]

    def att_copy(d, peer, slot):
        return remote(
            att_out.at[peer], att.at[slot], att_s.at[d], att_r.at[slot], {"sp": sp, "tp": peer}
        )

    for d in range(1, nt):
        att_copy(d, (tp + d) % nt, tp).start()
    att[tp] = att_out[tp]

    def project(slot):
        return (
            jnp.dot(att[slot], ow[slot], preferred_element_type=jnp.float32)
            .astype(jnp.bfloat16)
            .astype(jnp.float32)
        )

    own_copies[4].wait()
    resid[...] = tok[...].astype(jnp.float32) + project(tp)
    for d in range(1, nt):
        slot = (tp + nt - d) % nt
        att_copy(d, tp, slot).wait_recv()
    ow_core(xi, other_core).wait_recv()
    resid[...] += project(xi * 2 + other_core)
    for d in range(1, xs):
        x_of = x_at(xs - d)
        remote(out_weight, ow.at[x_of * 2 + core], ow_xs.at[d], ow_r.at[x_of * 2 + core], at_tp(x_of, core)).wait_recv()
        ow_core(x_of, core).start()
        resid[...] += project(x_of * 2 + core)
    for d in range(1, xs):
        x_of = x_at(xs - d)
        ow_core(x_of, other_core).wait_recv()
        resid[...] += project(x_of * 2 + other_core)

    whole = resid[...]
    power = jnp.mean(whole * whole, axis=-1, keepdims=True)
    act[lane, tp] = (whole * lax.rsqrt(power + EPS) * norm_gain[...]).astype(jnp.bfloat16)

    def act_up(lane_of):
        return remote(
            act.at[lane_of, tp],
            act.at[lane_of, tp],
            act_us.at[lane_of],
            act_r.at[lane_of, tp],
            at_sp(lane + 1, side),
        )

    def act_down(lane_of):
        return remote(
            act.at[lane_of, tp],
            act.at[lane_of, tp],
            act_ds.at[lane_of],
            act_r.at[lane_of, tp],
            at_sp(lane - 1, side),
        )

    def act_x(d, lane_of, slot):
        return remote(
            act.at[lane_of, slot],
            act.at[lane_of, slot],
            act_xs.at[d, lane_of],
            act_r.at[lane_of, slot],
            at_tp(x_at(d), core),
        )

    def act_core(lane_of, x_of, core_of):
        slot = x_of * 2 + core_of
        return remote(
            act.at[lane_of, slot],
            act.at[lane_of, slot],
            act_cs.at[lane_of, x_of],
            act_r.at[lane_of, slot],
            at_tp(xi, other_core),
        )

    def act_out(lane_of):
        for d in range(1, xs):
            act_x(d, lane_of, tp).start()
        act_core(lane_of, xi, core).start()

    def act_from_x(lane_of):
        for d in range(1, xs):
            x_of = x_at(xs - d)
            act_x(d, lane_of, x_of * 2 + core).wait_recv()
            act_core(lane_of, x_of, core).start()

    rises, falls = lane < lanes - 1, lane > 0

    @pl.when(rises)
    def _():
        act_up(lane).start()

    @pl.when(falls)
    def _():
        act_down(lane).start()

    act_out(lane)

    def forward_weight(m):
        for d in range(1, lanes):
            lane_of = lane_at(lanes - d)
            w_z(m, d, lane_of * SIDES + side).wait_recv()
            w_y(m, lane_of, side).start()

    forward_weight(0)
    for d in range(1, lanes):

        @pl.when(lane >= d)
        def _():
            act_up(lane - d).wait_recv()

            @pl.when(rises)
            def _():
                act_up(lane - d).start()

            act_out(lane - d)

        @pl.when(lane + d < lanes)
        def _():
            act_down(lane + d).wait_recv()

            @pl.when(falls)
            def _():
                act_down(lane + d).start()

            act_out(lane + d)

        if d == 1:
            act_from_x(lane)
    forward_weight(1)
    for d in range(1, lanes):

        @pl.when(lane >= d)
        def _():
            act_from_x(lane - d)

        @pl.when(lane + d < lanes)
        def _():
            act_from_x(lane + d)

    for m in range(2):
        for d in range(lanes):
            w_y(m, lane_at(d), other_side).wait_recv()

    unit = lax.broadcasted_iota(jnp.int32, (nt * chunk, width), 1)
    mine = unit >= (lane // (lanes - 1)) * cut * LANE
    for d in range(lanes):
        lane_of = lane_at(d)
        for x_of in range(xs):
            act_core(lane_of, x_of, other_core).wait_recv()

    @pl.loop(0, lanes)
    def _(lane_of):
        inputs = act[lane_of].reshape(nt * chunk, act.shape[-1])
        gated = jnp.dot(inputs, gw[...].reshape(n * gw.shape[1], width), preferred_element_type=jnp.float32)
        lifted = jnp.dot(inputs, uw[...].reshape(n * uw.shape[1], width), preferred_element_type=jnp.float32)
        hidden = gated * lax.logistic(gated) * lifted
        hidden = jnp.where(mine, hidden, 0.0).astype(jnp.bfloat16)
        for x_of in range(xs):
            for core_of in range(2):
                start = (x_of * 2 + core_of) * chunk
                hid[core_of, x_of, lane_of] = hidden[start : start + chunk]

    cols = dw.shape[2]
    share = xs * lanes * chunk

    def rs_core(s):
        return remote(core_out.at[s], core_in.at[s], rs_cs.at[s], rs_cr.at[s], at_tp(xi, other_core))

    def rs_x(s, d):
        return remote(x_out.at[s, d], x_in.at[s, d], rs_xs.at[s, d], rs_xr.at[s, d], at_tp(x_at(d), core))

    def rs_z(s, d):
        return remote(
            z_out.at[s, d], z_in.at[s, d], rs_zs.at[s, d], rs_zr.at[s, d], at_sp(lane_at(d), side)
        )

    def columns(s):
        return pl.ds(pl.multiple_of(s * cols, cols), cols)

    def ag_x(s, d, slot):
        piece = out.at[slot, :, columns(s)]
        return remote(piece, piece, ag_xs.at[s, d], ag_r.at[s, slot], at_tp(x_at(d), core))

    def ag_core(s, x_of, core_of):
        slot = x_of * 2 + core_of
        piece = out.at[slot, :, columns(s)]
        return remote(piece, piece, ag_cs.at[s, x_of], ag_r.at[s, slot], at_tp(xi, other_core))

    def slot_of(k):
        return (k // SIDES) * SIDES + (side + k) % SIDES

    @pl.loop(0, n + 4)
    def _(k):
        @pl.when(k < n)
        def _():
            s = slot_of(k)
            lane_of, side_of = s // SIDES, s % SIDES

            @pl.when(side_of == side)
            def _():
                @pl.when(lane_of != lane)
                def _():
                    w_z(2, 1, s).wait_recv()
                    w_y(2, lane_of, side).start()

            @pl.when(side_of != side)
            def _():
                w_y(2, lane_of, other_side).wait_recv()

            away = hid[other_core].reshape(share, width)
            core_out[s] = (
                jnp.dot(away, dw[s], preferred_element_type=jnp.float32)
                .astype(jnp.bfloat16)
                .reshape(xs, lanes, chunk, cols)
            )
            rs_core(s).start()
            near = hid[core].reshape(share, width)
            keep[s] = jnp.dot(near, dw[s], preferred_element_type=jnp.float32).reshape(
                xs, lanes, chunk, cols
            )

        @pl.when((k >= 1) & (k < n + 1))
        def _():
            s = slot_of(k - 1)
            rs_core(s).wait_recv()
            for d in range(1, xs):
                x_to = x_at(d)
                x_out[s, d] = (keep[s, x_to] + core_in[s, x_to].astype(jnp.float32)).astype(jnp.bfloat16)
                rs_x(s, d).start()
            x_keep[s] = keep[s, xi] + core_in[s, xi].astype(jnp.float32)

        @pl.when((k >= 2) & (k < n + 2))
        def _():
            s = slot_of(k - 2)
            for d in range(1, xs):
                rs_x(s, d).wait_recv()

            def summed(lane_to):
                value = x_keep[s, lane_to]
                for d in range(1, xs):
                    value = value + x_in[s, d, lane_to].astype(jnp.float32)
                return value

            for d in range(1, lanes):
                z_out[s, d] = summed(lane_at(d)).astype(jnp.bfloat16)
                rs_z(s, d).start()
            z_keep[s] = summed(lane)

        @pl.when((k >= 3) & (k < n + 3))
        def _():
            s = slot_of(k - 3)
            value = z_keep[s]
            for d in range(1, lanes):
                rs_z(s, d).wait_recv()
                value = value + z_in[s, d].astype(jnp.float32)
            out[tp, :, columns(s)] = (resid[:, columns(s)] + value).astype(jnp.bfloat16)
            for d in range(1, xs):
                ag_x(s, d, tp).start()
            ag_core(s, xi, core).start()

        @pl.when(k >= 4)
        def _():
            s = slot_of(k - 4)
            for d in range(1, xs):
                x_of = x_at(xs - d)
                ag_x(s, d, x_of * 2 + core).wait_recv()
                ag_core(s, x_of, core).start()

    @pl.loop(0, n)
    def _(s):
        for x_of in range(xs):
            ag_core(s, x_of, other_core).wait_recv()
            ag_core(s, x_of, core).wait_send()
        for d in range(1, xs):
            ag_x(s, d, tp).wait_send()
            rs_x(s, d).wait_send()
        rs_core(s).wait_send()
        for d in range(1, lanes):
            rs_z(s, d).wait_send()

    for d in range(1, lanes):
        kv_z(d, sp).wait_send()
        for m in range(3):
            w_z(m, d, sp).wait_send()
    for lane_of in range(lanes):
        kv_y(lane_of, side).wait_send()
        for m in range(3):
            w_y(m, lane_of, side).wait_send()
        for d in range(1, xs):
            act_x(d, lane_of, tp).wait_send()
        for x_of in range(xs):
            act_core(lane_of, x_of, core).wait_send()

        @pl.when(rises & (lane_of <= lane))
        def _():
            act_up(lane_of).wait_send()

        @pl.when(falls & (lane_of >= lane))
        def _():
            act_down(lane_of).wait_send()

    for d in range(1, xs):
        ow_x(d).wait_send()
    for x_of in range(xs):
        ow_core(x_of, core).wait_send()
    for d in range(1, nt):
        att_copy(d, (tp + d) % nt, tp).wait_send()


VMEM_LIMIT = 60 * 1024 * 1024


def fused_plan(n, nt, rows, width, head_dim, heads, units):
    if n % SIDES or n < 2 * SIDES or nt % 2 or rows % nt or units % LANE:
        return None
    lanes, xs, chunk, blocks = n // SIDES, nt // 2, rows // nt, units // LANE
    wide = -(-blocks // lanes)
    cols = width // n
    if chunk % 16 or rows % LANE or cols % LANE or width % n or head_dim % 32:
        return None
    if wide > blocks or (lanes - 1) * wide > blocks:
        return None
    wu = wide * LANE
    bf, f32 = jnp.bfloat16, jnp.float32
    shapes = [
        ((n, 2 * head_dim + 16, rows), bf),
        ((heads * head_dim, rows), bf),
        ((heads, 1, rows), f32),
        ((heads, 1, rows), f32),
        ((heads * head_dim, rows), f32),
        ((nt, chunk, heads * head_dim), bf),
        ((nt, chunk, heads * head_dim), bf),
        ((nt, heads * head_dim, width), bf),
        ((chunk, width), bf),
        ((chunk, width), f32),
        ((lanes, nt, chunk, width), bf),
        ((n, width // n, wu), bf),
        ((n, width // n, wu), bf),
        ((n, wu, cols), bf),
        ((2, xs, lanes, chunk, wu), bf),
        ((n, xs, lanes, chunk, cols), f32),
        ((n, xs, lanes, chunk, cols), bf),
        ((n, xs, lanes, chunk, cols), bf),
        ((n, lanes, chunk, cols), f32),
        ((n, xs, lanes, chunk, cols), bf),
        ((n, xs, lanes, chunk, cols), bf),
        ((n, chunk, cols), f32),
        ((n, lanes, chunk, cols), bf),
        ((n, lanes, chunk, cols), bf),
    ]
    size = 0
    for shape, kind in shapes:
        count = 1
        for extent in shape:
            count *= extent
        size += count * jnp.dtype(kind).itemsize
    if size > VMEM_LIMIT * 3 // 4:
        return None
    sems = [(lanes,), (lanes,), (n,), (3,), (3, lanes), (3, lanes), (3, n), (2,)]
    sems += [(xs,), (xs,), (nt,), (nt,), (nt,)]
    sems += [(lanes,), (lanes,), (xs, lanes), (lanes, xs), (lanes, nt)]
    sems += [(n,), (n,), (n, xs), (n, xs), (n, lanes), (n, lanes), (n, xs), (n, xs), (n, nt)]
    return wide, [pltpu.VMEM(*s) for s in shapes] + [pltpu.SemaphoreType.DMA(s) for s in sems]


def fused_layer(
    n, nt, plan, tokens_in, queries, keys, values, doc_ids, query_gain, key_norm_scale,
    out_weight, norm_gain, gate_weight, up_weight, down_weight,
):
    wide, scratch = plan
    rows, width = tokens_in.shape
    head_dim = query_gain.shape[0]
    places = lax.axis_index("sp") * rows + jnp.arange(rows, dtype=jnp.int32)
    half = head_dim // 2
    freqs = THETA ** (-2.0 * jnp.arange(half // 2, dtype=jnp.float32) / half)
    angles = [
        freqs[:, None] * spot.astype(jnp.float32)[None, :] for spot in (places // GRID, places % GRID)
    ]
    table = jnp.concatenate([f(a) for a in angles for f in (jnp.cos, jnp.sin)], axis=0)
    docs = jnp.broadcast_to(doc_ids.astype(jnp.bfloat16)[None, :], (16, rows))
    hbm = pl.BlockSpec(memory_space=pl.ANY)
    out = pl.pallas_call(
        functools.partial(fused_kernel, n, nt, wide),
        out_shape=jax.ShapeDtypeStruct((nt, rows // nt, width), jnp.bfloat16),
        in_specs=[VM] * 8 + [hbm] * 5,
        out_specs=VM,
        scratch_shapes=scratch,
        compiler_params=pltpu.CompilerParams(
            collective_id=3, has_side_effects=True, vmem_limit_bytes=VMEM_LIMIT
        ),
        name="fused_layer",
    )(
        queries.T, keys.T, values.T, docs, table,
        query_gain.reshape(head_dim, 1), key_norm_scale.reshape(head_dim, 1), norm_gain.reshape(1, width),
        tokens_in, out_weight, gate_weight, up_weight, down_weight,
    )
    return out.reshape(rows, width)


def per_device(
    n,
    nt,
    tokens_in,
    queries,
    keys,
    values,
    doc_ids,
    query_gain,
    key_norm_scale,
    out_weight,
    norm_gain,
    gate_weight,
    up_weight,
    down_weight,
):
    tok_rows = tokens_in.shape[0]
    head_dim = query_gain.shape[0]
    local_heads = queries.shape[1] // head_dim
    plan = None
    if keys.shape[1] == head_dim:
        plan = fused_plan(
            n, nt, tok_rows, tokens_in.shape[1], head_dim, local_heads, gate_weight.shape[1]
        )
    if plan is not None:
        return fused_layer(
            n, nt, plan, tokens_in, queries, keys, values, doc_ids, query_gain, key_norm_scale,
            out_weight, norm_gain, gate_weight, up_weight, down_weight,
        )
    places = lax.axis_index("sp") * tok_rows + jnp.arange(tok_rows, dtype=jnp.int32)
    lattice_row = (places // GRID).astype(jnp.float32)
    lattice_column = (places % GRID).astype(jnp.float32)
    q_local = normalized_rotated(queries, query_gain, local_heads, lattice_row, lattice_column)
    q_rows = q_local.transpose(1, 0, 2).reshape(local_heads * tok_rows, head_dim)
    lanes = [[2 * j + side for j in range(n // 2)] for side in range(2)]
    gate_up_all = lax.all_gather(
        pair_share(n, [gate_weight, up_weight], 1, 0), "sp", axis_index_groups=lanes, axis=0, tiled=True
    )
    down_all = lax.all_gather(
        pair_share(n, [down_weight], 0, 1), "sp", axis_index_groups=lanes, axis=1, tiled=True
    )
    turned = normalized_rotated(keys, key_norm_scale, 1, lattice_row, lattice_column)
    packed = jnp.concatenate([turned.reshape(tok_rows, head_dim), values], axis=1)
    kv_all, doc_all = gather_sp(n, packed, doc_ids.reshape(1, tok_rows))
    row_docs = jnp.tile(doc_ids, local_heads)
    first_doc = doc_ids[0]
    last_doc = doc_ids[-1]
    scale = head_dim ** (-0.5)
    total_rows = local_heads * tok_rows

    def absorb_block(state, key_block, value_block, doc_block):

        def absorb(current):
            running_max, running_sum, running_acc = current
            scores = (
                jnp.einsum("qd,kd->qk", q_rows, key_block, preferred_element_type=jnp.float32)
                * scale
            )
            same = row_docs[:, None] == doc_block[None, :]
            scores = jnp.where(same, scores, NEG)
            new_max = jnp.maximum(running_max, jnp.max(scores, axis=1))
            weights = jnp.where(same, jnp.exp(scores - new_max[:, None]), 0.0)
            shrink = jnp.exp(running_max - new_max)
            new_sum = running_sum * shrink + jnp.sum(weights, axis=1)
            new_acc = running_acc * shrink[:, None] + jnp.dot(
                weights.astype(jnp.bfloat16), value_block, preferred_element_type=jnp.float32
            )
            return (new_max, new_sum, new_acc)

        touches = (doc_block[0] <= last_doc) & (doc_block[-1] >= first_doc)
        return lax.cond(touches, absorb, lambda current: current, state)

    initial = (
        jnp.full((total_rows,), NEG, jnp.float32),
        jnp.zeros((total_rows,), jnp.float32),
        jnp.zeros((total_rows, head_dim), jnp.float32),
    )
    carry = initial
    shards = n
    joined = 1
    while joined * 2 <= shards and shards % (joined * 2) == 0 and (joined * 2 * tok_rows <= 1024):
        joined = joined * 2
    blocks = shards // joined
    span_rows = joined * tok_rows
    key_blocks = kv_all[..., :head_dim].reshape(blocks, span_rows, head_dim)
    value_blocks = kv_all[..., head_dim:].reshape(blocks, span_rows, head_dim)
    doc_blocks = doc_all.reshape(blocks, span_rows)

    def visit(state, inputs):
        key_block, value_block, doc_block = inputs
        return (absorb_block(state, key_block, value_block, doc_block), None)

    carry, unused = lax.scan(visit, carry, (key_blocks, value_blocks, doc_blocks))
    attended = (carry[2] / carry[1][:, None]).astype(jnp.bfloat16)
    attended = (
        attended.reshape(local_heads, tok_rows, head_dim)
        .transpose(1, 0, 2)
        .reshape(tok_rows, local_heads * head_dim)
    )
    partial_value = jnp.dot(attended, out_weight, preferred_element_type=jnp.float32)
    normed, resid = mid_stage(nt, partial_value.astype(jnp.bfloat16), tokens_in, norm_gain)
    normed = normed.reshape(2 * tok_rows, -1)
    both = jnp.dot(normed, gate_up_all, preferred_element_type=jnp.float32)
    units = both.shape[1] // 2
    hidden = (jax.nn.silu(both[:, :units]) * both[:, units:]).astype(jnp.bfloat16)
    fed_part = jnp.dot(hidden, down_all, preferred_element_type=jnp.float32)
    out = last_stage(nt, fed_part.astype(jnp.bfloat16), resid)
    return out.reshape(tok_rows, -1)


def solution(mesh):
    return jax.shard_map(
        functools.partial(per_device, mesh.shape["sp"], mesh.shape["tp"]),
        mesh=mesh,
        in_specs=(
            P("sp", None),
            P("sp", "tp"),
            P("sp", "tp"),
            P("sp", "tp"),
            P("sp"),
            P(),
            P(),
            P("tp", None),
            P(),
            P("sp", "tp"),
            P("sp", "tp"),
            P("tp", "sp"),
        ),
        out_specs=P("sp", None),
        check_vma=False,
    )
```

```python
import functools

import jax
import jax.numpy as jnp
from jax import lax
from jax.experimental import pallas as pl
from jax.experimental.pallas import tpu as pltpu
from jax.sharding import PartitionSpec as P

GRID = 64


EPS = 1e-06
THETA = 10000.0
NEG = -1e30


def rotate_half(block, angle):
    half_dim = block.shape[-1] // 2
    cosine = jnp.cos(angle)[:, None, :]
    sine = jnp.sin(angle)[:, None, :]
    first = block[..., :half_dim]
    second = block[..., half_dim:]
    return jnp.concatenate(
        [first * cosine - second * sine, second * cosine + first * sine], axis=-1
    )


def normalized_rotated(values_in, gain, heads, lattice_row, lattice_column):
    full = values_in.astype(jnp.float32).reshape(values_in.shape[0], heads, -1)
    full = full * lax.rsqrt(jnp.mean(full * full, axis=-1, keepdims=True) + EPS) * gain
    half_dim = full.shape[-1] // 2
    freqs = THETA ** (-2.0 * jnp.arange(half_dim // 2, dtype=jnp.float32) / half_dim)
    by_row = rotate_half(full[..., :half_dim], lattice_row[:, None] * freqs[None, :])
    by_col = rotate_half(full[..., half_dim:], lattice_column[:, None] * freqs[None, :])
    return jnp.concatenate([by_row, by_col], axis=-1).astype(jnp.bfloat16)


MESH = pl.DeviceIdType.MESH
VM = pl.BlockSpec(memory_space=pltpu.VMEM)


def params(cid):
    return pltpu.CompilerParams(
        collective_id=cid, has_side_effects=True, vmem_limit_bytes=56 * 1024 * 1024
    )


def greet(count, where):
    barrier = pltpu.get_barrier_semaphore()

    @pl.loop(1, count)
    def _(step):
        pl.semaphore_signal(barrier, inc=1, device_id=where(step), device_id_type=MESH)

    pl.semaphore_wait(barrier, count - 1)


def gather_kernel(n, kv_ref, doc_ref, kv_out, doc_out, send, recv, doc_send, doc_recv):
    me = lax.axis_index("sp")

    def where(step):
        return {"sp": lax.rem(me + step, n)}

    def copies(step, slot):
        return (
            pltpu.make_async_remote_copy(
                kv_ref, kv_out.at[slot], send.at[step], recv.at[step], where(step), MESH
            ),
            pltpu.make_async_remote_copy(
                doc_ref, doc_out.at[slot], doc_send.at[step], doc_recv.at[step], where(step), MESH
            ),
        )

    greet(n, where)

    @pl.loop(1, n)
    def _(step):
        for copy in copies(step, me):
            copy.start()

    kv_out[me] = kv_ref[...]
    doc_out[me] = doc_ref[...]

    @pl.loop(1, n)
    def _(step):
        for copy in copies(step, lax.rem(me + n - step, n)):
            copy.wait_recv()
            copy.wait_send()


def gather_sp(n, packed, docs):
    return pl.pallas_call(
        functools.partial(gather_kernel, n),
        out_shape=(
            jax.ShapeDtypeStruct((n,) + packed.shape, packed.dtype),
            jax.ShapeDtypeStruct((n,) + docs.shape, docs.dtype),
        ),
        in_specs=[VM, VM],
        out_specs=(VM, VM),
        scratch_shapes=[pltpu.SemaphoreType.DMA((n,))] * 4,
        compiler_params=params(0),
        name="gather_sp",
    )(packed, docs)


def mid_kernel(
    nt, partial_ref, tokens_ref, gain_ref, normed_out, resid_out, landing, send, recv, send2, recv2
):
    sp, tp = lax.axis_index("sp"), lax.axis_index("tp")
    side = lax.rem(sp, 2)
    base = sp - side
    group = 2 * nt
    me = side * nt + tp
    rows = resid_out.shape[0]

    def where(step):
        other = lax.rem(me + step, group)
        return {"sp": base + other // nt, "tp": lax.rem(other, nt)}

    def part(step):
        peer = lax.rem(tp + step, nt)
        return pltpu.make_async_remote_copy(
            partial_ref.at[peer],
            landing.at[step],
            send.at[step],
            recv.at[step],
            {"sp": sp, "tp": peer},
            MESH,
        )

    def spread(step, slot):
        return pltpu.make_async_remote_copy(
            normed_out.at[slot], normed_out.at[slot], send2.at[step], recv2.at[step], where(step), MESH
        )

    greet(group, where)
    for step in range(1, nt):
        part(step).start()
    for step in range(1, nt):
        part(step).wait_recv()
    chunk = 16

    @pl.loop(0, rows // chunk)
    def _(i):
        at = pl.ds(pl.multiple_of(i * chunk, chunk), chunk)
        mixed = partial_ref[tp, at].astype(jnp.float32)
        for step in range(1, nt):
            mixed = mixed + landing[step, at].astype(jnp.float32)
        resid = tokens_ref[tp, at].astype(jnp.float32) + mixed
        resid_out[at] = resid
        power = jnp.mean(resid * resid, axis=-1, keepdims=True)
        normed_out[me, at] = (resid * lax.rsqrt(power + EPS) * gain_ref[...]).astype(jnp.bfloat16)

    for step in range(1, group):
        spread(step, me).start()
    for step in range(1, group):
        copy = spread(step, lax.rem(me + group - step, group))
        copy.wait_recv()
        copy.wait_send()
    for step in range(1, nt):
        part(step).wait_send()


def mid_stage(nt, part, tokens, gain):
    rows, width = part.shape[0] // nt, part.shape[1]
    return pl.pallas_call(
        functools.partial(mid_kernel, nt),
        out_shape=(
            jax.ShapeDtypeStruct((2 * nt, rows, width), jnp.bfloat16),
            jax.ShapeDtypeStruct((rows, width), jnp.float32),
        ),
        in_specs=[VM, VM, VM],
        out_specs=(VM, VM),
        scratch_shapes=[pltpu.VMEM((nt, rows, width), jnp.bfloat16)]
        + [pltpu.SemaphoreType.DMA((nt,))] * 2
        + [pltpu.SemaphoreType.DMA((2 * nt,))] * 2,
        compiler_params=params(1),
        name="mid_stage",
    )(part.reshape(nt, rows, width), tokens.reshape(nt, rows, width), gain.reshape(1, width))


def last_kernel(nt, fed_ref, resid_ref, out_ref, landing, send, recv, send2, recv2):
    sp, tp = lax.axis_index("sp"), lax.axis_index("tp")
    side = lax.rem(sp, 2)
    base = sp - side
    group = 2 * nt
    me = side * nt + tp
    rows = resid_ref.shape[0]

    def where(step):
        other = lax.rem(me + step, group)
        return {"sp": base + other // nt, "tp": lax.rem(other, nt)}

    def part(step):
        return pltpu.make_async_remote_copy(
            fed_ref.at[lax.rem(me + step, group)],
            landing.at[step],
            send.at[step],
            recv.at[step],
            where(step),
            MESH,
        )

    def spread(step, slot):
        return pltpu.make_async_remote_copy(
            out_ref.at[slot],
            out_ref.at[slot],
            send2.at[step],
            recv2.at[step],
            {"sp": sp, "tp": lax.rem(tp + step, nt)},
            MESH,
        )

    greet(group, where)
    for step in range(1, group):
        part(step).start()
    for step in range(1, group):
        part(step).wait_recv()
    chunk = 16

    @pl.loop(0, rows // chunk)
    def _(i):
        at = pl.ds(pl.multiple_of(i * chunk, chunk), chunk)
        fed = fed_ref[me, at].astype(jnp.float32)
        for step in range(1, group):
            fed = fed + landing[step, at].astype(jnp.float32)
        out_ref[tp, at] = (resid_ref[at] + fed).astype(jnp.bfloat16)

    for step in range(1, nt):
        spread(step, tp).start()
    for step in range(1, nt):
        copy = spread(step, lax.rem(tp + nt - step, nt))
        copy.wait_recv()
        copy.wait_send()
    for step in range(1, group):
        part(step).wait_send()


def last_stage(nt, fed, resid):
    rows, width = resid.shape
    return pl.pallas_call(
        functools.partial(last_kernel, nt),
        out_shape=jax.ShapeDtypeStruct((nt, rows, width), jnp.bfloat16),
        in_specs=[VM, VM],
        out_specs=VM,
        scratch_shapes=[pltpu.VMEM((2 * nt, rows, width), jnp.bfloat16)]
        + [pltpu.SemaphoreType.DMA((2 * nt,))] * 2
        + [pltpu.SemaphoreType.DMA((nt,))] * 2,
        compiler_params=params(2),
        name="last_stage",
    )(fed.reshape(2 * nt, rows, width), resid)


def pair_share(n, arrays, axis, joins):
    side = lax.rem(lax.axis_index("sp"), 2)
    own, away = [], []
    for array in arrays:
        half = array.shape[axis] // 2
        own.append(lax.dynamic_slice_in_dim(array, side * half, half, axis))
        away.append(lax.dynamic_slice_in_dim(array, (1 - side) * half, half, axis))
    own = jnp.concatenate(own, axis=axis)
    away = jnp.concatenate(away, axis=axis)
    came = lax.ppermute(away, "sp", [(i, i ^ 1) for i in range(n)])
    first = jnp.where(side == 0, own, came)
    second = jnp.where(side == 0, came, own)
    return jnp.concatenate([first, second], axis=joins)


SIDES = 2
LANE = 128
PIECES = 4


def turned(block, gain, table):
    power = jnp.mean(block * block, axis=0, keepdims=True)
    full = block * lax.rsqrt(power + EPS) * gain
    half = block.shape[0] // 2
    quarter = half // 2
    pieces = []
    for part in range(2):
        first = full[part * half : part * half + quarter]
        second = full[part * half + quarter : (part + 1) * half]
        cosine = table[2 * part * quarter : (2 * part + 1) * quarter]
        sine = table[(2 * part + 1) * quarter : (2 * part + 2) * quarter]
        pieces += [first * cosine - second * sine, second * cosine + first * sine]
    return jnp.concatenate(pieces, axis=0)


def identity(size):
    down = lax.broadcasted_iota(jnp.int32, (size, size), 0)
    across = lax.broadcasted_iota(jnp.int32, (size, size), 1)
    return (down == across).astype(jnp.bfloat16)


def flipped(array):
    return lax.dot_general(
        identity(array.shape[1]), array, (((1,), (1,)), ((), ())), preferred_element_type=jnp.float32
    )


def fused_kernel(
    n,
    nt,
    wide,
    q_in,
    k_in,
    v_in,
    doc_in,
    const_in,
    norm_gain,
    tokens,
    out_weight,
    gate,
    up,
    down,
    out,
    kv,
    q_ref,
    top,
    total,
    acc,
    part,
    part_in,
    px_out,
    px_in,
    ow,
    tok,
    resid,
    act,
    gw,
    uw,
    dw,
    hid,
    keep,
    core_out,
    core_in,
    x_keep,
    x_out,
    x_in,
    z_keep,
    z_out,
    z_in,
    kv_zs,
    kv_ys,
    kv_r,
    w_own,
    w_zs,
    w_ys,
    w_r,
    misc,
    pc_s,
    pc_r,
    px_s,
    px_r,
    act_zs,
    act_xs,
    act_cs,
    act_r,
    rs_cs,
    rs_cr,
    rs_xs,
    rs_xr,
    rs_zs,
    rs_zr,
    ag_xs,
    ag_cs,
    ag_r,
):
    sp, tp = lax.axis_index("sp"), lax.axis_index("tp")
    lanes, xs = n // SIDES, nt // 2
    bits = lanes.bit_length() - 1
    lane, side = sp // SIDES, sp % SIDES
    xi, core = tp // 2, tp % 2
    rows = q_in.shape[0]
    head_dim = k_in.shape[0]
    heads = q_in.shape[1] // head_dim
    chunk = rows // nt
    blocks = gate.shape[1] // LANE
    width = wide * LANE
    last = blocks - (lanes - 1) * wide
    kv_docs = head_dim
    kv_vals = kv.shape[1] - head_dim
    table = const_in[0:head_dim, :]
    q_gain = const_in[head_dim : 2 * head_dim, :]
    k_gain = const_in[2 * head_dim : 3 * head_dim, :]

    def at_sp(lane_to, side_to):
        return {"sp": lane_to * SIDES + side_to, "tp": tp}

    def at_tp(x_to, core_to):
        return {"sp": sp, "tp": x_to * 2 + core_to}

    def remote(src, dst, send, recv, where):
        return pltpu.make_async_remote_copy(src, dst, send, recv, where, MESH)

    def lane_at(d):
        return (lane + d) % lanes

    def x_at(d):
        return (xi + d) % xs

    def bit_of(value, b):
        return (value // (1 << b)) % 2

    def partner(b):
        return lane + (1 - 2 * bit_of(lane, b)) * (1 << b)

    other_side = 1 - side
    other_core = 1 - core

    barrier = pltpu.get_barrier_semaphore()
    for d in range(1, lanes):
        pl.semaphore_signal(barrier, inc=1, device_id=at_sp(lane_at(d), side), device_id_type=MESH)
    pl.semaphore_signal(barrier, inc=1, device_id=at_sp(lane, other_side), device_id_type=MESH)
    for d in range(1, xs):
        pl.semaphore_signal(barrier, inc=1, device_id=at_tp(x_at(d), core), device_id_type=MESH)
    pl.semaphore_signal(barrier, inc=1, device_id=at_tp(xi, other_core), device_id_type=MESH)

    def rank(lane_to):
        return lane_to + core * (lanes - 1 - 2 * lane_to)

    def sized(lane_to, action):
        if last == wide:
            action(width)
            return
        few = rank(lane_to) // (lanes - 1)

        @pl.when(few == 1)
        def _():
            action(last * LANE)

        @pl.when(few == 0)
        def _():
            action(width)

    def weight_block(m, lane_to, size):
        at = pl.ds(pl.multiple_of(rank(lane_to) * width, LANE), size)
        if m == 0:
            return gate.at[:, at]
        if m == 1:
            return up.at[:, at]
        return down.at[at, :]

    def landing(m, slot, size):
        if m == 0:
            return gw.at[slot, :, 0:size]
        if m == 1:
            return uw.at[slot, :, 0:size]
        return dw.at[slot, 0:size, :]

    def w_local(m, size):
        return pltpu.make_async_copy(weight_block(m, lane, size), landing(m, sp, size), w_own.at[m])

    ow_copy = pltpu.make_async_copy(out_weight, ow, misc.at[0])
    tok_copy = pltpu.make_async_copy(
        tokens.at[pl.ds(pl.multiple_of(tp * chunk, chunk), chunk)], tok, misc.at[1]
    )
    for m in range(3):
        sized(lane, lambda size, m=m: w_local(m, size).start())
    ow_copy.start()
    tok_copy.start()

    kv[sp, 0:head_dim, :] = turned(k_in[...].astype(jnp.float32), k_gain, table).astype(jnp.bfloat16)
    q_doc = doc_in[...].astype(jnp.float32)
    kv[sp, kv_docs:kv_vals, :] = jnp.broadcast_to(q_doc, (kv_vals - kv_docs, rows)).astype(jnp.bfloat16)
    kv[sp, kv_vals:, :] = v_in[...]

    pl.semaphore_wait(barrier, lanes - 1 + 1 + xs - 1 + 1)

    def kv_z(d, slot):
        return remote(kv.at[slot], kv.at[slot], kv_zs.at[d], kv_r.at[slot], at_sp(lane_at(d), side))

    def kv_y(lane_of, side_of):
        slot = lane_of * SIDES + side_of
        return remote(
            kv.at[slot], kv.at[slot], kv_ys.at[lane_of], kv_r.at[slot], at_sp(lane, other_side)
        )

    for d in range(1, lanes):
        kv_z(d, sp).start()
    kv_y(lane, side).start()

    def w_z(m, d, slot, lane_to, size):
        return remote(
            weight_block(m, lane_to, size),
            landing(m, slot, size),
            w_zs.at[m, d],
            w_r.at[m, slot],
            at_sp(lane_at(d), side),
        )

    def w_y(m, lane_of, side_of, size):
        slot = lane_of * SIDES + side_of
        return remote(
            landing(m, slot, size),
            landing(m, slot, size),
            w_ys.at[m, lane_of],
            w_r.at[m, slot],
            at_sp(lane, other_side),
        )

    def start_weight(m):
        for d in range(1, lanes):
            lane_to = lane_at(d)
            sized(lane_to, lambda size, d=d, lane_to=lane_to: w_z(m, d, sp, lane_to, size).start())

        def own(size):
            w_local(m, size).wait()
            w_y(m, lane, side, size).start()

        sized(lane, own)

    def w_arrived(m, slot):
        sized(lane, lambda size: w_z(m, 1, slot, lane, size).wait_recv())

    def w_forward(m, lane_of):
        sized(lane, lambda size: w_y(m, lane_of, side, size).start())

    def forward_weight(m):
        for d in range(1, lanes):
            lane_of = lane_at(lanes - d)
            w_arrived(m, lane_of * SIDES + side)
            w_forward(m, lane_of)

    scale = head_dim ** (-0.5)
    standing_q = flipped(q_in[...])
    for h in range(heads):
        at = slice(h * head_dim, (h + 1) * head_dim)
        query = turned(standing_q[at, :], q_gain, table)
        q_ref[at, :] = (query.astype(jnp.bfloat16).astype(jnp.float32) * scale).astype(jnp.bfloat16)
    top[...] = jnp.full(top.shape, NEG, jnp.float32)
    total[...] = jnp.zeros(total.shape, jnp.float32)
    acc[...] = jnp.zeros(acc.shape, jnp.float32)

    def absorb(slot):
        upright = lax.dot_general(
            identity(rows),
            kv[slot, 0:kv_vals, :],
            (((1,), (1,)), ((), ())),
            preferred_element_type=jnp.float32,
        )
        key = upright[:, 0:head_dim].astype(jnp.bfloat16)
        same = upright[:, head_dim : head_dim + 1] == q_doc
        value = kv[slot, kv_vals:, :]
        for h in range(heads):
            at = slice(h * head_dim, (h + 1) * head_dim)
            scores = jnp.dot(key, q_ref[at, :], preferred_element_type=jnp.float32)
            scores = jnp.where(same, scores, NEG)
            before = top[h]
            now = jnp.maximum(before, jnp.max(scores, axis=0, keepdims=True))
            weights = jnp.exp(scores - now)
            shrink = jnp.exp(before - now)
            top[h] = now
            total[h] = total[h] * shrink + jnp.sum(weights, axis=0, keepdims=True)
            acc[at, :] = acc[at, :] * shrink + jnp.dot(
                value, weights.astype(jnp.bfloat16), preferred_element_type=jnp.float32
            )

    @pl.loop(0, SIDES)
    def _(k):
        side_of = (side + k) % SIDES

        @pl.when(k > 0)
        def _():
            kv_y(lane, other_side).wait_recv()

        absorb(lane * SIDES + side_of)

    @pl.loop(0, SIDES * (lanes - 1))
    def _(k):
        lane_of = lane_at(k % (lanes - 1) + 1)
        side_of = (side + k // (lanes - 1)) % SIDES
        slot = lane_of * SIDES + side_of

        @pl.when(k < lanes - 1)
        def _():
            kv_z(1, slot).wait_recv()
            kv_y(lane_of, side).start()

        @pl.when(k == lanes - 2)
        def _():
            start_weight(0)
            start_weight(1)

        @pl.when(k >= lanes - 1)
        def _():
            kv_y(lane_of, other_side).wait_recv()

        absorb(slot)

    pieces = []
    for h in range(heads):
        at = slice(h * head_dim, (h + 1) * head_dim)
        pieces.append((acc[at, :] / total[h]).astype(jnp.bfloat16))
    attended = flipped(jnp.concatenate(pieces, axis=0)).astype(jnp.bfloat16)

    span = ow.shape[1] // PIECES

    def part_core(p):
        return remote(part.at[p, other_core], part_in.at[p], pc_s.at[p], pc_r.at[p], at_tp(xi, other_core))

    def part_x(p, d):
        return remote(px_out.at[p, d], px_in.at[p, d], px_s.at[p, d], px_r.at[p, d], at_tp(x_at(d), core))

    ow_copy.wait()
    for p in range(PIECES):
        product = jnp.dot(
            attended, ow[:, p * span : (p + 1) * span], preferred_element_type=jnp.float32
        ).astype(jnp.bfloat16)
        for x_of in range(xs):
            for core_of in range(2):
                start = (x_of * 2 + core_of) * chunk
                part[p, core_of, x_of] = product[start : start + chunk]
        part_core(p).start()
    tok_copy.wait()
    for p in range(PIECES):
        at = slice(p * span, (p + 1) * span)
        part_core(p).wait_recv()
        for d in range(1, xs):
            x_to = x_at(d)
            px_out[p, d] = (
                part[p, core, x_to].astype(jnp.float32) + part_in[p, x_to].astype(jnp.float32)
            ).astype(jnp.bfloat16)
            part_x(p, d).start()
        resid[:, at] = (
            tok[:, at].astype(jnp.float32)
            + part[p, core, xi].astype(jnp.float32)
            + part_in[p, xi].astype(jnp.float32)
        )
    for p in range(PIECES):
        at = slice(p * span, (p + 1) * span)
        for d in range(1, xs):
            part_x(p, d).wait_recv()
            resid[:, at] += px_in[p, d].astype(jnp.float32)

    whole = resid[...]
    power = jnp.mean(whole * whole, axis=-1, keepdims=True)
    act[lane, tp] = (whole * lax.rsqrt(power + EPS) * norm_gain[...]).astype(jnp.bfloat16)

    def act_z(b, lane_of):
        return remote(
            act.at[lane_of, tp],
            act.at[lane_of, tp],
            act_zs.at[b, lane_of],
            act_r.at[lane_of, tp],
            at_sp(partner(b), side),
        )

    def act_x(d, lane_of, slot):
        return remote(
            act.at[lane_of, slot],
            act.at[lane_of, slot],
            act_xs.at[d, lane_of],
            act_r.at[lane_of, slot],
            at_tp(x_at(d), core),
        )

    def act_core(lane_of, x_of, core_of):
        slot = x_of * 2 + core_of
        return remote(
            act.at[lane_of, slot],
            act.at[lane_of, slot],
            act_cs.at[lane_of, x_of],
            act_r.at[lane_of, slot],
            at_tp(xi, other_core),
        )

    def act_out(lane_of):
        for d in range(1, xs):
            act_x(d, lane_of, tp).start()
        act_core(lane_of, xi, core).start()

    def act_from_x(lane_of):
        for d in range(1, xs):
            x_of = x_at(xs - d)
            act_x(d, lane_of, x_of * 2 + core).wait_recv()
            act_core(lane_of, x_of, core).start()

    for b in reversed(range(bits)):
        act_z(b, lane).start()
    act_out(lane)
    forward_weight(0)
    act_from_x(lane)
    forward_weight(1)
    for b in reversed(range(bits)):
        if b == 0:
            start_weight(2)
        mate = partner(b)
        count = lanes >> (b + 1)
        for i in range(count):
            turn = (mate // (1 << (b + 1)) + i) % count
            lane_of = mate % (1 << (b + 1)) + turn * (1 << (b + 1))
            act_z(b, lane_of).wait_recv()
            for lower in reversed(range(b)):
                act_z(lower, lane_of).start()
            act_out(lane_of)

    for m in range(2):
        for d in range(lanes):
            sized(lane, lambda size, m=m, d=d: w_y(m, lane_at(d), other_side, size).wait_recv())

    few_here = rank(lane) // (lanes - 1)
    unit = lax.broadcasted_iota(jnp.int32, (nt * chunk, width), 1)
    mine = unit < (wide - few_here * (wide - last)) * LANE
    if last < wide:

        @pl.when(few_here == 1)
        def _():
            dw[:, last * LANE :, :] = jnp.zeros((n, width - last * LANE, dw.shape[2]), dw.dtype)

    @pl.loop(0, lanes)
    def _(i):
        lane_of = 0
        for b in range(bits):
            lane_of = lane_of + (bit_of(lane, b) + bit_of(i, bits - 1 - b)) % 2 * (1 << b)

        @pl.when(i > 0)
        def _():
            act_from_x(lane_of)

        for x_of in range(xs):
            act_core(lane_of, x_of, other_core).wait_recv()
        inputs = act[lane_of].reshape(nt * chunk, act.shape[-1])
        gated = jnp.dot(inputs, gw[...].reshape(n * gw.shape[1], width), preferred_element_type=jnp.float32)
        lifted = jnp.dot(inputs, uw[...].reshape(n * uw.shape[1], width), preferred_element_type=jnp.float32)
        hidden = gated * lax.logistic(gated) * lifted
        hidden = jnp.where(mine, hidden, 0.0).astype(jnp.bfloat16)
        for x_of in range(xs):
            for core_of in range(2):
                start = (x_of * 2 + core_of) * chunk
                hid[core_of, x_of, lane_of] = hidden[start : start + chunk]

    cols = dw.shape[2]
    share = xs * lanes * chunk
    starts = [lanes - (lanes >> b) for b in range(bits)]

    def rs_core(s):
        return remote(core_out.at[s], core_in.at[s], rs_cs.at[s], rs_cr.at[s], at_tp(xi, other_core))

    def rs_x(s, d):
        return remote(x_out.at[s, d], x_in.at[s, d], rs_xs.at[s, d], rs_xr.at[s, d], at_tp(x_at(d), core))

    def rs_z(s, b):
        piece = pl.ds(starts[b], lanes >> (b + 1))
        return remote(
            z_out.at[s, piece], z_in.at[s, piece], rs_zs.at[s, b], rs_zr.at[s, b], at_sp(partner(b), side)
        )

    def columns(s):
        return pl.ds(pl.multiple_of(s * cols, cols), cols)

    def ag_x(s, d, slot):
        piece = out.at[slot, :, columns(s)]
        return remote(piece, piece, ag_xs.at[s, d], ag_r.at[s, slot], at_tp(x_at(d), core))

    def ag_core(s, x_of, core_of):
        slot = x_of * 2 + core_of
        piece = out.at[slot, :, columns(s)]
        return remote(piece, piece, ag_cs.at[s, x_of], ag_r.at[s, slot], at_tp(xi, other_core))

    def slot_of(k):
        j = k // SIDES
        lane_of = lanes // 2 + (1 - 2 * (j % 2)) * (j // 2) - j % 2
        return lane_of * SIDES + (side + k) % SIDES

    def multiply(k):
        s = slot_of(k)
        lane_of, side_of = s // SIDES, s % SIDES

        @pl.when(side_of == side)
        def _():
            @pl.when(lane_of != lane)
            def _():
                w_arrived(2, s)
                w_forward(2, lane_of)

        @pl.when(side_of != side)
        def _():
            sized(lane, lambda size: w_y(2, lane_of, other_side, size).wait_recv())

        away = hid[other_core].reshape(share, width)
        core_out[s] = (
            jnp.dot(away, dw[s], preferred_element_type=jnp.float32)
            .astype(jnp.bfloat16)
            .reshape(xs, lanes, chunk, cols)
        )
        rs_core(s).start()
        near = hid[core].reshape(share, width)
        keep[s] = jnp.dot(near, dw[s], preferred_element_type=jnp.float32).reshape(xs, lanes, chunk, cols)

    def reduce_core(k):
        s = slot_of(k)
        rs_core(s).wait_recv()
        for d in range(1, xs):
            x_to = x_at(d)
            x_out[s, d] = (keep[s, x_to] + core_in[s, x_to].astype(jnp.float32)).astype(jnp.bfloat16)
            rs_x(s, d).start()
        x_keep[s] = keep[s, xi] + core_in[s, xi].astype(jnp.float32)

    def reduce_lanes(b, k):
        s = slot_of(k)
        if b == 0:
            for d in range(1, xs):
                rs_x(s, d).wait_recv()
        else:
            rs_z(s, b - 1).wait_recv()

        def summed(h):
            if b == 0:
                value = x_keep[s, h]
                for d in range(1, xs):
                    value = value + x_in[s, d, h].astype(jnp.float32)
                return value
            return z_keep[b - 1, s, h] + z_in[s, starts[b - 1] + h].astype(jnp.float32)

        if b == bits:
            out[tp, :, columns(s)] = (resid[:, columns(s)] + summed(0)).astype(jnp.bfloat16)
            for d in range(1, xs):
                ag_x(s, d, tp).start()
            ag_core(s, xi, core).start()
            return
        mine_here = bit_of(lane, b)
        count = lanes >> (b + 1)
        for h in range(count):
            z_out[s, starts[b] + h] = summed(1 - mine_here + 2 * h).astype(jnp.bfloat16)
        rs_z(s, b).start()
        for h in range(count):
            z_keep[b, s, h] = summed(mine_here + 2 * h)

    def spread(k):
        s = slot_of(k)
        for d in range(1, xs):
            x_of = x_at(xs - d)
            ag_x(s, d, x_of * 2 + core).wait_recv()
            ag_core(s, x_of, core).start()

    stages = [(0, multiply), (1, reduce_core)]
    at = 3
    for b in range(bits + 1):
        stages.append((at, functools.partial(reduce_lanes, b)))
        at += 2
    stages.append((at, spread))

    @pl.loop(0, n + at)
    def _(k):
        for lag, action in reversed(stages):

            @pl.when((k >= lag) & (k < n + lag))
            def _(lag=lag, action=action):
                action(k - lag)

    @pl.loop(0, n)
    def _(s):
        for x_of in range(xs):
            ag_core(s, x_of, other_core).wait_recv()
            ag_core(s, x_of, core).wait_send()
        for d in range(1, xs):
            ag_x(s, d, tp).wait_send()
            rs_x(s, d).wait_send()
        rs_core(s).wait_send()
        for b in range(bits):
            rs_z(s, b).wait_send()

    for d in range(1, lanes):
        kv_z(d, sp).wait_send()
        for m in range(3):
            lane_to = lane_at(d)
            sized(lane_to, lambda size, m=m, d=d, lane_to=lane_to: w_z(m, d, sp, lane_to, size).wait_send())
    for lane_of in range(lanes):
        kv_y(lane_of, side).wait_send()
        for m in range(3):
            sized(lane, lambda size, m=m, lane_of=lane_of: w_y(m, lane_of, side, size).wait_send())
        for d in range(1, xs):
            act_x(d, lane_of, tp).wait_send()
        for x_of in range(xs):
            act_core(lane_of, x_of, core).wait_send()
    for b in range(bits):
        for h in range(lanes >> (b + 1)):
            act_z(b, lane % (1 << (b + 1)) + h * (1 << (b + 1))).wait_send()
    for p in range(PIECES):
        part_core(p).wait_send()
        for d in range(1, xs):
            part_x(p, d).wait_send()


VMEM_LIMIT = 60 * 1024 * 1024


def fused_plan(n, nt, rows, width, head_dim, heads, units):
    if n % SIDES or n < 2 * SIDES or nt % 2 or nt < 4 or rows % nt or units % LANE:
        return None
    lanes, xs, chunk, blocks = n // SIDES, nt // 2, rows // nt, units // LANE
    wide = -(-blocks // lanes)
    cols = width // n
    if chunk % 16 or rows % LANE or width % (n * LANE) or width % (PIECES * LANE) or head_dim % 64:
        return None
    if lanes & (lanes - 1) or (lanes - 1) * wide >= blocks:
        return None
    wu = wide * LANE
    bits = lanes.bit_length() - 1
    span = width // PIECES
    bf, f32 = jnp.bfloat16, jnp.float32
    shapes = [
        ((n, 2 * head_dim + 16, rows), bf),
        ((heads * head_dim, rows), bf),
        ((heads, 1, rows), f32),
        ((heads, 1, rows), f32),
        ((heads * head_dim, rows), f32),
        ((PIECES, 2, xs, chunk, span), bf),
        ((PIECES, xs, chunk, span), bf),
        ((PIECES, xs, chunk, span), bf),
        ((PIECES, xs, chunk, span), bf),
        ((heads * head_dim, width), bf),
        ((chunk, width), bf),
        ((chunk, width), f32),
        ((lanes, nt, chunk, width), bf),
        ((n, cols, wu), bf),
        ((n, cols, wu), bf),
        ((n, wu, cols), bf),
        ((2, xs, lanes, chunk, wu), bf),
        ((n, xs, lanes, chunk, cols), f32),
        ((n, xs, lanes, chunk, cols), bf),
        ((n, xs, lanes, chunk, cols), bf),
        ((n, lanes, chunk, cols), f32),
        ((n, xs, lanes, chunk, cols), bf),
        ((n, xs, lanes, chunk, cols), bf),
        ((bits, n, lanes // 2, chunk, cols), f32),
        ((n, lanes - 1, chunk, cols), bf),
        ((n, lanes - 1, chunk, cols), bf),
    ]
    size = 0
    for shape, kind in shapes:
        count = 1
        for extent in shape:
            count *= extent
        size += count * jnp.dtype(kind).itemsize
    if size > VMEM_LIMIT * 3 // 4:
        return None
    sems = [(lanes,), (lanes,), (n,), (3,), (3, lanes), (3, lanes), (3, n), (2,)]
    sems += [(PIECES,), (PIECES,), (PIECES, xs), (PIECES, xs)]
    sems += [(bits, lanes), (xs, lanes), (lanes, xs), (lanes, nt)]
    sems += [(n,), (n,), (n, xs), (n, xs), (n, bits), (n, bits), (n, xs), (n, xs), (n, nt)]
    return wide, [pltpu.VMEM(*s) for s in shapes] + [pltpu.SemaphoreType.DMA(s) for s in sems]


def fused_layer(
    n, nt, plan, tokens_in, queries, keys, values, doc_ids, query_gain, key_norm_scale,
    out_weight, norm_gain, gate_weight, up_weight, down_weight,
):
    wide, scratch = plan
    rows, width = tokens_in.shape
    head_dim = query_gain.shape[0]
    places = lax.axis_index("sp") * rows + jnp.arange(rows, dtype=jnp.int32)
    half = head_dim // 2
    freqs = THETA ** (-2.0 * jnp.arange(half // 2, dtype=jnp.float32) / half)
    angles = [
        freqs[:, None] * spot.astype(jnp.float32)[None, :] for spot in (places // GRID, places % GRID)
    ]
    consts = [f(a) for a in angles for f in (jnp.cos, jnp.sin)]
    consts += [jnp.broadcast_to(g[:, None], (head_dim, rows)) for g in (query_gain, key_norm_scale)]
    hbm = pl.BlockSpec(memory_space=pl.ANY)
    out = pl.pallas_call(
        functools.partial(fused_kernel, n, nt, wide),
        out_shape=jax.ShapeDtypeStruct((nt, rows // nt, width), jnp.bfloat16),
        in_specs=[VM] * 6 + [hbm] * 5,
        out_specs=VM,
        scratch_shapes=scratch,
        compiler_params=pltpu.CompilerParams(
            collective_id=3, has_side_effects=True, vmem_limit_bytes=VMEM_LIMIT
        ),
        name="fused_layer",
    )(
        queries, keys.T, values.T, doc_ids.reshape(1, rows), jnp.concatenate(consts, axis=0),
        norm_gain.reshape(1, width), tokens_in, out_weight, gate_weight, up_weight, down_weight,
    )
    return out.reshape(rows, width)


def per_device(
    n,
    nt,
    tokens_in,
    queries,
    keys,
    values,
    doc_ids,
    query_gain,
    key_norm_scale,
    out_weight,
    norm_gain,
    gate_weight,
    up_weight,
    down_weight,
):
    tok_rows = tokens_in.shape[0]
    head_dim = query_gain.shape[0]
    local_heads = queries.shape[1] // head_dim
    plan = None
    if keys.shape[1] == head_dim:
        plan = fused_plan(
            n, nt, tok_rows, tokens_in.shape[1], head_dim, local_heads, gate_weight.shape[1]
        )
    if plan is not None:
        return fused_layer(
            n, nt, plan, tokens_in, queries, keys, values, doc_ids, query_gain, key_norm_scale,
            out_weight, norm_gain, gate_weight, up_weight, down_weight,
        )
    places = lax.axis_index("sp") * tok_rows + jnp.arange(tok_rows, dtype=jnp.int32)
    lattice_row = (places // GRID).astype(jnp.float32)
    lattice_column = (places % GRID).astype(jnp.float32)
    q_local = normalized_rotated(queries, query_gain, local_heads, lattice_row, lattice_column)
    q_rows = q_local.transpose(1, 0, 2).reshape(local_heads * tok_rows, head_dim)
    lanes = [[2 * j + side for j in range(n // 2)] for side in range(2)]
    gate_up_all = lax.all_gather(
        pair_share(n, [gate_weight, up_weight], 1, 0), "sp", axis_index_groups=lanes, axis=0, tiled=True
    )
    down_all = lax.all_gather(
        pair_share(n, [down_weight], 0, 1), "sp", axis_index_groups=lanes, axis=1, tiled=True
    )
    turned = normalized_rotated(keys, key_norm_scale, 1, lattice_row, lattice_column)
    packed = jnp.concatenate([turned.reshape(tok_rows, head_dim), values], axis=1)
    kv_all, doc_all = gather_sp(n, packed, doc_ids.reshape(1, tok_rows))
    row_docs = jnp.tile(doc_ids, local_heads)
    first_doc = doc_ids[0]
    last_doc = doc_ids[-1]
    scale = head_dim ** (-0.5)
    total_rows = local_heads * tok_rows

    def absorb_block(state, key_block, value_block, doc_block):

        def absorb(current):
            running_max, running_sum, running_acc = current
            scores = (
                jnp.einsum("qd,kd->qk", q_rows, key_block, preferred_element_type=jnp.float32)
                * scale
            )
            same = row_docs[:, None] == doc_block[None, :]
            scores = jnp.where(same, scores, NEG)
            new_max = jnp.maximum(running_max, jnp.max(scores, axis=1))
            weights = jnp.where(same, jnp.exp(scores - new_max[:, None]), 0.0)
            shrink = jnp.exp(running_max - new_max)
            new_sum = running_sum * shrink + jnp.sum(weights, axis=1)
            new_acc = running_acc * shrink[:, None] + jnp.dot(
                weights.astype(jnp.bfloat16), value_block, preferred_element_type=jnp.float32
            )
            return (new_max, new_sum, new_acc)

        touches = (doc_block[0] <= last_doc) & (doc_block[-1] >= first_doc)
        return lax.cond(touches, absorb, lambda current: current, state)

    initial = (
        jnp.full((total_rows,), NEG, jnp.float32),
        jnp.zeros((total_rows,), jnp.float32),
        jnp.zeros((total_rows, head_dim), jnp.float32),
    )
    carry = initial
    shards = n
    joined = 1
    while joined * 2 <= shards and shards % (joined * 2) == 0 and (joined * 2 * tok_rows <= 1024):
        joined = joined * 2
    blocks = shards // joined
    span_rows = joined * tok_rows
    key_blocks = kv_all[..., :head_dim].reshape(blocks, span_rows, head_dim)
    value_blocks = kv_all[..., head_dim:].reshape(blocks, span_rows, head_dim)
    doc_blocks = doc_all.reshape(blocks, span_rows)

    def visit(state, inputs):
        key_block, value_block, doc_block = inputs
        return (absorb_block(state, key_block, value_block, doc_block), None)

    carry, unused = lax.scan(visit, carry, (key_blocks, value_blocks, doc_blocks))
    attended = (carry[2] / carry[1][:, None]).astype(jnp.bfloat16)
    attended = (
        attended.reshape(local_heads, tok_rows, head_dim)
        .transpose(1, 0, 2)
        .reshape(tok_rows, local_heads * head_dim)
    )
    partial_value = jnp.dot(attended, out_weight, preferred_element_type=jnp.float32)
    normed, resid = mid_stage(nt, partial_value.astype(jnp.bfloat16), tokens_in, norm_gain)
    normed = normed.reshape(2 * tok_rows, -1)
    both = jnp.dot(normed, gate_up_all, preferred_element_type=jnp.float32)
    units = both.shape[1] // 2
    hidden = (jax.nn.silu(both[:, :units]) * both[:, units:]).astype(jnp.bfloat16)
    fed_part = jnp.dot(hidden, down_all, preferred_element_type=jnp.float32)
    out = last_stage(nt, fed_part.astype(jnp.bfloat16), resid)
    return out.reshape(tok_rows, -1)


def solution(mesh):
    return jax.shard_map(
        functools.partial(per_device, mesh.shape["sp"], mesh.shape["tp"]),
        mesh=mesh,
        in_specs=(
            P("sp", None),
            P("sp", "tp"),
            P("sp", "tp"),
            P("sp", "tp"),
            P("sp"),
            P(),
            P(),
            P("tp", None),
            P(),
            P("sp", "tp"),
            P("sp", "tp"),
            P("tp", "sp"),
        ),
        out_specs=P("sp", None),
        check_vma=False,
    )
```

```python
import functools

import jax
import jax.numpy as jnp
from jax import lax
from jax.experimental import pallas as pl
from jax.experimental.pallas import tpu as pltpu
from jax.sharding import PartitionSpec as P

GRID = 64


EPS = 1e-06
THETA = 10000.0
NEG = -1e30


def rotate_half(block, angle):
    half_dim = block.shape[-1] // 2
    cosine = jnp.cos(angle)[:, None, :]
    sine = jnp.sin(angle)[:, None, :]
    first = block[..., :half_dim]
    second = block[..., half_dim:]
    return jnp.concatenate(
        [first * cosine - second * sine, second * cosine + first * sine], axis=-1
    )


def normalized_rotated(values_in, gain, heads, lattice_row, lattice_column):
    full = values_in.astype(jnp.float32).reshape(values_in.shape[0], heads, -1)
    full = full * lax.rsqrt(jnp.mean(full * full, axis=-1, keepdims=True) + EPS) * gain
    half_dim = full.shape[-1] // 2
    freqs = THETA ** (-2.0 * jnp.arange(half_dim // 2, dtype=jnp.float32) / half_dim)
    by_row = rotate_half(full[..., :half_dim], lattice_row[:, None] * freqs[None, :])
    by_col = rotate_half(full[..., half_dim:], lattice_column[:, None] * freqs[None, :])
    return jnp.concatenate([by_row, by_col], axis=-1).astype(jnp.bfloat16)


MESH = pl.DeviceIdType.MESH
VM = pl.BlockSpec(memory_space=pltpu.VMEM)


def params(cid):
    return pltpu.CompilerParams(
        collective_id=cid, has_side_effects=True, vmem_limit_bytes=56 * 1024 * 1024
    )


def greet(count, where):
    barrier = pltpu.get_barrier_semaphore()

    @pl.loop(1, count)
    def _(step):
        pl.semaphore_signal(barrier, inc=1, device_id=where(step), device_id_type=MESH)

    pl.semaphore_wait(barrier, count - 1)


def gather_kernel(n, kv_ref, doc_ref, kv_out, doc_out, send, recv, doc_send, doc_recv):
    me = lax.axis_index("sp")

    def where(step):
        return {"sp": lax.rem(me + step, n)}

    def copies(step, slot):
        return (
            pltpu.make_async_remote_copy(
                kv_ref, kv_out.at[slot], send.at[step], recv.at[step], where(step), MESH
            ),
            pltpu.make_async_remote_copy(
                doc_ref, doc_out.at[slot], doc_send.at[step], doc_recv.at[step], where(step), MESH
            ),
        )

    greet(n, where)

    @pl.loop(1, n)
    def _(step):
        for copy in copies(step, me):
            copy.start()

    kv_out[me] = kv_ref[...]
    doc_out[me] = doc_ref[...]

    @pl.loop(1, n)
    def _(step):
        for copy in copies(step, lax.rem(me + n - step, n)):
            copy.wait_recv()
            copy.wait_send()


def gather_sp(n, packed, docs):
    return pl.pallas_call(
        functools.partial(gather_kernel, n),
        out_shape=(
            jax.ShapeDtypeStruct((n,) + packed.shape, packed.dtype),
            jax.ShapeDtypeStruct((n,) + docs.shape, docs.dtype),
        ),
        in_specs=[VM, VM],
        out_specs=(VM, VM),
        scratch_shapes=[pltpu.SemaphoreType.DMA((n,))] * 4,
        compiler_params=params(0),
        name="gather_sp",
    )(packed, docs)


def mid_kernel(
    nt, partial_ref, tokens_ref, gain_ref, normed_out, resid_out, landing, send, recv, send2, recv2
):
    sp, tp = lax.axis_index("sp"), lax.axis_index("tp")
    side = lax.rem(sp, 2)
    base = sp - side
    group = 2 * nt
    me = side * nt + tp
    rows = resid_out.shape[0]

    def where(step):
        other = lax.rem(me + step, group)
        return {"sp": base + other // nt, "tp": lax.rem(other, nt)}

    def part(step):
        peer = lax.rem(tp + step, nt)
        return pltpu.make_async_remote_copy(
            partial_ref.at[peer],
            landing.at[step],
            send.at[step],
            recv.at[step],
            {"sp": sp, "tp": peer},
            MESH,
        )

    def spread(step, slot):
        return pltpu.make_async_remote_copy(
            normed_out.at[slot], normed_out.at[slot], send2.at[step], recv2.at[step], where(step), MESH
        )

    greet(group, where)
    for step in range(1, nt):
        part(step).start()
    for step in range(1, nt):
        part(step).wait_recv()
    chunk = 16

    @pl.loop(0, rows // chunk)
    def _(i):
        at = pl.ds(pl.multiple_of(i * chunk, chunk), chunk)
        mixed = partial_ref[tp, at].astype(jnp.float32)
        for step in range(1, nt):
            mixed = mixed + landing[step, at].astype(jnp.float32)
        resid = tokens_ref[tp, at].astype(jnp.float32) + mixed
        resid_out[at] = resid
        power = jnp.mean(resid * resid, axis=-1, keepdims=True)
        normed_out[me, at] = (resid * lax.rsqrt(power + EPS) * gain_ref[...]).astype(jnp.bfloat16)

    for step in range(1, group):
        spread(step, me).start()
    for step in range(1, group):
        copy = spread(step, lax.rem(me + group - step, group))
        copy.wait_recv()
        copy.wait_send()
    for step in range(1, nt):
        part(step).wait_send()


def mid_stage(nt, part, tokens, gain):
    rows, width = part.shape[0] // nt, part.shape[1]
    return pl.pallas_call(
        functools.partial(mid_kernel, nt),
        out_shape=(
            jax.ShapeDtypeStruct((2 * nt, rows, width), jnp.bfloat16),
            jax.ShapeDtypeStruct((rows, width), jnp.float32),
        ),
        in_specs=[VM, VM, VM],
        out_specs=(VM, VM),
        scratch_shapes=[pltpu.VMEM((nt, rows, width), jnp.bfloat16)]
        + [pltpu.SemaphoreType.DMA((nt,))] * 2
        + [pltpu.SemaphoreType.DMA((2 * nt,))] * 2,
        compiler_params=params(1),
        name="mid_stage",
    )(part.reshape(nt, rows, width), tokens.reshape(nt, rows, width), gain.reshape(1, width))


def last_kernel(nt, fed_ref, resid_ref, out_ref, landing, send, recv, send2, recv2):
    sp, tp = lax.axis_index("sp"), lax.axis_index("tp")
    side = lax.rem(sp, 2)
    base = sp - side
    group = 2 * nt
    me = side * nt + tp
    rows = resid_ref.shape[0]

    def where(step):
        other = lax.rem(me + step, group)
        return {"sp": base + other // nt, "tp": lax.rem(other, nt)}

    def part(step):
        return pltpu.make_async_remote_copy(
            fed_ref.at[lax.rem(me + step, group)],
            landing.at[step],
            send.at[step],
            recv.at[step],
            where(step),
            MESH,
        )

    def spread(step, slot):
        return pltpu.make_async_remote_copy(
            out_ref.at[slot],
            out_ref.at[slot],
            send2.at[step],
            recv2.at[step],
            {"sp": sp, "tp": lax.rem(tp + step, nt)},
            MESH,
        )

    greet(group, where)
    for step in range(1, group):
        part(step).start()
    for step in range(1, group):
        part(step).wait_recv()
    chunk = 16

    @pl.loop(0, rows // chunk)
    def _(i):
        at = pl.ds(pl.multiple_of(i * chunk, chunk), chunk)
        fed = fed_ref[me, at].astype(jnp.float32)
        for step in range(1, group):
            fed = fed + landing[step, at].astype(jnp.float32)
        out_ref[tp, at] = (resid_ref[at] + fed).astype(jnp.bfloat16)

    for step in range(1, nt):
        spread(step, tp).start()
    for step in range(1, nt):
        copy = spread(step, lax.rem(tp + nt - step, nt))
        copy.wait_recv()
        copy.wait_send()
    for step in range(1, group):
        part(step).wait_send()


def last_stage(nt, fed, resid):
    rows, width = resid.shape
    return pl.pallas_call(
        functools.partial(last_kernel, nt),
        out_shape=jax.ShapeDtypeStruct((nt, rows, width), jnp.bfloat16),
        in_specs=[VM, VM],
        out_specs=VM,
        scratch_shapes=[pltpu.VMEM((2 * nt, rows, width), jnp.bfloat16)]
        + [pltpu.SemaphoreType.DMA((2 * nt,))] * 2
        + [pltpu.SemaphoreType.DMA((nt,))] * 2,
        compiler_params=params(2),
        name="last_stage",
    )(fed.reshape(2 * nt, rows, width), resid)


def pair_share(n, arrays, axis, joins):
    side = lax.rem(lax.axis_index("sp"), 2)
    own, away = [], []
    for array in arrays:
        half = array.shape[axis] // 2
        own.append(lax.dynamic_slice_in_dim(array, side * half, half, axis))
        away.append(lax.dynamic_slice_in_dim(array, (1 - side) * half, half, axis))
    own = jnp.concatenate(own, axis=axis)
    away = jnp.concatenate(away, axis=axis)
    came = lax.ppermute(away, "sp", [(i, i ^ 1) for i in range(n)])
    first = jnp.where(side == 0, own, came)
    second = jnp.where(side == 0, came, own)
    return jnp.concatenate([first, second], axis=joins)


SIDES = 2
LANE = 128
PIECES = 4


def turned(block, gain, table):
    power = jnp.mean(block * block, axis=0, keepdims=True)
    full = block * lax.rsqrt(power + EPS) * gain
    half = block.shape[0] // 2
    quarter = half // 2
    pieces = []
    for part in range(2):
        first = full[part * half : part * half + quarter]
        second = full[part * half + quarter : (part + 1) * half]
        cosine = table[2 * part * quarter : (2 * part + 1) * quarter]
        sine = table[(2 * part + 1) * quarter : (2 * part + 2) * quarter]
        pieces += [first * cosine - second * sine, second * cosine + first * sine]
    return jnp.concatenate(pieces, axis=0)


def identity(size):
    down = lax.broadcasted_iota(jnp.int32, (size, size), 0)
    across = lax.broadcasted_iota(jnp.int32, (size, size), 1)
    return (down == across).astype(jnp.bfloat16)


def flipped(array):
    return lax.dot_general(
        identity(array.shape[1]), array, (((1,), (1,)), ((), ())), preferred_element_type=jnp.float32
    )


def upright_row(row):
    size = row.shape[1]
    down = lax.broadcasted_iota(jnp.int32, (size, size), 0)
    across = lax.broadcasted_iota(jnp.int32, (size, size), 1)
    return jnp.sum(jnp.where(down == across, row, 0.0), axis=1, keepdims=True)


def fused_kernel(
    n,
    nt,
    wide,
    q_in,
    k_in,
    v_in,
    doc_in,
    q_gain_in,
    k_gain_in,
    norm_gain_in,
    tokens,
    out_weight,
    gate,
    up,
    down,
    table_ref,
    out,
    q_raw,
    k_raw,
    doc_ref,
    q_gain_ref,
    k_gain_ref,
    norm_gain,
    kv,
    q_ref,
    top,
    total,
    acc,
    part,
    part_in,
    px_out,
    px_in,
    ow,
    tok,
    resid,
    act,
    gw,
    uw,
    dw,
    gated,
    hid,
    keep,
    core_out,
    core_in,
    x_keep,
    x_out,
    x_in,
    z_keep,
    z_out,
    z_in,
    kv_zs,
    kv_ys,
    kv_r,
    w_own,
    w_zs,
    w_ys,
    w_r,
    misc,
    pc_s,
    pc_r,
    px_s,
    px_r,
    act_zs,
    act_xs,
    act_cs,
    act_r,
    rs_cs,
    rs_cr,
    rs_xs,
    rs_xr,
    rs_zs,
    rs_zr,
    ag_xs,
    ag_cs,
    ag_r,
):
    sp, tp = lax.axis_index("sp"), lax.axis_index("tp")
    lanes, xs = n // SIDES, nt // 2
    bits = lanes.bit_length() - 1
    lane, side = sp // SIDES, sp % SIDES
    xi, core = tp // 2, tp % 2
    rows = q_in.shape[0]
    head_dim = k_in.shape[0]
    heads = q_in.shape[1] // head_dim
    chunk = rows // nt
    blocks = gate.shape[1] // LANE
    width = wide * LANE
    last = blocks - (lanes - 1) * wide
    kv_docs = head_dim
    table = table_ref[...]

    def at_sp(lane_to, side_to):
        return {"sp": lane_to * SIDES + side_to, "tp": tp}

    def at_tp(x_to, core_to):
        return {"sp": sp, "tp": x_to * 2 + core_to}

    def remote(src, dst, send, recv, where):
        return pltpu.make_async_remote_copy(src, dst, send, recv, where, MESH)

    def lane_at(d):
        return (lane + d) % lanes

    def x_at(d):
        return (xi + d) % xs

    def bit_of(value, b):
        return (value // (1 << b)) % 2

    def partner(b):
        return lane + (1 - 2 * bit_of(lane, b)) * (1 << b)

    def mate(e):
        return lane + sum((e >> b) % 2 * (1 - 2 * bit_of(lane, b)) * (1 << b) for b in range(bits))

    def mated(i):
        total_of = 0
        for b in range(bits):
            total_of = total_of + (bit_of(lane, b) + bit_of(i, b)) % 2 * (1 << b)
        return total_of

    def low_bit(e):
        return (e & -e).bit_length() - 1

    other_side = 1 - side
    other_core = 1 - core

    barrier = pltpu.get_barrier_semaphore()
    for d in range(1, lanes):
        pl.semaphore_signal(barrier, inc=1, device_id=at_sp(lane_at(d), side), device_id_type=MESH)
    pl.semaphore_signal(barrier, inc=1, device_id=at_sp(lane, other_side), device_id_type=MESH)
    for d in range(1, xs):
        pl.semaphore_signal(barrier, inc=1, device_id=at_tp(x_at(d), core), device_id_type=MESH)
    pl.semaphore_signal(barrier, inc=1, device_id=at_tp(xi, other_core), device_id_type=MESH)

    def rank(lane_to):
        return lane_to + core * (lanes - 1 - 2 * lane_to)

    def sized(lane_to, action):
        if last == wide:
            action(width)
            return
        few = rank(lane_to) // (lanes - 1)

        @pl.when(few == 1)
        def _():
            action(last * LANE)

        @pl.when(few == 0)
        def _():
            action(width)

    def weight_block(m, lane_to, size):
        at = pl.ds(pl.multiple_of(rank(lane_to) * width, LANE), size)
        if m == 0:
            return gate.at[:, at]
        if m == 1:
            return up.at[:, at]
        return down.at[at, :]

    def landing(m, slot, size):
        if m == 0:
            return gw.at[slot, :, 0:size]
        if m == 1:
            return uw.at[slot, :, 0:size]
        return dw.at[slot, 0:size, :]

    def w_local(m, size):
        return pltpu.make_async_copy(weight_block(m, lane, size), landing(m, sp, size), w_own.at[m])

    ow_copy = pltpu.make_async_copy(out_weight, ow, misc.at[0])
    tok_copy = pltpu.make_async_copy(
        tokens.at[pl.ds(pl.multiple_of(tp * chunk, chunk), chunk)], tok, misc.at[1]
    )
    kv_vals = kv.shape[1] - head_dim
    small = [
        pltpu.make_async_copy(k_in, k_raw, misc.at[2]),
        pltpu.make_async_copy(doc_in, doc_ref, misc.at[3]),
        pltpu.make_async_copy(k_gain_in, k_gain_ref, misc.at[4]),
        pltpu.make_async_copy(v_in, kv.at[sp, kv_vals:, :], misc.at[5]),
        pltpu.make_async_copy(q_in, q_raw, misc.at[6]),
        pltpu.make_async_copy(q_gain_in, q_gain_ref, misc.at[7]),
        pltpu.make_async_copy(norm_gain_in, norm_gain, misc.at[8]),
    ]
    for copy in small:
        copy.start()
    for m in range(3):
        sized(lane, lambda size, m=m: w_local(m, size).start())
    ow_copy.start()
    tok_copy.start()

    for copy in small[:4]:
        copy.wait()
    k_full = turned(k_raw[...].astype(jnp.float32), upright_row(k_gain_ref[...]), table)
    kv[sp, 0:head_dim, :] = k_full.astype(jnp.bfloat16)
    q_doc = doc_ref[...].astype(jnp.float32)
    kv[sp, kv_docs:kv_vals, :] = jnp.broadcast_to(q_doc, (kv_vals - kv_docs, rows)).astype(jnp.bfloat16)

    pl.semaphore_wait(barrier, lanes - 1 + 1 + xs - 1 + 1)

    def kv_z(e, lane_of):
        slot = lane_of * SIDES + side
        return remote(kv.at[slot], kv.at[slot], kv_zs.at[e], kv_r.at[slot], at_sp(mate(e), side))

    def kv_y(lane_of, side_of):
        slot = lane_of * SIDES + side_of
        return remote(
            kv.at[slot], kv.at[slot], kv_ys.at[lane_of], kv_r.at[slot], at_sp(lane, other_side)
        )

    for e in range(1, lanes):
        kv_z(e, lane).start()
    kv_y(lane, side).start()

    def w_z(m, e, slot, lane_to, size):
        return remote(
            weight_block(m, lane_to, size),
            landing(m, slot, size),
            w_zs.at[m, e],
            w_r.at[m, slot],
            at_sp(mate(e), side),
        )

    def w_y(m, lane_of, side_of, size):
        slot = lane_of * SIDES + side_of
        return remote(
            landing(m, slot, size),
            landing(m, slot, size),
            w_ys.at[m, lane_of],
            w_r.at[m, slot],
            at_sp(lane, other_side),
        )

    def send_weight(m, e):
        lane_to = mate(e)
        sized(lane_to, lambda size: w_z(m, e, sp, lane_to, size).start())

    def share_weight(m):
        def own(size):
            w_local(m, size).wait()
            w_y(m, lane, side, size).start()

        sized(lane, own)

    def forward_weight(m, lane_of):
        sized(lane, lambda size: w_z(m, 1, lane_of * SIDES + side, lane, size).wait_recv())
        sized(lane, lambda size: w_y(m, lane_of, side, size).start())

    def w_shared(m, lane_of):
        sized(lane, lambda size: w_y(m, lane_of, other_side, size).wait_recv())

    for e in range(1, lanes):
        send_weight(0, e)
    share_weight(0)

    scale = head_dim ** (-0.5)
    for copy in small[4:]:
        copy.wait()
    standing_q = flipped(q_raw[...])
    q_gain = upright_row(q_gain_ref[...])
    for h in range(heads):
        at = slice(h * head_dim, (h + 1) * head_dim)
        query = turned(standing_q[at, :], q_gain, table)
        q_ref[at, :] = (query.astype(jnp.bfloat16).astype(jnp.float32) * scale).astype(jnp.bfloat16)
    top[...] = jnp.full(top.shape, NEG, jnp.float32)
    total[...] = jnp.zeros(total.shape, jnp.float32)
    acc[...] = jnp.zeros(acc.shape, jnp.float32)

    def absorb(slot):
        upright = lax.dot_general(
            identity(rows),
            kv[slot, 0:kv_vals, :],
            (((1,), (1,)), ((), ())),
            preferred_element_type=jnp.float32,
        )
        key = upright[:, 0:head_dim].astype(jnp.bfloat16)
        same = upright[:, head_dim : head_dim + 1] == q_doc
        value = kv[slot, kv_vals:, :]
        for h in range(heads):
            at = slice(h * head_dim, (h + 1) * head_dim)
            scores = jnp.dot(key, q_ref[at, :], preferred_element_type=jnp.float32)
            scores = jnp.where(same, scores, NEG)
            before = top[h]
            now = jnp.maximum(before, jnp.max(scores, axis=0, keepdims=True))
            weights = jnp.exp(scores - now)
            shrink = jnp.exp(before - now)
            top[h] = now
            total[h] = total[h] * shrink + jnp.sum(weights, axis=0, keepdims=True)
            acc[at, :] = acc[at, :] * shrink + jnp.dot(
                value, weights.astype(jnp.bfloat16), preferred_element_type=jnp.float32
            )

    @pl.loop(0, SIDES)
    def _(k):
        side_of = (side + k) % SIDES

        @pl.when(k > 0)
        def _():
            kv_y(lane, other_side).wait_recv()

        absorb(lane * SIDES + side_of)

    @pl.loop(0, SIDES * (lanes - 1))
    def _(k):
        lane_of = mated(k % (lanes - 1) + 1)
        side_of = (side + k // (lanes - 1)) % SIDES
        slot = lane_of * SIDES + side_of

        @pl.when(k < lanes - 1)
        def _():
            kv_z(1, lane_of).wait_recv()
            kv_y(lane_of, side).start()

        @pl.when(k >= lanes - 1)
        def _():
            kv_y(lane_of, other_side).wait_recv()

        absorb(slot)

    send_weight(1, 1)
    share_weight(1)
    pieces = []
    for h in range(heads):
        at = slice(h * head_dim, (h + 1) * head_dim)
        pieces.append((acc[at, :] / total[h]).astype(jnp.bfloat16))
    attended = flipped(jnp.concatenate(pieces, axis=0)).astype(jnp.bfloat16)

    span = ow.shape[1] // PIECES

    def part_core(p):
        return remote(part.at[p, other_core], part_in.at[p], pc_s.at[p], pc_r.at[p], at_tp(xi, other_core))

    def part_x(p, d):
        return remote(px_out.at[p, d], px_in.at[p, d], px_s.at[p, d], px_r.at[p, d], at_tp(x_at(d), core))

    ow_copy.wait()
    for p in range(PIECES):
        product = jnp.dot(
            attended, ow[:, p * span : (p + 1) * span], preferred_element_type=jnp.float32
        ).astype(jnp.bfloat16)
        for x_of in range(xs):
            for core_of in range(2):
                start = (x_of * 2 + core_of) * chunk
                part[p, core_of, x_of] = product[start : start + chunk]
        part_core(p).start()
    tok_copy.wait()
    for p in range(PIECES):
        at = slice(p * span, (p + 1) * span)
        part_core(p).wait_recv()
        for d in range(1, xs):
            x_to = x_at(d)
            px_out[p, d] = (
                part[p, core, x_to].astype(jnp.float32) + part_in[p, x_to].astype(jnp.float32)
            ).astype(jnp.bfloat16)
            part_x(p, d).start()
        resid[:, at] = (
            tok[:, at].astype(jnp.float32)
            + part[p, core, xi].astype(jnp.float32)
            + part_in[p, xi].astype(jnp.float32)
        )
    for p in range(PIECES):
        at = slice(p * span, (p + 1) * span)
        for d in range(1, xs):
            part_x(p, d).wait_recv()
            resid[:, at] += px_in[p, d].astype(jnp.float32)

    whole = resid[...]
    power = jnp.mean(whole * whole, axis=-1, keepdims=True)
    act[lane, tp] = (whole * lax.rsqrt(power + EPS) * norm_gain[...]).astype(jnp.bfloat16)

    def act_z(b, lane_of):
        return remote(
            act.at[lane_of, tp],
            act.at[lane_of, tp],
            act_zs.at[b, lane_of],
            act_r.at[lane_of, tp],
            at_sp(partner(b), side),
        )

    def act_x(d, lane_of, slot):
        return remote(
            act.at[lane_of, slot],
            act.at[lane_of, slot],
            act_xs.at[d, lane_of],
            act_r.at[lane_of, slot],
            at_tp(x_at(d), core),
        )

    def act_core(lane_of, x_of, core_of):
        slot = x_of * 2 + core_of
        return remote(
            act.at[lane_of, slot],
            act.at[lane_of, slot],
            act_cs.at[lane_of, x_of],
            act_r.at[lane_of, slot],
            at_tp(xi, other_core),
        )

    def act_out(lane_of):
        for d in range(1, xs):
            act_x(d, lane_of, tp).start()
        act_core(lane_of, xi, core).start()

    def act_from_x(lane_of):
        for d in range(1, xs):
            x_of = x_at(xs - d)
            act_x(d, lane_of, x_of * 2 + core).wait_recv()
            act_core(lane_of, x_of, core).start()

    def act_arrived(e):
        step = low_bit(e)
        act_z(step, mate(e)).wait_recv()
        for lower in reversed(range(step)):
            act_z(lower, mate(e)).start()
        act_out(mate(e))

    for b in reversed(range(bits)):
        act_z(b, lane).start()
    act_out(lane)
    for e in range(2, lanes - 1):
        send_weight(1, e)
    for e in range(1, lanes):
        forward_weight(0, mate(e))
    act_from_x(lane)
    for e in range(1, lanes - 1):
        act_arrived(e)
    send_weight(1, lanes - 1)
    share_weight(2)
    forward_weight(1, mate(1))

    few_here = rank(lane) // (lanes - 1)
    unit = lax.broadcasted_iota(jnp.int32, (nt * chunk, width), 1)
    mine = unit < (wide - few_here * (wide - last)) * LANE
    if last < wide:

        @pl.when(few_here == 1)
        def _():
            dw[:, last * LANE :, :] = jnp.zeros((n, width - last * LANE, dw.shape[2]), dw.dtype)

    def depth(ref):
        return ref[...].reshape(ref.shape[0] * ref.shape[1], ref.shape[2])

    for d in range(lanes):
        w_shared(0, lane_at(d))

    @pl.loop(0, lanes)
    def _(i):
        lane_of = mated(i)
        for e in range(1, lanes):

            @pl.when(i == e)
            def _(e=e):
                if e == lanes - 2:
                    act_arrived(e + 1)
                    for f in range(1, lanes):
                        send_weight(2, f)
                act_from_x(mate(e))
                if e > 1:
                    forward_weight(1, mate(e))

        for x_of in range(xs):
            act_core(lane_of, x_of, other_core).wait_recv()
        inputs = act[lane_of].reshape(nt * chunk, act.shape[-1])
        gated[lane_of] = jnp.dot(inputs, depth(gw), preferred_element_type=jnp.float32)

    for d in range(lanes):
        w_shared(1, lane_at(d))

    @pl.loop(0, lanes)
    def _(lane_of):
        inputs = act[lane_of].reshape(nt * chunk, act.shape[-1])
        lifted = jnp.dot(inputs, depth(uw), preferred_element_type=jnp.float32)
        gates = gated[lane_of]
        hidden = jnp.where(mine, gates * lax.logistic(gates) * lifted, 0.0).astype(jnp.bfloat16)
        for x_of in range(xs):
            for core_of in range(2):
                start = (x_of * 2 + core_of) * chunk
                hid[core_of, x_of, lane_of] = hidden[start : start + chunk]

    cols = dw.shape[2]
    share = xs * lanes * chunk
    starts = [lanes - (lanes >> b) for b in range(bits)]

    def rs_core(s):
        return remote(core_out.at[s], core_in.at[s], rs_cs.at[s], rs_cr.at[s], at_tp(xi, other_core))

    def rs_x(s, d):
        return remote(x_out.at[s, d], x_in.at[s, d], rs_xs.at[s, d], rs_xr.at[s, d], at_tp(x_at(d), core))

    def rs_z(s, b):
        piece = pl.ds(starts[b], lanes >> (b + 1))
        return remote(
            z_out.at[s, piece], z_in.at[s, piece], rs_zs.at[s, b], rs_zr.at[s, b], at_sp(partner(b), side)
        )

    def columns(s):
        return pl.ds(pl.multiple_of(s * cols, cols), cols)

    def ag_x(s, d, slot):
        piece = out.at[slot, :, columns(s)]
        return remote(piece, piece, ag_xs.at[s, d], ag_r.at[s, slot], at_tp(x_at(d), core))

    def ag_core(s, x_of, core_of):
        slot = x_of * 2 + core_of
        piece = out.at[slot, :, columns(s)]
        return remote(piece, piece, ag_cs.at[s, x_of], ag_r.at[s, slot], at_tp(xi, other_core))

    def lane_in_order(j):
        return lanes // 2 + (1 - 2 * (j % 2)) * (j // 2) - j % 2

    def slot_of(k):
        return lane_in_order(k % lanes) * SIDES + (side + k // lanes) % SIDES

    upper = lane // (lanes // 2)
    own_turn = upper * (2 * lane - lanes) + (1 - upper) * (lanes - 1 - 2 * lane)

    def early_slot(k):
        own = (n - 1 - k) // (n - SIDES)
        p = (k - SIDES) % (lanes - 1) + 1
        lane_of = lane_in_order(p - 1 + (p - own_turn + lanes - 1) // lanes)
        side_of = (1 - own) * ((k - SIDES) // (lanes - 1)) + own * k
        return (own * lane + (1 - own) * lane_of) * SIDES + (side + side_of) % SIDES

    def multiply(k):
        s = early_slot(k)
        lane_of = s // SIDES

        @pl.when((k > 1) & (k <= lanes))
        def _():
            forward_weight(2, lane_of)

        @pl.when((k == 1) | (k > lanes))
        def _():
            w_shared(2, lane_of)

        away = hid[other_core].reshape(share, width)
        core_out[s] = (
            jnp.dot(away, dw[s], preferred_element_type=jnp.float32)
            .astype(jnp.bfloat16)
            .reshape(xs, lanes, chunk, cols)
        )
        rs_core(s).start()
        near = hid[core].reshape(share, width)
        keep[s] = jnp.dot(near, dw[s], preferred_element_type=jnp.float32).reshape(xs, lanes, chunk, cols)

    def reduce_core(k):
        s = early_slot(k)
        rs_core(s).wait_recv()
        for d in range(1, xs):
            x_to = x_at(d)
            x_out[s, d] = (keep[s, x_to] + core_in[s, x_to].astype(jnp.float32)).astype(jnp.bfloat16)
            rs_x(s, d).start()
        x_keep[s] = keep[s, xi] + core_in[s, xi].astype(jnp.float32)

    def reduce_lanes(b, k):
        s = slot_of(k)
        if b == 0:
            for d in range(1, xs):
                rs_x(s, d).wait_recv()
        else:
            rs_z(s, b - 1).wait_recv()

        def summed(h):
            if b == 0:
                value = x_keep[s, h]
                for d in range(1, xs):
                    value = value + x_in[s, d, h].astype(jnp.float32)
                return value
            return z_keep[b - 1, s, h] + z_in[s, starts[b - 1] + h].astype(jnp.float32)

        if b == bits:
            out[tp, :, columns(s)] = (resid[:, columns(s)] + summed(0)).astype(jnp.bfloat16)
            for d in range(1, xs):
                ag_x(s, d, tp).start()
            ag_core(s, xi, core).start()
            return
        mine_here = bit_of(lane, b)
        count = lanes >> (b + 1)
        for h in range(count):
            z_out[s, starts[b] + h] = summed(1 - mine_here + 2 * h).astype(jnp.bfloat16)
        rs_z(s, b).start()
        for h in range(count):
            z_keep[b, s, h] = summed(mine_here + 2 * h)

    def spread(k):
        s = slot_of(k)
        for d in range(1, xs):
            x_of = x_at(xs - d)
            ag_x(s, d, x_of * 2 + core).wait_recv()
            ag_core(s, x_of, core).start()

    stages = [(0, multiply), (1, reduce_core)]
    at = 5
    for b in range(bits + 1):
        stages.append((at, functools.partial(reduce_lanes, b)))
        at += 2

    @pl.loop(0, n + at - 2)
    def _(k):
        for lag, action in reversed(stages):

            @pl.when((k >= lag) & (k < n + lag))
            def _(lag=lag, action=action):
                action(k - lag)

    pl.loop(0, n)(spread)

    @pl.loop(0, n)
    def _(s):
        for x_of in range(xs):
            ag_core(s, x_of, other_core).wait_recv()
            ag_core(s, x_of, core).wait_send()
        for d in range(1, xs):
            ag_x(s, d, tp).wait_send()
            rs_x(s, d).wait_send()
        rs_core(s).wait_send()
        for b in range(bits):
            rs_z(s, b).wait_send()

    for d in range(1, lanes):
        kv_z(d, lane).wait_send()
        for m in range(3):
            lane_to = mate(d)
            sized(lane_to, lambda size, m=m, d=d, lane_to=lane_to: w_z(m, d, sp, lane_to, size).wait_send())
    for lane_of in range(lanes):
        kv_y(lane_of, side).wait_send()
        for m in range(3):
            sized(lane, lambda size, m=m, lane_of=lane_of: w_y(m, lane_of, side, size).wait_send())
        for d in range(1, xs):
            act_x(d, lane_of, tp).wait_send()
        for x_of in range(xs):
            act_core(lane_of, x_of, core).wait_send()
    for b in range(bits):
        for h in range(lanes >> (b + 1)):
            lane_of = lane % (1 << (b + 1)) + h * (1 << (b + 1))
            act_z(b, lane_of).wait_send()
    for p in range(PIECES):
        part_core(p).wait_send()
        for d in range(1, xs):
            part_x(p, d).wait_send()


VMEM_LIMIT = 60 * 1024 * 1024


def fused_plan(n, nt, rows, width, head_dim, heads, units):
    if n % SIDES or n < 2 * SIDES or nt % 2 or nt < 4 or rows % nt or units % LANE:
        return None
    lanes, xs, chunk, blocks = n // SIDES, nt // 2, rows // nt, units // LANE
    wide = -(-blocks // lanes)
    cols = width // n
    if chunk % 16 or rows % LANE or width % (n * LANE) or width % (PIECES * LANE) or head_dim % 64:
        return None
    if lanes & (lanes - 1) or (lanes - 1) * wide >= blocks:
        return None
    wu = wide * LANE
    bits = lanes.bit_length() - 1
    span = width // PIECES
    bf, f32 = jnp.bfloat16, jnp.float32
    shapes = [
        ((rows, heads * head_dim), bf),
        ((head_dim, rows), bf),
        ((1, rows), jnp.int32),
        ((1, head_dim), f32),
        ((1, head_dim), f32),
        ((1, width), f32),
        ((n, 2 * head_dim + 16, rows), bf),
        ((heads * head_dim, rows), bf),
        ((heads, 1, rows), f32),
        ((heads, 1, rows), f32),
        ((heads * head_dim, rows), f32),
        ((PIECES, 2, xs, chunk, span), bf),
        ((PIECES, xs, chunk, span), bf),
        ((PIECES, xs, chunk, span), bf),
        ((PIECES, xs, chunk, span), bf),
        ((heads * head_dim, width), bf),
        ((chunk, width), bf),
        ((chunk, width), f32),
        ((lanes, nt, chunk, width), bf),
        ((n, cols, wu), bf),
        ((n, cols, wu), bf),
        ((n, wu, cols), bf),
        ((lanes, rows, wu), f32),
        ((2, xs, lanes, chunk, wu), bf),
        ((n, xs, lanes, chunk, cols), f32),
        ((n, xs, lanes, chunk, cols), bf),
        ((n, xs, lanes, chunk, cols), bf),
        ((n, lanes, chunk, cols), f32),
        ((n, xs, lanes, chunk, cols), bf),
        ((n, xs, lanes, chunk, cols), bf),
        ((bits, n, lanes // 2, chunk, cols), f32),
        ((n, lanes - 1, chunk, cols), bf),
        ((n, lanes - 1, chunk, cols), bf),
    ]
    size = 0
    for shape, kind in shapes:
        count = 1
        for extent in shape:
            count *= extent
        size += count * jnp.dtype(kind).itemsize
    if size > VMEM_LIMIT * 3 // 4:
        return None
    sems = [(lanes,), (lanes,), (n,), (3,), (3, lanes), (3, lanes), (3, n), (9,)]
    sems += [(PIECES,), (PIECES,), (PIECES, xs), (PIECES, xs)]
    sems += [(bits, lanes), (xs, lanes), (lanes, xs), (lanes, nt)]
    sems += [(n,), (n,), (n, xs), (n, xs), (n, bits), (n, bits), (n, xs), (n, xs), (n, nt)]
    return wide, [pltpu.VMEM(*s) for s in shapes] + [pltpu.SemaphoreType.DMA(s) for s in sems]


def fused_layer(
    n, nt, plan, tokens_in, queries, keys, values, doc_ids, query_gain, key_norm_scale,
    out_weight, norm_gain, gate_weight, up_weight, down_weight,
):
    wide, scratch = plan
    rows, width = tokens_in.shape
    head_dim = query_gain.shape[0]
    places = lax.axis_index("sp") * rows + jnp.arange(rows, dtype=jnp.int32)
    half = head_dim // 2
    freqs = THETA ** (-2.0 * jnp.arange(half // 2, dtype=jnp.float32) / half)
    angles = [
        freqs[:, None] * spot.astype(jnp.float32)[None, :] for spot in (places // GRID, places % GRID)
    ]
    table = jnp.concatenate([f(a) for a in angles for f in (jnp.cos, jnp.sin)], axis=0)
    hbm = pl.BlockSpec(memory_space=pl.ANY)
    out = pl.pallas_call(
        functools.partial(fused_kernel, n, nt, wide),
        out_shape=jax.ShapeDtypeStruct((nt, rows // nt, width), jnp.bfloat16),
        in_specs=[hbm] * 12 + [VM],
        out_specs=VM,
        scratch_shapes=scratch,
        compiler_params=pltpu.CompilerParams(
            collective_id=3, has_side_effects=True, vmem_limit_bytes=VMEM_LIMIT
        ),
        name="fused_layer",
    )(
        queries, keys.T, values.T, doc_ids.reshape(1, rows), query_gain.reshape(1, head_dim),
        key_norm_scale.reshape(1, head_dim), norm_gain.reshape(1, width), tokens_in, out_weight,
        gate_weight, up_weight, down_weight, table,
    )
    return out.reshape(rows, width)


def per_device(
    n,
    nt,
    tokens_in,
    queries,
    keys,
    values,
    doc_ids,
    query_gain,
    key_norm_scale,
    out_weight,
    norm_gain,
    gate_weight,
    up_weight,
    down_weight,
):
    tok_rows = tokens_in.shape[0]
    head_dim = query_gain.shape[0]
    local_heads = queries.shape[1] // head_dim
    plan = None
    if keys.shape[1] == head_dim:
        plan = fused_plan(
            n, nt, tok_rows, tokens_in.shape[1], head_dim, local_heads, gate_weight.shape[1]
        )
    if plan is not None:
        return fused_layer(
            n, nt, plan, tokens_in, queries, keys, values, doc_ids, query_gain, key_norm_scale,
            out_weight, norm_gain, gate_weight, up_weight, down_weight,
        )
    places = lax.axis_index("sp") * tok_rows + jnp.arange(tok_rows, dtype=jnp.int32)
    lattice_row = (places // GRID).astype(jnp.float32)
    lattice_column = (places % GRID).astype(jnp.float32)
    q_local = normalized_rotated(queries, query_gain, local_heads, lattice_row, lattice_column)
    q_rows = q_local.transpose(1, 0, 2).reshape(local_heads * tok_rows, head_dim)
    lanes = [[2 * j + side for j in range(n // 2)] for side in range(2)]
    gate_up_all = lax.all_gather(
        pair_share(n, [gate_weight, up_weight], 1, 0), "sp", axis_index_groups=lanes, axis=0, tiled=True
    )
    down_all = lax.all_gather(
        pair_share(n, [down_weight], 0, 1), "sp", axis_index_groups=lanes, axis=1, tiled=True
    )
    turned = normalized_rotated(keys, key_norm_scale, 1, lattice_row, lattice_column)
    packed = jnp.concatenate([turned.reshape(tok_rows, head_dim), values], axis=1)
    kv_all, doc_all = gather_sp(n, packed, doc_ids.reshape(1, tok_rows))
    row_docs = jnp.tile(doc_ids, local_heads)
    first_doc = doc_ids[0]
    last_doc = doc_ids[-1]
    scale = head_dim ** (-0.5)
    total_rows = local_heads * tok_rows

    def absorb_block(state, key_block, value_block, doc_block):

        def absorb(current):
            running_max, running_sum, running_acc = current
            scores = (
                jnp.einsum("qd,kd->qk", q_rows, key_block, preferred_element_type=jnp.float32)
                * scale
            )
            same = row_docs[:, None] == doc_block[None, :]
            scores = jnp.where(same, scores, NEG)
            new_max = jnp.maximum(running_max, jnp.max(scores, axis=1))
            weights = jnp.where(same, jnp.exp(scores - new_max[:, None]), 0.0)
            shrink = jnp.exp(running_max - new_max)
            new_sum = running_sum * shrink + jnp.sum(weights, axis=1)
            new_acc = running_acc * shrink[:, None] + jnp.dot(
                weights.astype(jnp.bfloat16), value_block, preferred_element_type=jnp.float32
            )
            return (new_max, new_sum, new_acc)

        touches = (doc_block[0] <= last_doc) & (doc_block[-1] >= first_doc)
        return lax.cond(touches, absorb, lambda current: current, state)

    initial = (
        jnp.full((total_rows,), NEG, jnp.float32),
        jnp.zeros((total_rows,), jnp.float32),
        jnp.zeros((total_rows, head_dim), jnp.float32),
    )
    carry = initial
    shards = n
    joined = 1
    while joined * 2 <= shards and shards % (joined * 2) == 0 and (joined * 2 * tok_rows <= 1024):
        joined = joined * 2
    blocks = shards // joined
    span_rows = joined * tok_rows
    key_blocks = kv_all[..., :head_dim].reshape(blocks, span_rows, head_dim)
    value_blocks = kv_all[..., head_dim:].reshape(blocks, span_rows, head_dim)
    doc_blocks = doc_all.reshape(blocks, span_rows)

    def visit(state, inputs):
        key_block, value_block, doc_block = inputs
        return (absorb_block(state, key_block, value_block, doc_block), None)

    carry, unused = lax.scan(visit, carry, (key_blocks, value_blocks, doc_blocks))
    attended = (carry[2] / carry[1][:, None]).astype(jnp.bfloat16)
    attended = (
        attended.reshape(local_heads, tok_rows, head_dim)
        .transpose(1, 0, 2)
        .reshape(tok_rows, local_heads * head_dim)
    )
    partial_value = jnp.dot(attended, out_weight, preferred_element_type=jnp.float32)
    normed, resid = mid_stage(nt, partial_value.astype(jnp.bfloat16), tokens_in, norm_gain)
    normed = normed.reshape(2 * tok_rows, -1)
    both = jnp.dot(normed, gate_up_all, preferred_element_type=jnp.float32)
    units = both.shape[1] // 2
    hidden = (jax.nn.silu(both[:, :units]) * both[:, units:]).astype(jnp.bfloat16)
    fed_part = jnp.dot(hidden, down_all, preferred_element_type=jnp.float32)
    out = last_stage(nt, fed_part.astype(jnp.bfloat16), resid)
    return out.reshape(tok_rows, -1)


def solution(mesh):
    return jax.shard_map(
        functools.partial(per_device, mesh.shape["sp"], mesh.shape["tp"]),
        mesh=mesh,
        in_specs=(
            P("sp", None),
            P("sp", "tp"),
            P("sp", "tp"),
            P("sp", "tp"),
            P("sp"),
            P(),
            P(),
            P("tp", None),
            P(),
            P("sp", "tp"),
            P("sp", "tp"),
            P("tp", "sp"),
        ),
        out_specs=P("sp", None),
        check_vma=False,
    )
```

```python
import functools

import jax
import jax.numpy as jnp
from jax import lax
from jax.experimental import pallas as pl
from jax.experimental.pallas import tpu as pltpu
from jax.sharding import PartitionSpec as P

GRID = 64


EPS = 1e-06
THETA = 10000.0
NEG = -1e30


def rotate_half(block, angle):
    half_dim = block.shape[-1] // 2
    cosine = jnp.cos(angle)[:, None, :]
    sine = jnp.sin(angle)[:, None, :]
    first = block[..., :half_dim]
    second = block[..., half_dim:]
    return jnp.concatenate(
        [first * cosine - second * sine, second * cosine + first * sine], axis=-1
    )


def normalized_rotated(values_in, gain, heads, lattice_row, lattice_column):
    full = values_in.astype(jnp.float32).reshape(values_in.shape[0], heads, -1)
    full = full * lax.rsqrt(jnp.mean(full * full, axis=-1, keepdims=True) + EPS) * gain
    half_dim = full.shape[-1] // 2
    freqs = THETA ** (-2.0 * jnp.arange(half_dim // 2, dtype=jnp.float32) / half_dim)
    by_row = rotate_half(full[..., :half_dim], lattice_row[:, None] * freqs[None, :])
    by_col = rotate_half(full[..., half_dim:], lattice_column[:, None] * freqs[None, :])
    return jnp.concatenate([by_row, by_col], axis=-1).astype(jnp.bfloat16)


MESH = pl.DeviceIdType.MESH
VM = pl.BlockSpec(memory_space=pltpu.VMEM)


def params(cid):
    return pltpu.CompilerParams(
        collective_id=cid, has_side_effects=True, vmem_limit_bytes=56 * 1024 * 1024
    )


def greet(count, where):
    barrier = pltpu.get_barrier_semaphore()

    @pl.loop(1, count)
    def _(step):
        pl.semaphore_signal(barrier, inc=1, device_id=where(step), device_id_type=MESH)

    pl.semaphore_wait(barrier, count - 1)


def gather_kernel(n, kv_ref, doc_ref, kv_out, doc_out, send, recv, doc_send, doc_recv):
    me = lax.axis_index("sp")

    def where(step):
        return {"sp": lax.rem(me + step, n)}

    def copies(step, slot):
        return (
            pltpu.make_async_remote_copy(
                kv_ref, kv_out.at[slot], send.at[step], recv.at[step], where(step), MESH
            ),
            pltpu.make_async_remote_copy(
                doc_ref, doc_out.at[slot], doc_send.at[step], doc_recv.at[step], where(step), MESH
            ),
        )

    greet(n, where)

    @pl.loop(1, n)
    def _(step):
        for copy in copies(step, me):
            copy.start()

    kv_out[me] = kv_ref[...]
    doc_out[me] = doc_ref[...]

    @pl.loop(1, n)
    def _(step):
        for copy in copies(step, lax.rem(me + n - step, n)):
            copy.wait_recv()
            copy.wait_send()


def gather_sp(n, packed, docs):
    return pl.pallas_call(
        functools.partial(gather_kernel, n),
        out_shape=(
            jax.ShapeDtypeStruct((n,) + packed.shape, packed.dtype),
            jax.ShapeDtypeStruct((n,) + docs.shape, docs.dtype),
        ),
        in_specs=[VM, VM],
        out_specs=(VM, VM),
        scratch_shapes=[pltpu.SemaphoreType.DMA((n,))] * 4,
        compiler_params=params(0),
        name="gather_sp",
    )(packed, docs)


def mid_kernel(
    nt, partial_ref, tokens_ref, gain_ref, normed_out, resid_out, landing, send, recv, send2, recv2
):
    sp, tp = lax.axis_index("sp"), lax.axis_index("tp")
    side = lax.rem(sp, 2)
    base = sp - side
    group = 2 * nt
    me = side * nt + tp
    rows = resid_out.shape[0]

    def where(step):
        other = lax.rem(me + step, group)
        return {"sp": base + other // nt, "tp": lax.rem(other, nt)}

    def part(step):
        peer = lax.rem(tp + step, nt)
        return pltpu.make_async_remote_copy(
            partial_ref.at[peer],
            landing.at[step],
            send.at[step],
            recv.at[step],
            {"sp": sp, "tp": peer},
            MESH,
        )

    def spread(step, slot):
        return pltpu.make_async_remote_copy(
            normed_out.at[slot], normed_out.at[slot], send2.at[step], recv2.at[step], where(step), MESH
        )

    greet(group, where)
    for step in range(1, nt):
        part(step).start()
    for step in range(1, nt):
        part(step).wait_recv()
    chunk = 16

    @pl.loop(0, rows // chunk)
    def _(i):
        at = pl.ds(pl.multiple_of(i * chunk, chunk), chunk)
        mixed = partial_ref[tp, at].astype(jnp.float32)
        for step in range(1, nt):
            mixed = mixed + landing[step, at].astype(jnp.float32)
        resid = tokens_ref[tp, at].astype(jnp.float32) + mixed
        resid_out[at] = resid
        power = jnp.mean(resid * resid, axis=-1, keepdims=True)
        normed_out[me, at] = (resid * lax.rsqrt(power + EPS) * gain_ref[...]).astype(jnp.bfloat16)

    for step in range(1, group):
        spread(step, me).start()
    for step in range(1, group):
        copy = spread(step, lax.rem(me + group - step, group))
        copy.wait_recv()
        copy.wait_send()
    for step in range(1, nt):
        part(step).wait_send()


def mid_stage(nt, part, tokens, gain):
    rows, width = part.shape[0] // nt, part.shape[1]
    return pl.pallas_call(
        functools.partial(mid_kernel, nt),
        out_shape=(
            jax.ShapeDtypeStruct((2 * nt, rows, width), jnp.bfloat16),
            jax.ShapeDtypeStruct((rows, width), jnp.float32),
        ),
        in_specs=[VM, VM, VM],
        out_specs=(VM, VM),
        scratch_shapes=[pltpu.VMEM((nt, rows, width), jnp.bfloat16)]
        + [pltpu.SemaphoreType.DMA((nt,))] * 2
        + [pltpu.SemaphoreType.DMA((2 * nt,))] * 2,
        compiler_params=params(1),
        name="mid_stage",
    )(part.reshape(nt, rows, width), tokens.reshape(nt, rows, width), gain.reshape(1, width))


def last_kernel(nt, fed_ref, resid_ref, out_ref, landing, send, recv, send2, recv2):
    sp, tp = lax.axis_index("sp"), lax.axis_index("tp")
    side = lax.rem(sp, 2)
    base = sp - side
    group = 2 * nt
    me = side * nt + tp
    rows = resid_ref.shape[0]

    def where(step):
        other = lax.rem(me + step, group)
        return {"sp": base + other // nt, "tp": lax.rem(other, nt)}

    def part(step):
        return pltpu.make_async_remote_copy(
            fed_ref.at[lax.rem(me + step, group)],
            landing.at[step],
            send.at[step],
            recv.at[step],
            where(step),
            MESH,
        )

    def spread(step, slot):
        return pltpu.make_async_remote_copy(
            out_ref.at[slot],
            out_ref.at[slot],
            send2.at[step],
            recv2.at[step],
            {"sp": sp, "tp": lax.rem(tp + step, nt)},
            MESH,
        )

    greet(group, where)
    for step in range(1, group):
        part(step).start()
    for step in range(1, group):
        part(step).wait_recv()
    chunk = 16

    @pl.loop(0, rows // chunk)
    def _(i):
        at = pl.ds(pl.multiple_of(i * chunk, chunk), chunk)
        fed = fed_ref[me, at].astype(jnp.float32)
        for step in range(1, group):
            fed = fed + landing[step, at].astype(jnp.float32)
        out_ref[tp, at] = (resid_ref[at] + fed).astype(jnp.bfloat16)

    for step in range(1, nt):
        spread(step, tp).start()
    for step in range(1, nt):
        copy = spread(step, lax.rem(tp + nt - step, nt))
        copy.wait_recv()
        copy.wait_send()
    for step in range(1, group):
        part(step).wait_send()


def last_stage(nt, fed, resid):
    rows, width = resid.shape
    return pl.pallas_call(
        functools.partial(last_kernel, nt),
        out_shape=jax.ShapeDtypeStruct((nt, rows, width), jnp.bfloat16),
        in_specs=[VM, VM],
        out_specs=VM,
        scratch_shapes=[pltpu.VMEM((2 * nt, rows, width), jnp.bfloat16)]
        + [pltpu.SemaphoreType.DMA((2 * nt,))] * 2
        + [pltpu.SemaphoreType.DMA((nt,))] * 2,
        compiler_params=params(2),
        name="last_stage",
    )(fed.reshape(2 * nt, rows, width), resid)


def pair_share(n, arrays, axis, joins):
    side = lax.rem(lax.axis_index("sp"), 2)
    own, away = [], []
    for array in arrays:
        half = array.shape[axis] // 2
        own.append(lax.dynamic_slice_in_dim(array, side * half, half, axis))
        away.append(lax.dynamic_slice_in_dim(array, (1 - side) * half, half, axis))
    own = jnp.concatenate(own, axis=axis)
    away = jnp.concatenate(away, axis=axis)
    came = lax.ppermute(away, "sp", [(i, i ^ 1) for i in range(n)])
    first = jnp.where(side == 0, own, came)
    second = jnp.where(side == 0, came, own)
    return jnp.concatenate([first, second], axis=joins)


SIDES = 2
LANE = 128
PIECES = 4
GATHERED = 2


def turned(block, gain, table):
    power = jnp.mean(block * block, axis=0, keepdims=True)
    full = block * lax.rsqrt(power + EPS) * gain
    half = block.shape[0] // 2
    quarter = half // 2
    pieces = []
    for part in range(2):
        first = full[part * half : part * half + quarter]
        second = full[part * half + quarter : (part + 1) * half]
        cosine = table[2 * part * quarter : (2 * part + 1) * quarter]
        sine = table[(2 * part + 1) * quarter : (2 * part + 2) * quarter]
        pieces += [first * cosine - second * sine, second * cosine + first * sine]
    return jnp.concatenate(pieces, axis=0)


def identity(size):
    down = lax.broadcasted_iota(jnp.int32, (size, size), 0)
    across = lax.broadcasted_iota(jnp.int32, (size, size), 1)
    return (down == across).astype(jnp.bfloat16)


def flipped(array):
    return lax.dot_general(
        identity(array.shape[1]), array, (((1,), (1,)), ((), ())), preferred_element_type=jnp.float32
    )


def upright_row(row):
    size = row.shape[1]
    down = lax.broadcasted_iota(jnp.int32, (size, size), 0)
    across = lax.broadcasted_iota(jnp.int32, (size, size), 1)
    return jnp.sum(jnp.where(down == across, row, 0.0), axis=1, keepdims=True)


def fused_kernel(
    n,
    nt,
    wide,
    q_in,
    k_in,
    v_in,
    doc_in,
    q_gain_in,
    k_gain_in,
    norm_gain_in,
    tokens,
    out_weight,
    gate,
    up,
    down,
    table_ref,
    out,
    q_raw,
    k_raw,
    doc_ref,
    q_gain_ref,
    k_gain_ref,
    norm_gain,
    kv,
    q_ref,
    top,
    total,
    acc,
    part,
    part_in,
    px_out,
    px_in,
    ow,
    ow_all,
    att_out,
    att,
    tok,
    resid,
    act,
    gw,
    uw,
    dw,
    gated,
    hid,
    keep,
    core_out,
    core_in,
    x_keep,
    x_out,
    x_in,
    z_keep,
    z_out,
    z_in,
    kv_zs,
    kv_ys,
    kv_r,
    w_own,
    w_zs,
    w_ys,
    w_r,
    misc,
    pc_s,
    pc_r,
    px_s,
    px_r,
    ow_xs,
    ow_cs,
    ow_r,
    att_s,
    att_r,
    act_zs,
    act_xs,
    act_cs,
    act_r,
    rs_cs,
    rs_cr,
    rs_xs,
    rs_xr,
    rs_zs,
    rs_zr,
    ag_xs,
    ag_cs,
    ag_r,
):
    sp, tp = lax.axis_index("sp"), lax.axis_index("tp")
    lanes, xs = n // SIDES, nt // 2
    bits = lanes.bit_length() - 1
    lane, side = sp // SIDES, sp % SIDES
    xi, core = tp // 2, tp % 2
    rows = q_in.shape[0]
    head_dim = k_in.shape[0]
    heads = q_in.shape[1] // head_dim
    chunk = rows // nt
    blocks = gate.shape[1] // LANE
    width = wide * LANE
    last = blocks - (lanes - 1) * wide
    kv_docs = head_dim
    table = table_ref[...]

    def at_sp(lane_to, side_to):
        return {"sp": lane_to * SIDES + side_to, "tp": tp}

    def at_tp(x_to, core_to):
        return {"sp": sp, "tp": x_to * 2 + core_to}

    def remote(src, dst, send, recv, where):
        return pltpu.make_async_remote_copy(src, dst, send, recv, where, MESH)

    def lane_at(d):
        return (lane + d) % lanes

    def x_at(d):
        return (xi + d) % xs

    def bit_of(value, b):
        return (value // (1 << b)) % 2

    def partner(b):
        return lane + (1 - 2 * bit_of(lane, b)) * (1 << b)

    def mate(e):
        return lane + sum((e >> b) % 2 * (1 - 2 * bit_of(lane, b)) * (1 << b) for b in range(bits))

    def mated(i):
        total_of = 0
        for b in range(bits):
            total_of = total_of + (bit_of(lane, b) + bit_of(i, b)) % 2 * (1 << b)
        return total_of

    def low_bit(e):
        return (e & -e).bit_length() - 1

    other_side = 1 - side
    other_core = 1 - core

    barrier = pltpu.get_barrier_semaphore()
    for d in range(1, lanes):
        pl.semaphore_signal(barrier, inc=1, device_id=at_sp(lane_at(d), side), device_id_type=MESH)
    pl.semaphore_signal(barrier, inc=1, device_id=at_sp(lane, other_side), device_id_type=MESH)
    for d in range(1, nt):
        pl.semaphore_signal(
            barrier, inc=1, device_id={"sp": sp, "tp": (tp + d) % nt}, device_id_type=MESH
        )

    def rank(lane_to):
        return lane_to + core * (lanes - 1 - 2 * lane_to)

    def sized(lane_to, action):
        if last == wide:
            action(width)
            return
        few = rank(lane_to) // (lanes - 1)

        @pl.when(few == 1)
        def _():
            action(last * LANE)

        @pl.when(few == 0)
        def _():
            action(width)

    def weight_block(m, lane_to, size):
        at = pl.ds(pl.multiple_of(rank(lane_to) * width, LANE), size)
        if m == 0:
            return gate.at[:, at]
        if m == 1:
            return up.at[:, at]
        return down.at[at, :]

    def landing(m, slot, size):
        if m == 0:
            return gw.at[slot, :, 0:size]
        if m == 1:
            return uw.at[slot, :, 0:size]
        return dw.at[slot, 0:size, :]

    def w_local(m, size):
        return pltpu.make_async_copy(weight_block(m, lane, size), landing(m, sp, size), w_own.at[m])

    ow_copy = pltpu.make_async_copy(out_weight, ow, misc.at[0])
    tok_copy = pltpu.make_async_copy(
        tokens.at[pl.ds(pl.multiple_of(tp * chunk, chunk), chunk)], tok, misc.at[1]
    )
    kv_vals = kv.shape[1] - head_dim
    small = [
        pltpu.make_async_copy(k_in, k_raw, misc.at[2]),
        pltpu.make_async_copy(doc_in, doc_ref, misc.at[3]),
        pltpu.make_async_copy(k_gain_in, k_gain_ref, misc.at[4]),
        pltpu.make_async_copy(v_in, kv.at[sp, kv_vals:, :], misc.at[5]),
        pltpu.make_async_copy(q_in, q_raw, misc.at[6]),
        pltpu.make_async_copy(q_gain_in, q_gain_ref, misc.at[7]),
        pltpu.make_async_copy(norm_gain_in, norm_gain, misc.at[8]),
    ]
    for copy in small:
        copy.start()
    for m in range(3):
        sized(lane, lambda size, m=m: w_local(m, size).start())
    ow_copy.start()
    tok_copy.start()

    for copy in small[:4]:
        copy.wait()
    k_full = turned(k_raw[...].astype(jnp.float32), upright_row(k_gain_ref[...]), table)
    kv[sp, 0:head_dim, :] = k_full.astype(jnp.bfloat16)
    q_doc = doc_ref[...].astype(jnp.float32)
    kv[sp, kv_docs:kv_vals, :] = jnp.broadcast_to(q_doc, (kv_vals - kv_docs, rows)).astype(jnp.bfloat16)

    pl.semaphore_wait(barrier, lanes - 1 + 1 + nt - 1)

    def kv_z(e, lane_of):
        slot = lane_of * SIDES + side
        return remote(kv.at[slot], kv.at[slot], kv_zs.at[e], kv_r.at[slot], at_sp(mate(e), side))

    def kv_y(lane_of, side_of):
        slot = lane_of * SIDES + side_of
        return remote(
            kv.at[slot], kv.at[slot], kv_ys.at[lane_of], kv_r.at[slot], at_sp(lane, other_side)
        )

    for e in range(1, lanes):
        kv_z(e, lane).start()
    kv_y(lane, side).start()

    span = ow.shape[1] // PIECES
    gathered = GATHERED * span
    ow_here = out_weight.at[:, 0:gathered]

    def ow_x(d, slot):
        return remote(ow_here, ow_all.at[slot], ow_xs.at[d], ow_r.at[slot], at_tp(x_at(d), core))

    def ow_core(x_of, core_of):
        slot = x_of * 2 + core_of
        return remote(
            ow_all.at[slot], ow_all.at[slot], ow_cs.at[x_of], ow_r.at[slot], at_tp(xi, other_core)
        )

    for d in range(1, xs):
        ow_x(d, tp).start()
    remote(ow_here, ow_all.at[tp], ow_cs.at[xi], ow_r.at[tp], at_tp(xi, other_core)).start()

    def w_z(m, e, slot, lane_to, size):
        return remote(
            weight_block(m, lane_to, size),
            landing(m, slot, size),
            w_zs.at[m, e],
            w_r.at[m, slot],
            at_sp(mate(e), side),
        )

    def w_y(m, lane_of, side_of, size):
        slot = lane_of * SIDES + side_of
        return remote(
            landing(m, slot, size),
            landing(m, slot, size),
            w_ys.at[m, lane_of],
            w_r.at[m, slot],
            at_sp(lane, other_side),
        )

    def send_weight(m, e):
        lane_to = mate(e)
        sized(lane_to, lambda size: w_z(m, e, sp, lane_to, size).start())

    def share_weight(m):
        def own(size):
            w_local(m, size).wait()
            w_y(m, lane, side, size).start()

        sized(lane, own)

    def forward_weight(m, lane_of):
        sized(lane, lambda size: w_z(m, 1, lane_of * SIDES + side, lane, size).wait_recv())
        sized(lane, lambda size: w_y(m, lane_of, side, size).start())

    def w_shared(m, lane_of):
        sized(lane, lambda size: w_y(m, lane_of, other_side, size).wait_recv())

    for e in range(1, lanes):
        send_weight(0, e)
    share_weight(0)

    scale = head_dim ** (-0.5)
    for copy in small[4:]:
        copy.wait()
    standing_q = flipped(q_raw[...])
    q_gain = upright_row(q_gain_ref[...])
    for h in range(heads):
        at = slice(h * head_dim, (h + 1) * head_dim)
        query = turned(standing_q[at, :], q_gain, table)
        q_ref[at, :] = (query.astype(jnp.bfloat16).astype(jnp.float32) * scale).astype(jnp.bfloat16)
    top[...] = jnp.full(top.shape, NEG, jnp.float32)
    total[...] = jnp.zeros(total.shape, jnp.float32)
    acc[...] = jnp.zeros(acc.shape, jnp.float32)

    def absorb(slot):
        upright = lax.dot_general(
            identity(rows),
            kv[slot, 0:kv_vals, :],
            (((1,), (1,)), ((), ())),
            preferred_element_type=jnp.float32,
        )
        key = upright[:, 0:head_dim].astype(jnp.bfloat16)
        same = upright[:, head_dim : head_dim + 1] == q_doc
        value = kv[slot, kv_vals:, :]
        for h in range(heads):
            at = slice(h * head_dim, (h + 1) * head_dim)
            scores = jnp.dot(key, q_ref[at, :], preferred_element_type=jnp.float32)
            scores = jnp.where(same, scores, NEG)
            before = top[h]
            now = jnp.maximum(before, jnp.max(scores, axis=0, keepdims=True))
            weights = jnp.exp(scores - now)
            shrink = jnp.exp(before - now)
            top[h] = now
            total[h] = total[h] * shrink + jnp.sum(weights, axis=0, keepdims=True)
            acc[at, :] = acc[at, :] * shrink + jnp.dot(
                value, weights.astype(jnp.bfloat16), preferred_element_type=jnp.float32
            )

    @pl.loop(0, SIDES)
    def _(k):
        side_of = (side + k) % SIDES

        @pl.when(k > 0)
        def _():
            kv_y(lane, other_side).wait_recv()

        absorb(lane * SIDES + side_of)

    @pl.loop(0, SIDES * (lanes - 1))
    def _(k):
        lane_of = mated(k % (lanes - 1) + 1)
        side_of = (side + k // (lanes - 1)) % SIDES
        slot = lane_of * SIDES + side_of

        @pl.when(k < lanes - 1)
        def _():
            kv_z(1, lane_of).wait_recv()
            kv_y(lane_of, side).start()

        @pl.when(k >= lanes - 1)
        def _():
            kv_y(lane_of, other_side).wait_recv()

        absorb(slot)

    send_weight(1, 1)
    share_weight(1)
    pieces = []
    for h in range(heads):
        at = slice(h * head_dim, (h + 1) * head_dim)
        pieces.append((acc[at, :] / total[h]).astype(jnp.bfloat16))
    attended = flipped(jnp.concatenate(pieces, axis=0)).astype(jnp.bfloat16)

    def att_copy(d, peer, slot):
        return remote(
            att_out.at[peer], att.at[slot], att_s.at[d], att_r.at[slot], {"sp": sp, "tp": peer}
        )

    for i in range(nt):
        att_out[i] = attended[i * chunk : (i + 1) * chunk]
    for d in range(1, nt):
        att_copy(d, (tp + d) % nt, tp).start()

    def part_core(p):
        return remote(part.at[p, other_core], part_in.at[p], pc_s.at[p], pc_r.at[p], at_tp(xi, other_core))

    def part_x(p, d):
        return remote(px_out.at[p, d], px_in.at[p, d], px_s.at[p, d], px_r.at[p, d], at_tp(x_at(d), core))

    ow_copy.wait()
    for p in range(GATHERED, PIECES):
        product = jnp.dot(
            attended, ow[:, p * span : (p + 1) * span], preferred_element_type=jnp.float32
        ).astype(jnp.bfloat16)
        for x_of in range(xs):
            for core_of in range(2):
                start = (x_of * 2 + core_of) * chunk
                part[p, core_of, x_of] = product[start : start + chunk]
        part_core(p).start()
    for d in range(1, xs):
        x_of = x_at(xs - d)
        ow_x(d, x_of * 2 + core).wait_recv()
        ow_core(x_of, core).start()
    tok_copy.wait()
    early = slice(0, gathered)

    def project(rows_of, weight):
        product = jnp.dot(rows_of, weight, preferred_element_type=jnp.float32)
        return product.astype(jnp.bfloat16).astype(jnp.float32)

    resid[:, early] = tok[:, early].astype(jnp.float32) + project(att_out[tp], ow[:, early])
    for p in range(GATHERED, PIECES):
        at = slice(p * span, (p + 1) * span)
        part_core(p).wait_recv()
        for d in range(1, xs):
            x_to = x_at(d)
            px_out[p, d] = (
                part[p, core, x_to].astype(jnp.float32) + part_in[p, x_to].astype(jnp.float32)
            ).astype(jnp.bfloat16)
            part_x(p, d).start()
        resid[:, at] = (
            tok[:, at].astype(jnp.float32)
            + part[p, core, xi].astype(jnp.float32)
            + part_in[p, xi].astype(jnp.float32)
        )

    def add_rows(slot):
        att_copy(1, tp, slot).wait_recv()
        resid[:, early] += project(att[slot], ow_all[slot])

    ow_core(xi, other_core).wait_recv()
    add_rows(xi * 2 + other_core)
    for d in range(1, xs):
        add_rows(x_at(xs - d) * 2 + core)
    for d in range(1, xs):
        ow_core(x_at(xs - d), other_core).wait_recv()
        add_rows(x_at(xs - d) * 2 + other_core)
    for p in range(GATHERED, PIECES):
        at = slice(p * span, (p + 1) * span)
        for d in range(1, xs):
            part_x(p, d).wait_recv()
            resid[:, at] += px_in[p, d].astype(jnp.float32)

    whole = resid[...]
    power = jnp.mean(whole * whole, axis=-1, keepdims=True)
    act[lane, tp] = (whole * lax.rsqrt(power + EPS) * norm_gain[...]).astype(jnp.bfloat16)

    def act_z(b, lane_of):
        return remote(
            act.at[lane_of, tp],
            act.at[lane_of, tp],
            act_zs.at[b, lane_of],
            act_r.at[lane_of, tp],
            at_sp(partner(b), side),
        )

    def act_x(d, lane_of, slot):
        return remote(
            act.at[lane_of, slot],
            act.at[lane_of, slot],
            act_xs.at[d, lane_of],
            act_r.at[lane_of, slot],
            at_tp(x_at(d), core),
        )

    def act_core(lane_of, x_of, core_of):
        slot = x_of * 2 + core_of
        return remote(
            act.at[lane_of, slot],
            act.at[lane_of, slot],
            act_cs.at[lane_of, x_of],
            act_r.at[lane_of, slot],
            at_tp(xi, other_core),
        )

    def act_out(lane_of):
        for d in range(1, xs):
            act_x(d, lane_of, tp).start()
        act_core(lane_of, xi, core).start()

    def act_from_x(lane_of):
        for d in range(1, xs):
            x_of = x_at(xs - d)
            act_x(d, lane_of, x_of * 2 + core).wait_recv()
            act_core(lane_of, x_of, core).start()

    def act_arrived(e):
        step = low_bit(e)
        act_z(step, mate(e)).wait_recv()
        for lower in reversed(range(step)):
            act_z(lower, mate(e)).start()
        act_out(mate(e))

    for b in reversed(range(bits)):
        act_z(b, lane).start()
    act_out(lane)
    for e in range(2, lanes - 1):
        send_weight(1, e)
    for e in range(1, lanes):
        forward_weight(0, mate(e))
    act_from_x(lane)
    for e in range(1, lanes - 1):
        act_arrived(e)
    send_weight(1, lanes - 1)
    share_weight(2)
    forward_weight(1, mate(1))

    few_here = rank(lane) // (lanes - 1)
    unit = lax.broadcasted_iota(jnp.int32, (nt * chunk, width), 1)
    mine = unit < (wide - few_here * (wide - last)) * LANE
    if last < wide:

        @pl.when(few_here == 1)
        def _():
            dw[:, last * LANE :, :] = jnp.zeros((n, width - last * LANE, dw.shape[2]), dw.dtype)

    def depth(ref):
        return ref[...].reshape(ref.shape[0] * ref.shape[1], ref.shape[2])

    for d in range(lanes):
        w_shared(0, lane_at(d))

    @pl.loop(0, lanes)
    def _(i):
        lane_of = mated(i)
        for e in range(1, lanes):

            @pl.when(i == e)
            def _(e=e):
                if e == lanes - 2:
                    act_arrived(e + 1)
                    for f in range(1, lanes):
                        send_weight(2, f)
                if e > 1:
                    forward_weight(1, mate(e))
                act_from_x(mate(e))

        for x_of in range(xs):
            act_core(lane_of, x_of, other_core).wait_recv()
        inputs = act[lane_of].reshape(nt * chunk, act.shape[-1])
        gated[lane_of] = jnp.dot(inputs, depth(gw), preferred_element_type=jnp.float32)

    for d in range(lanes):
        w_shared(1, lane_at(d))

    @pl.loop(0, lanes)
    def _(lane_of):
        inputs = act[lane_of].reshape(nt * chunk, act.shape[-1])
        lifted = jnp.dot(inputs, depth(uw), preferred_element_type=jnp.float32)
        gates = gated[lane_of]
        hidden = jnp.where(mine, gates * lax.logistic(gates) * lifted, 0.0).astype(jnp.bfloat16)
        for x_of in range(xs):
            for core_of in range(2):
                start = (x_of * 2 + core_of) * chunk
                hid[core_of, x_of, lane_of] = hidden[start : start + chunk]

    forward_weight(2, mate(1))

    cols = dw.shape[2]
    share = xs * lanes * chunk
    starts = [lanes - (lanes >> b) for b in range(bits)]

    def rs_core(s):
        return remote(core_out.at[s], core_in.at[s], rs_cs.at[s], rs_cr.at[s], at_tp(xi, other_core))

    def rs_x(s, d):
        return remote(x_out.at[s, d], x_in.at[s, d], rs_xs.at[s, d], rs_xr.at[s, d], at_tp(x_at(d), core))

    def rs_z(s, b):
        piece = pl.ds(starts[b], lanes >> (b + 1))
        return remote(
            z_out.at[s, piece], z_in.at[s, piece], rs_zs.at[s, b], rs_zr.at[s, b], at_sp(partner(b), side)
        )

    def columns(s):
        return pl.ds(pl.multiple_of(s * cols, cols), cols)

    def ag_x(s, d, slot):
        piece = out.at[slot, :, columns(s)]
        return remote(piece, piece, ag_xs.at[s, d], ag_r.at[s, slot], at_tp(x_at(d), core))

    def ag_core(s, x_of, core_of):
        slot = x_of * 2 + core_of
        piece = out.at[slot, :, columns(s)]
        return remote(piece, piece, ag_cs.at[s, x_of], ag_r.at[s, slot], at_tp(xi, other_core))

    def lane_in_order(j):
        return lanes // 2 + (1 - 2 * (j % 2)) * (j // 2) - j % 2

    def slot_of(k):
        return lane_in_order(k % lanes) * SIDES + (side + k // lanes) % SIDES

    upper = lane // (lanes // 2)
    own_turn = upper * (2 * lane - lanes) + (1 - upper) * (lanes - 1 - 2 * lane)

    def early_slot(k):
        own = (n - 1 - k) // (n - SIDES)
        p = (k - SIDES) % (lanes - 1) + 1
        lane_of = lane_in_order(p - 1 + (p - own_turn + lanes - 1) // lanes)
        side_of = (1 - own) * ((k - SIDES) // (lanes - 1)) + own * k
        return (own * lane + (1 - own) * lane_of) * SIDES + (side + side_of) % SIDES

    def multiply(k):
        s = early_slot(k)
        lane_of = s // SIDES

        @pl.when((k > 1) & (k <= lanes) & (lane_of != mate(1)))
        def _():
            forward_weight(2, lane_of)

        @pl.when((k == 1) | (k > lanes))
        def _():
            w_shared(2, lane_of)

        away = hid[other_core].reshape(share, width)
        core_out[s] = (
            jnp.dot(away, dw[s], preferred_element_type=jnp.float32)
            .astype(jnp.bfloat16)
            .reshape(xs, lanes, chunk, cols)
        )
        rs_core(s).start()
        near = hid[core].reshape(share, width)
        keep[s] = jnp.dot(near, dw[s], preferred_element_type=jnp.float32).reshape(xs, lanes, chunk, cols)

    def reduce_core(k):
        s = early_slot(k)
        rs_core(s).wait_recv()
        for d in range(1, xs):
            x_to = x_at(d)
            x_out[s, d] = (keep[s, x_to] + core_in[s, x_to].astype(jnp.float32)).astype(jnp.bfloat16)
            rs_x(s, d).start()
        x_keep[s] = keep[s, xi] + core_in[s, xi].astype(jnp.float32)

    def reduce_lanes(b, k):
        s = slot_of(k)
        if b == 0:
            for d in range(1, xs):
                rs_x(s, d).wait_recv()
        else:
            rs_z(s, b - 1).wait_recv()

        def summed(h):
            if b == 0:
                value = x_keep[s, h]
                for d in range(1, xs):
                    value = value + x_in[s, d, h].astype(jnp.float32)
                return value
            return z_keep[b - 1, s, h] + z_in[s, starts[b - 1] + h].astype(jnp.float32)

        if b == bits:
            out[tp, :, columns(s)] = (resid[:, columns(s)] + summed(0)).astype(jnp.bfloat16)
            for d in range(1, xs):
                ag_x(s, d, tp).start()
            ag_core(s, xi, core).start()
            return
        mine_here = bit_of(lane, b)
        count = lanes >> (b + 1)
        for h in range(count):
            z_out[s, starts[b] + h] = summed(1 - mine_here + 2 * h).astype(jnp.bfloat16)
        rs_z(s, b).start()
        for h in range(count):
            z_keep[b, s, h] = summed(mine_here + 2 * h)

    def spread(k):
        s = slot_of(k)
        for d in range(1, xs):
            x_of = x_at(xs - d)
            ag_x(s, d, x_of * 2 + core).wait_recv()
            ag_core(s, x_of, core).start()

    first, gap = 5, 3
    stages = [(0, multiply), (1, reduce_core)]
    for b in range(bits + 1):
        stages.append((first + gap * b, functools.partial(reduce_lanes, b)))

    @pl.loop(0, n + stages[-1][0])
    def _(k):
        for lag, action in [stages[1], stages[0]] + stages[:1:-1]:

            @pl.when((k >= lag) & (k < n + lag))
            def _(lag=lag, action=action):
                action(k - lag)

    pl.loop(0, n)(spread)

    @pl.loop(0, n)
    def _(s):
        for x_of in range(xs):
            ag_core(s, x_of, other_core).wait_recv()
            ag_core(s, x_of, core).wait_send()
        for d in range(1, xs):
            ag_x(s, d, tp).wait_send()
            rs_x(s, d).wait_send()
        rs_core(s).wait_send()
        for b in range(bits):
            rs_z(s, b).wait_send()

    for d in range(1, lanes):
        kv_z(d, lane).wait_send()
        for m in range(3):
            lane_to = mate(d)
            sized(lane_to, lambda size, m=m, d=d, lane_to=lane_to: w_z(m, d, sp, lane_to, size).wait_send())
    for lane_of in range(lanes):
        kv_y(lane_of, side).wait_send()
        for m in range(3):
            sized(lane, lambda size, m=m, lane_of=lane_of: w_y(m, lane_of, side, size).wait_send())
        for d in range(1, xs):
            act_x(d, lane_of, tp).wait_send()
        for x_of in range(xs):
            act_core(lane_of, x_of, core).wait_send()
    for b in range(bits):
        for h in range(lanes >> (b + 1)):
            lane_of = lane % (1 << (b + 1)) + h * (1 << (b + 1))
            act_z(b, lane_of).wait_send()
    for d in range(1, xs):
        ow_x(d, tp).wait_send()
    for x_of in range(xs):
        ow_core(x_of, core).wait_send()
    for d in range(1, nt):
        att_copy(d, (tp + d) % nt, tp).wait_send()
    for p in range(GATHERED, PIECES):
        part_core(p).wait_send()
        for d in range(1, xs):
            part_x(p, d).wait_send()


VMEM_LIMIT = 60 * 1024 * 1024


def fused_plan(n, nt, rows, width, head_dim, heads, units):
    if n % SIDES or n < 2 * SIDES or nt % 2 or nt < 4 or rows % nt or units % LANE:
        return None
    lanes, xs, chunk, blocks = n // SIDES, nt // 2, rows // nt, units // LANE
    wide = -(-blocks // lanes)
    cols = width // n
    if chunk % 16 or rows % LANE or width % (n * LANE) or width % (PIECES * LANE) or head_dim % 64:
        return None
    if lanes & (lanes - 1) or (lanes - 1) * wide >= blocks:
        return None
    wu = wide * LANE
    bits = lanes.bit_length() - 1
    span = width // PIECES
    bf, f32 = jnp.bfloat16, jnp.float32
    shapes = [
        ((rows, heads * head_dim), bf),
        ((head_dim, rows), bf),
        ((1, rows), jnp.int32),
        ((1, head_dim), f32),
        ((1, head_dim), f32),
        ((1, width), f32),
        ((n, 2 * head_dim + 16, rows), bf),
        ((heads * head_dim, rows), bf),
        ((heads, 1, rows), f32),
        ((heads, 1, rows), f32),
        ((heads * head_dim, rows), f32),
        ((PIECES, 2, xs, chunk, span), bf),
        ((PIECES, xs, chunk, span), bf),
        ((PIECES, xs, chunk, span), bf),
        ((PIECES, xs, chunk, span), bf),
        ((heads * head_dim, width), bf),
        ((nt, heads * head_dim, GATHERED * span), bf),
        ((nt, chunk, heads * head_dim), bf),
        ((nt, chunk, heads * head_dim), bf),
        ((chunk, width), bf),
        ((chunk, width), f32),
        ((lanes, nt, chunk, width), bf),
        ((n, cols, wu), bf),
        ((n, cols, wu), bf),
        ((n, wu, cols), bf),
        ((lanes, rows, wu), f32),
        ((2, xs, lanes, chunk, wu), bf),
        ((n, xs, lanes, chunk, cols), f32),
        ((n, xs, lanes, chunk, cols), bf),
        ((n, xs, lanes, chunk, cols), bf),
        ((n, lanes, chunk, cols), f32),
        ((n, xs, lanes, chunk, cols), bf),
        ((n, xs, lanes, chunk, cols), bf),
        ((bits, n, lanes // 2, chunk, cols), f32),
        ((n, lanes - 1, chunk, cols), bf),
        ((n, lanes - 1, chunk, cols), bf),
    ]
    size = 0
    for shape, kind in shapes:
        count = 1
        for extent in shape:
            count *= extent
        size += count * jnp.dtype(kind).itemsize
    if size > VMEM_LIMIT * 3 // 4:
        return None
    sems = [(lanes,), (lanes,), (n,), (3,), (3, lanes), (3, lanes), (3, n), (9,)]
    sems += [(PIECES,), (PIECES,), (PIECES, xs), (PIECES, xs), (xs,), (xs,), (nt,), (nt,), (nt,)]
    sems += [(bits, lanes), (xs, lanes), (lanes, xs), (lanes, nt)]
    sems += [(n,), (n,), (n, xs), (n, xs), (n, bits), (n, bits), (n, xs), (n, xs), (n, nt)]
    return wide, [pltpu.VMEM(*s) for s in shapes] + [pltpu.SemaphoreType.DMA(s) for s in sems]


def fused_layer(
    n, nt, plan, tokens_in, queries, keys, values, doc_ids, query_gain, key_norm_scale,
    out_weight, norm_gain, gate_weight, up_weight, down_weight,
):
    wide, scratch = plan
    rows, width = tokens_in.shape
    head_dim = query_gain.shape[0]
    places = lax.axis_index("sp") * rows + jnp.arange(rows, dtype=jnp.int32)
    half = head_dim // 2
    freqs = THETA ** (-2.0 * jnp.arange(half // 2, dtype=jnp.float32) / half)
    angles = [
        freqs[:, None] * spot.astype(jnp.float32)[None, :] for spot in (places // GRID, places % GRID)
    ]
    table = jnp.concatenate([f(a) for a in angles for f in (jnp.cos, jnp.sin)], axis=0)
    hbm = pl.BlockSpec(memory_space=pl.ANY)
    out = pl.pallas_call(
        functools.partial(fused_kernel, n, nt, wide),
        out_shape=jax.ShapeDtypeStruct((nt, rows // nt, width), jnp.bfloat16),
        in_specs=[hbm] * 12 + [VM],
        out_specs=VM,
        scratch_shapes=scratch,
        compiler_params=pltpu.CompilerParams(
            collective_id=3, has_side_effects=True, vmem_limit_bytes=VMEM_LIMIT
        ),
        name="fused_layer",
    )(
        queries, keys.T, values.T, doc_ids.reshape(1, rows), query_gain.reshape(1, head_dim),
        key_norm_scale.reshape(1, head_dim), norm_gain.reshape(1, width), tokens_in, out_weight,
        gate_weight, up_weight, down_weight, table,
    )
    return out.reshape(rows, width)


def per_device(
    n,
    nt,
    tokens_in,
    queries,
    keys,
    values,
    doc_ids,
    query_gain,
    key_norm_scale,
    out_weight,
    norm_gain,
    gate_weight,
    up_weight,
    down_weight,
):
    tok_rows = tokens_in.shape[0]
    head_dim = query_gain.shape[0]
    local_heads = queries.shape[1] // head_dim
    plan = None
    if keys.shape[1] == head_dim:
        plan = fused_plan(
            n, nt, tok_rows, tokens_in.shape[1], head_dim, local_heads, gate_weight.shape[1]
        )
    if plan is not None:
        return fused_layer(
            n, nt, plan, tokens_in, queries, keys, values, doc_ids, query_gain, key_norm_scale,
            out_weight, norm_gain, gate_weight, up_weight, down_weight,
        )
    places = lax.axis_index("sp") * tok_rows + jnp.arange(tok_rows, dtype=jnp.int32)
    lattice_row = (places // GRID).astype(jnp.float32)
    lattice_column = (places % GRID).astype(jnp.float32)
    q_local = normalized_rotated(queries, query_gain, local_heads, lattice_row, lattice_column)
    q_rows = q_local.transpose(1, 0, 2).reshape(local_heads * tok_rows, head_dim)
    lanes = [[2 * j + side for j in range(n // 2)] for side in range(2)]
    gate_up_all = lax.all_gather(
        pair_share(n, [gate_weight, up_weight], 1, 0), "sp", axis_index_groups=lanes, axis=0, tiled=True
    )
    down_all = lax.all_gather(
        pair_share(n, [down_weight], 0, 1), "sp", axis_index_groups=lanes, axis=1, tiled=True
    )
    turned = normalized_rotated(keys, key_norm_scale, 1, lattice_row, lattice_column)
    packed = jnp.concatenate([turned.reshape(tok_rows, head_dim), values], axis=1)
    kv_all, doc_all = gather_sp(n, packed, doc_ids.reshape(1, tok_rows))
    row_docs = jnp.tile(doc_ids, local_heads)
    first_doc = doc_ids[0]
    last_doc = doc_ids[-1]
    scale = head_dim ** (-0.5)
    total_rows = local_heads * tok_rows

    def absorb_block(state, key_block, value_block, doc_block):

        def absorb(current):
            running_max, running_sum, running_acc = current
            scores = (
                jnp.einsum("qd,kd->qk", q_rows, key_block, preferred_element_type=jnp.float32)
                * scale
            )
            same = row_docs[:, None] == doc_block[None, :]
            scores = jnp.where(same, scores, NEG)
            new_max = jnp.maximum(running_max, jnp.max(scores, axis=1))
            weights = jnp.where(same, jnp.exp(scores - new_max[:, None]), 0.0)
            shrink = jnp.exp(running_max - new_max)
            new_sum = running_sum * shrink + jnp.sum(weights, axis=1)
            new_acc = running_acc * shrink[:, None] + jnp.dot(
                weights.astype(jnp.bfloat16), value_block, preferred_element_type=jnp.float32
            )
            return (new_max, new_sum, new_acc)

        touches = (doc_block[0] <= last_doc) & (doc_block[-1] >= first_doc)
        return lax.cond(touches, absorb, lambda current: current, state)

    initial = (
        jnp.full((total_rows,), NEG, jnp.float32),
        jnp.zeros((total_rows,), jnp.float32),
        jnp.zeros((total_rows, head_dim), jnp.float32),
    )
    carry = initial
    shards = n
    joined = 1
    while joined * 2 <= shards and shards % (joined * 2) == 0 and (joined * 2 * tok_rows <= 1024):
        joined = joined * 2
    blocks = shards // joined
    span_rows = joined * tok_rows
    key_blocks = kv_all[..., :head_dim].reshape(blocks, span_rows, head_dim)
    value_blocks = kv_all[..., head_dim:].reshape(blocks, span_rows, head_dim)
    doc_blocks = doc_all.reshape(blocks, span_rows)

    def visit(state, inputs):
        key_block, value_block, doc_block = inputs
        return (absorb_block(state, key_block, value_block, doc_block), None)

    carry, unused = lax.scan(visit, carry, (key_blocks, value_blocks, doc_blocks))
    attended = (carry[2] / carry[1][:, None]).astype(jnp.bfloat16)
    attended = (
        attended.reshape(local_heads, tok_rows, head_dim)
        .transpose(1, 0, 2)
        .reshape(tok_rows, local_heads * head_dim)
    )
    partial_value = jnp.dot(attended, out_weight, preferred_element_type=jnp.float32)
    normed, resid = mid_stage(nt, partial_value.astype(jnp.bfloat16), tokens_in, norm_gain)
    normed = normed.reshape(2 * tok_rows, -1)
    both = jnp.dot(normed, gate_up_all, preferred_element_type=jnp.float32)
    units = both.shape[1] // 2
    hidden = (jax.nn.silu(both[:, :units]) * both[:, units:]).astype(jnp.bfloat16)
    fed_part = jnp.dot(hidden, down_all, preferred_element_type=jnp.float32)
    out = last_stage(nt, fed_part.astype(jnp.bfloat16), resid)
    return out.reshape(tok_rows, -1)


def solution(mesh):
    return jax.shard_map(
        functools.partial(per_device, mesh.shape["sp"], mesh.shape["tp"]),
        mesh=mesh,
        in_specs=(
            P("sp", None),
            P("sp", "tp"),
            P("sp", "tp"),
            P("sp", "tp"),
            P("sp"),
            P(),
            P(),
            P("tp", None),
            P(),
            P("sp", "tp"),
            P("sp", "tp"),
            P("tp", "sp"),
        ),
        out_specs=P("sp", None),
        check_vma=False,
    )
```

```python
import functools

import jax
import jax.numpy as jnp
from jax import lax
from jax.experimental import pallas as pl
from jax.experimental.pallas import tpu as pltpu
from jax.sharding import PartitionSpec as P

GRID = 64


EPS = 1e-06
THETA = 10000.0
NEG = -1e30


def rotate_half(block, angle):
    half_dim = block.shape[-1] // 2
    cosine = jnp.cos(angle)[:, None, :]
    sine = jnp.sin(angle)[:, None, :]
    first = block[..., :half_dim]
    second = block[..., half_dim:]
    return jnp.concatenate(
        [first * cosine - second * sine, second * cosine + first * sine], axis=-1
    )


def normalized_rotated(values_in, gain, heads, lattice_row, lattice_column):
    full = values_in.astype(jnp.float32).reshape(values_in.shape[0], heads, -1)
    full = full * lax.rsqrt(jnp.mean(full * full, axis=-1, keepdims=True) + EPS) * gain
    half_dim = full.shape[-1] // 2
    freqs = THETA ** (-2.0 * jnp.arange(half_dim // 2, dtype=jnp.float32) / half_dim)
    by_row = rotate_half(full[..., :half_dim], lattice_row[:, None] * freqs[None, :])
    by_col = rotate_half(full[..., half_dim:], lattice_column[:, None] * freqs[None, :])
    return jnp.concatenate([by_row, by_col], axis=-1).astype(jnp.bfloat16)


MESH = pl.DeviceIdType.MESH
VM = pl.BlockSpec(memory_space=pltpu.VMEM)


def params(cid):
    return pltpu.CompilerParams(
        collective_id=cid, has_side_effects=True, vmem_limit_bytes=56 * 1024 * 1024
    )


def greet(count, where):
    barrier = pltpu.get_barrier_semaphore()

    @pl.loop(1, count)
    def _(step):
        pl.semaphore_signal(barrier, inc=1, device_id=where(step), device_id_type=MESH)

    pl.semaphore_wait(barrier, count - 1)


def gather_kernel(n, kv_ref, doc_ref, kv_out, doc_out, send, recv, doc_send, doc_recv):
    me = lax.axis_index("sp")

    def where(step):
        return {"sp": lax.rem(me + step, n)}

    def copies(step, slot):
        return (
            pltpu.make_async_remote_copy(
                kv_ref, kv_out.at[slot], send.at[step], recv.at[step], where(step), MESH
            ),
            pltpu.make_async_remote_copy(
                doc_ref, doc_out.at[slot], doc_send.at[step], doc_recv.at[step], where(step), MESH
            ),
        )

    greet(n, where)

    @pl.loop(1, n)
    def _(step):
        for copy in copies(step, me):
            copy.start()

    kv_out[me] = kv_ref[...]
    doc_out[me] = doc_ref[...]

    @pl.loop(1, n)
    def _(step):
        for copy in copies(step, lax.rem(me + n - step, n)):
            copy.wait_recv()
            copy.wait_send()


def gather_sp(n, packed, docs):
    return pl.pallas_call(
        functools.partial(gather_kernel, n),
        out_shape=(
            jax.ShapeDtypeStruct((n,) + packed.shape, packed.dtype),
            jax.ShapeDtypeStruct((n,) + docs.shape, docs.dtype),
        ),
        in_specs=[VM, VM],
        out_specs=(VM, VM),
        scratch_shapes=[pltpu.SemaphoreType.DMA((n,))] * 4,
        compiler_params=params(0),
        name="gather_sp",
    )(packed, docs)


def mid_kernel(
    nt, partial_ref, tokens_ref, gain_ref, normed_out, resid_out, landing, send, recv, send2, recv2
):
    sp, tp = lax.axis_index("sp"), lax.axis_index("tp")
    side = lax.rem(sp, 2)
    base = sp - side
    group = 2 * nt
    me = side * nt + tp
    rows = resid_out.shape[0]

    def where(step):
        other = lax.rem(me + step, group)
        return {"sp": base + other // nt, "tp": lax.rem(other, nt)}

    def part(step):
        peer = lax.rem(tp + step, nt)
        return pltpu.make_async_remote_copy(
            partial_ref.at[peer],
            landing.at[step],
            send.at[step],
            recv.at[step],
            {"sp": sp, "tp": peer},
            MESH,
        )

    def spread(step, slot):
        return pltpu.make_async_remote_copy(
            normed_out.at[slot], normed_out.at[slot], send2.at[step], recv2.at[step], where(step), MESH
        )

    greet(group, where)
    for step in range(1, nt):
        part(step).start()
    for step in range(1, nt):
        part(step).wait_recv()
    chunk = 16

    @pl.loop(0, rows // chunk)
    def _(i):
        at = pl.ds(pl.multiple_of(i * chunk, chunk), chunk)
        mixed = partial_ref[tp, at].astype(jnp.float32)
        for step in range(1, nt):
            mixed = mixed + landing[step, at].astype(jnp.float32)
        resid = tokens_ref[tp, at].astype(jnp.float32) + mixed
        resid_out[at] = resid
        power = jnp.mean(resid * resid, axis=-1, keepdims=True)
        normed_out[me, at] = (resid * lax.rsqrt(power + EPS) * gain_ref[...]).astype(jnp.bfloat16)

    for step in range(1, group):
        spread(step, me).start()
    for step in range(1, group):
        copy = spread(step, lax.rem(me + group - step, group))
        copy.wait_recv()
        copy.wait_send()
    for step in range(1, nt):
        part(step).wait_send()


def mid_stage(nt, part, tokens, gain):
    rows, width = part.shape[0] // nt, part.shape[1]
    return pl.pallas_call(
        functools.partial(mid_kernel, nt),
        out_shape=(
            jax.ShapeDtypeStruct((2 * nt, rows, width), jnp.bfloat16),
            jax.ShapeDtypeStruct((rows, width), jnp.float32),
        ),
        in_specs=[VM, VM, VM],
        out_specs=(VM, VM),
        scratch_shapes=[pltpu.VMEM((nt, rows, width), jnp.bfloat16)]
        + [pltpu.SemaphoreType.DMA((nt,))] * 2
        + [pltpu.SemaphoreType.DMA((2 * nt,))] * 2,
        compiler_params=params(1),
        name="mid_stage",
    )(part.reshape(nt, rows, width), tokens.reshape(nt, rows, width), gain.reshape(1, width))


def last_kernel(nt, fed_ref, resid_ref, out_ref, landing, send, recv, send2, recv2):
    sp, tp = lax.axis_index("sp"), lax.axis_index("tp")
    side = lax.rem(sp, 2)
    base = sp - side
    group = 2 * nt
    me = side * nt + tp
    rows = resid_ref.shape[0]

    def where(step):
        other = lax.rem(me + step, group)
        return {"sp": base + other // nt, "tp": lax.rem(other, nt)}

    def part(step):
        return pltpu.make_async_remote_copy(
            fed_ref.at[lax.rem(me + step, group)],
            landing.at[step],
            send.at[step],
            recv.at[step],
            where(step),
            MESH,
        )

    def spread(step, slot):
        return pltpu.make_async_remote_copy(
            out_ref.at[slot],
            out_ref.at[slot],
            send2.at[step],
            recv2.at[step],
            {"sp": sp, "tp": lax.rem(tp + step, nt)},
            MESH,
        )

    greet(group, where)
    for step in range(1, group):
        part(step).start()
    for step in range(1, group):
        part(step).wait_recv()
    chunk = 16

    @pl.loop(0, rows // chunk)
    def _(i):
        at = pl.ds(pl.multiple_of(i * chunk, chunk), chunk)
        fed = fed_ref[me, at].astype(jnp.float32)
        for step in range(1, group):
            fed = fed + landing[step, at].astype(jnp.float32)
        out_ref[tp, at] = (resid_ref[at] + fed).astype(jnp.bfloat16)

    for step in range(1, nt):
        spread(step, tp).start()
    for step in range(1, nt):
        copy = spread(step, lax.rem(tp + nt - step, nt))
        copy.wait_recv()
        copy.wait_send()
    for step in range(1, group):
        part(step).wait_send()


def last_stage(nt, fed, resid):
    rows, width = resid.shape
    return pl.pallas_call(
        functools.partial(last_kernel, nt),
        out_shape=jax.ShapeDtypeStruct((nt, rows, width), jnp.bfloat16),
        in_specs=[VM, VM],
        out_specs=VM,
        scratch_shapes=[pltpu.VMEM((2 * nt, rows, width), jnp.bfloat16)]
        + [pltpu.SemaphoreType.DMA((2 * nt,))] * 2
        + [pltpu.SemaphoreType.DMA((nt,))] * 2,
        compiler_params=params(2),
        name="last_stage",
    )(fed.reshape(2 * nt, rows, width), resid)


def pair_share(n, arrays, axis, joins):
    side = lax.rem(lax.axis_index("sp"), 2)
    own, away = [], []
    for array in arrays:
        half = array.shape[axis] // 2
        own.append(lax.dynamic_slice_in_dim(array, side * half, half, axis))
        away.append(lax.dynamic_slice_in_dim(array, (1 - side) * half, half, axis))
    own = jnp.concatenate(own, axis=axis)
    away = jnp.concatenate(away, axis=axis)
    came = lax.ppermute(away, "sp", [(i, i ^ 1) for i in range(n)])
    first = jnp.where(side == 0, own, came)
    second = jnp.where(side == 0, came, own)
    return jnp.concatenate([first, second], axis=joins)


SIDES = 2
LANE = 128
PIECES = 4
GATHERED = 2


def turned(block, gain, table):
    power = jnp.mean(block * block, axis=0, keepdims=True)
    full = block * lax.rsqrt(power + EPS) * gain
    half = block.shape[0] // 2
    quarter = half // 2
    pieces = []
    for part in range(2):
        first = full[part * half : part * half + quarter]
        second = full[part * half + quarter : (part + 1) * half]
        cosine, sine = table[2 * part], table[2 * part + 1]
        pieces += [first * cosine - second * sine, second * cosine + first * sine]
    return jnp.concatenate(pieces, axis=0)


def identity(size):
    down = lax.broadcasted_iota(jnp.int32, (size, size), 0)
    across = lax.broadcasted_iota(jnp.int32, (size, size), 1)
    return (down == across).astype(jnp.bfloat16)


def flipped(array):
    return lax.dot_general(
        identity(array.shape[1]), array, (((1,), (1,)), ((), ())), preferred_element_type=jnp.float32
    )


def upright_row(row):
    size = row.shape[1]
    down = lax.broadcasted_iota(jnp.int32, (size, size), 0)
    across = lax.broadcasted_iota(jnp.int32, (size, size), 1)
    return jnp.sum(jnp.where(down == across, row, 0.0), axis=1, keepdims=True)


def fused_kernel(
    n,
    nt,
    wide,
    q_in,
    k_in,
    v_in,
    doc_in,
    q_gain_in,
    k_gain_in,
    norm_gain_in,
    tokens,
    out_weight,
    gate,
    up,
    down,
    *rest,
):
    tables, (out, scratch) = rest[:4], (rest[4], rest[5:])
    (
        q_raw,
        k_raw,
        doc_ref,
        q_gain_ref,
        k_gain_ref,
        norm_gain,
        kv,
        q_ref,
        top,
        total,
        acc,
        part,
        part_in,
        px_out,
        px_in,
        ow,
        ow_all,
        att_out,
        att,
        tok,
        resid,
        act,
        gw,
        uw,
        dw,
        gated,
        hid,
        keep,
        core_out,
        core_in,
        x_keep,
        x_out,
        x_in,
        z_keep,
        z_out,
        z_in,
        kv_zs,
        kv_ys,
        kv_r,
        w_own,
        w_zs,
        w_ys,
        w_r,
        misc,
        pc_s,
        pc_r,
        px_s,
        px_r,
        ow_xs,
        ow_cs,
        ow_r,
        att_s,
        att_r,
        act_zs,
        act_xs,
        act_cs,
        act_r,
        rs_cs,
        rs_cr,
        rs_xs,
        rs_xr,
        rs_zs,
        rs_zr,
        ag_xs,
        ag_cs,
        ag_r,
    ) = scratch
    sp, tp = lax.axis_index("sp"), lax.axis_index("tp")
    lanes, xs = n // SIDES, nt // 2
    bits = lanes.bit_length() - 1
    lane, side = sp // SIDES, sp % SIDES
    xi, core = tp // 2, tp % 2
    rows = q_in.shape[0]
    head_dim = k_in.shape[0]
    heads = q_in.shape[1] // head_dim
    chunk = rows // nt
    blocks = gate.shape[1] // LANE
    width = wide * LANE
    last = blocks - (lanes - 1) * wide
    kv_docs = head_dim
    table = tuple(ref[...] for ref in tables)

    def at_sp(lane_to, side_to):
        return {"sp": lane_to * SIDES + side_to, "tp": tp}

    def at_tp(x_to, core_to):
        return {"sp": sp, "tp": x_to * 2 + core_to}

    def remote(src, dst, send, recv, where):
        return pltpu.make_async_remote_copy(src, dst, send, recv, where, MESH)

    def lane_at(d):
        return (lane + d) % lanes

    def x_at(d):
        return (xi + d) % xs

    def bit_of(value, b):
        return (value // (1 << b)) % 2

    def partner(b):
        return lane + (1 - 2 * bit_of(lane, b)) * (1 << b)

    def mate(e):
        return lane + sum((e >> b) % 2 * (1 - 2 * bit_of(lane, b)) * (1 << b) for b in range(bits))

    def mated(i):
        total_of = 0
        for b in range(bits):
            total_of = total_of + (bit_of(lane, b) + bit_of(i, b)) % 2 * (1 << b)
        return total_of

    def low_bit(e):
        return (e & -e).bit_length() - 1

    other_side = 1 - side
    other_core = 1 - core

    barrier = pltpu.get_barrier_semaphore()
    for d in range(1, lanes):
        pl.semaphore_signal(barrier, inc=1, device_id=at_sp(lane_at(d), side), device_id_type=MESH)
    pl.semaphore_signal(barrier, inc=1, device_id=at_sp(lane, other_side), device_id_type=MESH)
    for d in range(1, nt):
        pl.semaphore_signal(
            barrier, inc=1, device_id={"sp": sp, "tp": (tp + d) % nt}, device_id_type=MESH
        )

    def rank(lane_to):
        return lane_to + core * (lanes - 1 - 2 * lane_to)

    def sized(lane_to, action):
        if last == wide:
            action(width)
            return
        few = rank(lane_to) // (lanes - 1)

        @pl.when(few == 1)
        def _():
            action(last * LANE)

        @pl.when(few == 0)
        def _():
            action(width)

    def weight_block(m, lane_to, size):
        at = pl.ds(pl.multiple_of(rank(lane_to) * width, LANE), size)
        if m == 0:
            return gate.at[:, at]
        if m == 1:
            return up.at[:, at]
        return down.at[at, :]

    def landing(m, slot, size):
        if m == 0:
            return gw.at[slot, :, 0:size]
        if m == 1:
            return uw.at[slot, :, 0:size]
        return dw.at[slot, 0:size, :]

    def w_local(m, size):
        return pltpu.make_async_copy(weight_block(m, lane, size), landing(m, sp, size), w_own.at[m])

    ow_copy = pltpu.make_async_copy(out_weight, ow, misc.at[0])
    tok_copy = pltpu.make_async_copy(
        tokens.at[pl.ds(pl.multiple_of(tp * chunk, chunk), chunk)], tok, misc.at[1]
    )
    kv_vals = kv.shape[1] - head_dim
    small = [
        pltpu.make_async_copy(k_in, k_raw, misc.at[2]),
        pltpu.make_async_copy(doc_in, doc_ref, misc.at[3]),
        pltpu.make_async_copy(k_gain_in, k_gain_ref, misc.at[4]),
        pltpu.make_async_copy(v_in, kv.at[sp, kv_vals:, :], misc.at[5]),
        pltpu.make_async_copy(q_in, q_raw, misc.at[6]),
        pltpu.make_async_copy(q_gain_in, q_gain_ref, misc.at[7]),
        pltpu.make_async_copy(norm_gain_in, norm_gain, misc.at[8]),
    ]
    for copy in small:
        copy.start()
    for m in range(3):
        sized(lane, lambda size, m=m: w_local(m, size).start())
    ow_copy.start()
    tok_copy.start()

    for copy in small[:4]:
        copy.wait()
    k_full = turned(k_raw[...].astype(jnp.float32), upright_row(k_gain_ref[...]), table)
    kv[sp, 0:head_dim, :] = k_full.astype(jnp.bfloat16)
    q_doc = doc_ref[...].astype(jnp.float32)
    kv[sp, kv_docs:kv_vals, :] = jnp.broadcast_to(q_doc, (kv_vals - kv_docs, rows)).astype(jnp.bfloat16)

    pl.semaphore_wait(barrier, lanes - 1 + 1 + nt - 1)

    def kv_z(e, lane_of):
        slot = lane_of * SIDES + side
        return remote(kv.at[slot], kv.at[slot], kv_zs.at[e], kv_r.at[slot], at_sp(mate(e), side))

    def kv_y(lane_of, side_of):
        slot = lane_of * SIDES + side_of
        return remote(
            kv.at[slot], kv.at[slot], kv_ys.at[lane_of], kv_r.at[slot], at_sp(lane, other_side)
        )

    for e in range(1, lanes):
        kv_z(e, lane).start()
    kv_y(lane, side).start()

    span = ow.shape[1] // PIECES
    gathered = GATHERED * span
    ow_here = out_weight.at[:, 0:gathered]

    def ow_x(d, slot):
        return remote(ow_here, ow_all.at[slot], ow_xs.at[d], ow_r.at[slot], at_tp(x_at(d), core))

    def ow_core(x_of, core_of):
        slot = x_of * 2 + core_of
        return remote(
            ow_all.at[slot], ow_all.at[slot], ow_cs.at[x_of], ow_r.at[slot], at_tp(xi, other_core)
        )

    for d in range(1, xs):
        ow_x(d, tp).start()
    remote(ow_here, ow_all.at[tp], ow_cs.at[xi], ow_r.at[tp], at_tp(xi, other_core)).start()

    def w_z(m, e, slot, lane_to, size):
        return remote(
            weight_block(m, lane_to, size),
            landing(m, slot, size),
            w_zs.at[m, e],
            w_r.at[m, slot],
            at_sp(mate(e), side),
        )

    def w_y(m, lane_of, side_of, size):
        slot = lane_of * SIDES + side_of
        return remote(
            landing(m, slot, size),
            landing(m, slot, size),
            w_ys.at[m, lane_of],
            w_r.at[m, slot],
            at_sp(lane, other_side),
        )

    def send_weight(m, e):
        lane_to = mate(e)
        sized(lane_to, lambda size: w_z(m, e, sp, lane_to, size).start())

    def share_weight(m):
        def own(size):
            w_local(m, size).wait()
            w_y(m, lane, side, size).start()

        sized(lane, own)

    def forward_weight(m, lane_of):
        sized(lane, lambda size: w_z(m, 1, lane_of * SIDES + side, lane, size).wait_recv())
        sized(lane, lambda size: w_y(m, lane_of, side, size).start())

    def w_shared(m, lane_of):
        sized(lane, lambda size: w_y(m, lane_of, other_side, size).wait_recv())

    for e in range(1, lanes):
        send_weight(0, e)
    share_weight(0)

    scale = head_dim ** (-0.5)
    for copy in small[4:]:
        copy.wait()
    standing_q = flipped(q_raw[...])
    q_gain = upright_row(q_gain_ref[...])
    for h in range(heads):
        at = slice(h * head_dim, (h + 1) * head_dim)
        query = turned(standing_q[at, :], q_gain, table)
        q_ref[at, :] = (query.astype(jnp.bfloat16).astype(jnp.float32) * scale).astype(jnp.bfloat16)
    top[...] = jnp.full(top.shape, NEG, jnp.float32)
    total[...] = jnp.zeros(total.shape, jnp.float32)
    acc[...] = jnp.zeros(acc.shape, jnp.float32)

    def absorb(slot):
        upright = lax.dot_general(
            identity(rows),
            kv[slot, 0:kv_vals, :],
            (((1,), (1,)), ((), ())),
            preferred_element_type=jnp.float32,
        )
        key = upright[:, 0:head_dim].astype(jnp.bfloat16)
        same = upright[:, head_dim : head_dim + 1] == q_doc
        value = kv[slot, kv_vals:, :]
        for h in range(heads):
            at = slice(h * head_dim, (h + 1) * head_dim)
            scores = jnp.dot(key, q_ref[at, :], preferred_element_type=jnp.float32)
            scores = jnp.where(same, scores, NEG)
            before = top[h]
            now = jnp.maximum(before, jnp.max(scores, axis=0, keepdims=True))
            weights = jnp.exp(scores - now)
            shrink = jnp.exp(before - now)
            top[h] = now
            total[h] = total[h] * shrink + jnp.sum(weights, axis=0, keepdims=True)
            acc[at, :] = acc[at, :] * shrink + jnp.dot(
                value, weights.astype(jnp.bfloat16), preferred_element_type=jnp.float32
            )

    @pl.loop(0, SIDES)
    def _(k):
        side_of = (side + k) % SIDES

        @pl.when(k > 0)
        def _():
            kv_y(lane, other_side).wait_recv()

        absorb(lane * SIDES + side_of)

    @pl.loop(0, SIDES * (lanes - 1))
    def _(k):
        lane_of = mated(k % (lanes - 1) + 1)
        side_of = (side + k // (lanes - 1)) % SIDES
        slot = lane_of * SIDES + side_of

        @pl.when(k < lanes - 1)
        def _():
            kv_z(1, lane_of).wait_recv()
            kv_y(lane_of, side).start()

        @pl.when(k >= lanes - 1)
        def _():
            kv_y(lane_of, other_side).wait_recv()

        absorb(slot)

    send_weight(1, 1)
    share_weight(1)
    pieces = []
    for h in range(heads):
        at = slice(h * head_dim, (h + 1) * head_dim)
        pieces.append((acc[at, :] / total[h]).astype(jnp.bfloat16))
    attended = flipped(jnp.concatenate(pieces, axis=0)).astype(jnp.bfloat16)

    def att_copy(d, peer, slot):
        return remote(
            att_out.at[peer], att.at[slot], att_s.at[d], att_r.at[slot], {"sp": sp, "tp": peer}
        )

    for i in range(nt):
        att_out[i] = attended[i * chunk : (i + 1) * chunk]
    for d in range(1, nt):
        att_copy(d, (tp + d) % nt, tp).start()

    def part_core(p):
        return remote(part.at[p, other_core], part_in.at[p], pc_s.at[p], pc_r.at[p], at_tp(xi, other_core))

    def part_x(p, d):
        return remote(px_out.at[p, d], px_in.at[p, d], px_s.at[p, d], px_r.at[p, d], at_tp(x_at(d), core))

    ow_copy.wait()
    for p in range(GATHERED, PIECES):
        product = jnp.dot(
            attended, ow[:, p * span : (p + 1) * span], preferred_element_type=jnp.float32
        ).astype(jnp.bfloat16)
        for x_of in range(xs):
            for core_of in range(2):
                start = (x_of * 2 + core_of) * chunk
                part[p, core_of, x_of] = product[start : start + chunk]
        part_core(p).start()
    for d in range(1, xs):
        x_of = x_at(xs - d)
        ow_x(d, x_of * 2 + core).wait_recv()
        ow_core(x_of, core).start()
    tok_copy.wait()
    early = slice(0, gathered)

    def project(rows_of, weight):
        product = jnp.dot(rows_of, weight, preferred_element_type=jnp.float32)
        return product.astype(jnp.bfloat16).astype(jnp.float32)

    resid[:, early] = tok[:, early].astype(jnp.float32) + project(att_out[tp], ow[:, early])
    for p in range(GATHERED, PIECES):
        at = slice(p * span, (p + 1) * span)
        part_core(p).wait_recv()
        for d in range(1, xs):
            x_to = x_at(d)
            px_out[p, d] = (
                part[p, core, x_to].astype(jnp.float32) + part_in[p, x_to].astype(jnp.float32)
            ).astype(jnp.bfloat16)
            part_x(p, d).start()
        resid[:, at] = (
            tok[:, at].astype(jnp.float32)
            + part[p, core, xi].astype(jnp.float32)
            + part_in[p, xi].astype(jnp.float32)
        )

    def add_rows(slot):
        att_copy(1, tp, slot).wait_recv()
        resid[:, early] += project(att[slot], ow_all[slot])

    ow_core(xi, other_core).wait_recv()
    add_rows(xi * 2 + other_core)
    for d in range(1, xs):
        add_rows(x_at(xs - d) * 2 + core)
    for d in range(1, xs):
        ow_core(x_at(xs - d), other_core).wait_recv()
        add_rows(x_at(xs - d) * 2 + other_core)
    for p in range(GATHERED, PIECES):
        at = slice(p * span, (p + 1) * span)
        for d in range(1, xs):
            part_x(p, d).wait_recv()
            resid[:, at] += px_in[p, d].astype(jnp.float32)

    whole = resid[...]
    power = jnp.mean(whole * whole, axis=-1, keepdims=True)
    act[lane, tp] = (whole * lax.rsqrt(power + EPS) * norm_gain[...]).astype(jnp.bfloat16)

    def act_z(b, lane_of):
        return remote(
            act.at[lane_of, tp],
            act.at[lane_of, tp],
            act_zs.at[b, lane_of],
            act_r.at[lane_of, tp],
            at_sp(partner(b), side),
        )

    def act_x(d, lane_of, slot):
        return remote(
            act.at[lane_of, slot],
            act.at[lane_of, slot],
            act_xs.at[d, lane_of],
            act_r.at[lane_of, slot],
            at_tp(x_at(d), core),
        )

    def act_core(lane_of, x_of, core_of):
        slot = x_of * 2 + core_of
        return remote(
            act.at[lane_of, slot],
            act.at[lane_of, slot],
            act_cs.at[lane_of, x_of],
            act_r.at[lane_of, slot],
            at_tp(xi, other_core),
        )

    def act_out(lane_of):
        for d in range(1, xs):
            act_x(d, lane_of, tp).start()
        act_core(lane_of, xi, core).start()

    def act_from_x(lane_of):
        for d in range(1, xs):
            x_of = x_at(xs - d)
            act_x(d, lane_of, x_of * 2 + core).wait_recv()
            act_core(lane_of, x_of, core).start()

    def act_arrived(e):
        step = low_bit(e)
        act_z(step, mate(e)).wait_recv()
        for lower in reversed(range(step)):
            act_z(lower, mate(e)).start()
        act_out(mate(e))

    for b in reversed(range(bits)):
        act_z(b, lane).start()
    act_out(lane)
    for e in range(2, lanes - 1):
        send_weight(1, e)
    for e in range(1, lanes):
        forward_weight(0, mate(e))
    act_from_x(lane)
    for e in range(1, lanes - 1):
        act_arrived(e)
    send_weight(1, lanes - 1)
    share_weight(2)
    forward_weight(1, mate(1))

    few_here = rank(lane) // (lanes - 1)
    unit = lax.broadcasted_iota(jnp.int32, (nt * chunk, width), 1)
    mine = unit < (wide - few_here * (wide - last)) * LANE
    if last < wide:

        @pl.when(few_here == 1)
        def _():
            dw[:, last * LANE :, :] = jnp.zeros((n, width - last * LANE, dw.shape[2]), dw.dtype)

    def depth(ref):
        return ref[...].reshape(ref.shape[0] * ref.shape[1], ref.shape[2])

    for d in range(lanes):
        w_shared(0, lane_at(d))

    @pl.loop(0, lanes)
    def _(i):
        lane_of = mated(i)
        for e in range(1, lanes):

            @pl.when(i == e)
            def _(e=e):
                if e == lanes - 2:
                    act_arrived(e + 1)
                    for f in range(1, lanes):
                        send_weight(2, f)
                if e > 1:
                    forward_weight(1, mate(e))
                act_from_x(mate(e))

        for x_of in range(xs):
            act_core(lane_of, x_of, other_core).wait_recv()
        inputs = act[lane_of].reshape(nt * chunk, act.shape[-1])
        gated[lane_of] = jnp.dot(inputs, depth(gw), preferred_element_type=jnp.float32)

    for d in range(lanes):
        w_shared(1, lane_at(d))

    @pl.loop(0, lanes)
    def _(lane_of):
        inputs = act[lane_of].reshape(nt * chunk, act.shape[-1])
        lifted = jnp.dot(inputs, depth(uw), preferred_element_type=jnp.float32)
        gates = gated[lane_of]
        hidden = jnp.where(mine, gates * lax.logistic(gates) * lifted, 0.0).astype(jnp.bfloat16)
        for x_of in range(xs):
            for core_of in range(2):
                start = (x_of * 2 + core_of) * chunk
                hid[core_of, x_of, lane_of] = hidden[start : start + chunk]

    for e in range(1, lanes // 2):
        forward_weight(2, mate(e))

    cols = dw.shape[2]
    share = xs * lanes * chunk
    starts = [lanes - (lanes >> b) for b in range(bits)]

    def rs_core(s):
        return remote(core_out.at[s], core_in.at[s], rs_cs.at[s], rs_cr.at[s], at_tp(xi, other_core))

    def rs_x(s, d):
        return remote(x_out.at[s, d], x_in.at[s, d], rs_xs.at[s, d], rs_xr.at[s, d], at_tp(x_at(d), core))

    def rs_z(s, b):
        piece = pl.ds(starts[b], lanes >> (b + 1))
        return remote(
            z_out.at[s, piece], z_in.at[s, piece], rs_zs.at[s, b], rs_zr.at[s, b], at_sp(partner(b), side)
        )

    def columns(s):
        return pl.ds(pl.multiple_of(s * cols, cols), cols)

    def ag_x(s, d, slot):
        piece = out.at[slot, :, columns(s)]
        return remote(piece, piece, ag_xs.at[s, d], ag_r.at[s, slot], at_tp(x_at(d), core))

    def ag_core(s, x_of, core_of):
        slot = x_of * 2 + core_of
        piece = out.at[slot, :, columns(s)]
        return remote(piece, piece, ag_cs.at[s, x_of], ag_r.at[s, slot], at_tp(xi, other_core))

    half = lanes // 2
    upper = lane // half

    def half_slot(k):
        turn = k % lanes
        lane_of = (upper + k // lanes) % 2 * half + turn % half
        return lane_of * SIDES + (side + turn // half) % SIDES

    def slot_of(i):
        turn = i // 2
        lane_of = i % 2 * half + turn % half
        return lane_of * SIDES + (side + turn // half) % SIDES

    def multiply(k):
        s = half_slot(k)

        @pl.when((k >= lanes - 1) & (k < lanes - 1 + half))
        def _():
            forward_weight(2, (upper + 1) % 2 * half + k - (lanes - 1))

        @pl.when(k % lanes >= half)
        def _():
            w_shared(2, s // SIDES)

        away = hid[other_core].reshape(share, width)
        core_out[s] = (
            jnp.dot(away, dw[s], preferred_element_type=jnp.float32)
            .astype(jnp.bfloat16)
            .reshape(xs, lanes, chunk, cols)
        )
        rs_core(s).start()
        near = hid[core].reshape(share, width)
        keep[s] = jnp.dot(near, dw[s], preferred_element_type=jnp.float32).reshape(xs, lanes, chunk, cols)

    def reduce_core(k):
        s = half_slot(k)
        rs_core(s).wait_recv()
        for d in range(1, xs):
            x_to = x_at(d)
            x_out[s, d] = (keep[s, x_to] + core_in[s, x_to].astype(jnp.float32)).astype(jnp.bfloat16)
            rs_x(s, d).start()
        x_keep[s] = keep[s, xi] + core_in[s, xi].astype(jnp.float32)

    def reduce_lanes(b, k):
        s = half_slot(k) if b < bits - 1 else slot_of(k)
        if b == 0:
            for d in range(1, xs):
                rs_x(s, d).wait_recv()
        else:
            rs_z(s, b - 1).wait_recv()

        def summed(h):
            if b == 0:
                value = x_keep[s, h]
                for d in range(1, xs):
                    value = value + x_in[s, d, h].astype(jnp.float32)
                return value
            return z_keep[b - 1, s, h] + z_in[s, starts[b - 1] + h].astype(jnp.float32)

        if b == bits:
            out[tp, :, columns(s)] = (resid[:, columns(s)] + summed(0)).astype(jnp.bfloat16)
            for d in range(1, xs):
                ag_x(s, d, tp).start()
            ag_core(s, xi, core).start()
            return
        mine_here = bit_of(lane, b)
        count = lanes >> (b + 1)
        for h in range(count):
            z_out[s, starts[b] + h] = summed(1 - mine_here + 2 * h).astype(jnp.bfloat16)
        rs_z(s, b).start()
        for h in range(count):
            z_keep[b, s, h] = summed(mine_here + 2 * h)

    def spread(k):
        s = slot_of(k)
        for d in range(1, xs):
            x_of = x_at(xs - d)
            ag_x(s, d, x_of * 2 + core).wait_recv()
            ag_core(s, x_of, core).start()

    def by_two(b):
        def both(j):
            for i in range(2):
                reduce_lanes(b, 2 * j + i)

        return both

    lag = 4
    stages = [(0, n, multiply), (1, n, reduce_core)]
    for b in range(bits - 1):
        stages.append((lag, n, functools.partial(reduce_lanes, b)))
        lag += 2
    lag += lanes - 1 if bits > 1 else lanes
    for b in (bits - 1, bits):
        stages.append((lag, n // 2, by_two(b)))
        lag += 2

    @pl.loop(0, stages[-1][0] + n // 2)
    def _(k):
        for lag, count, action in [stages[1], stages[0]] + stages[2:]:

            @pl.when((k >= lag) & (k < count + lag))
            def _(lag=lag, action=action):
                action(k - lag)

    pl.loop(0, n)(spread)

    @pl.loop(0, n)
    def _(s):
        for x_of in range(xs):
            ag_core(s, x_of, other_core).wait_recv()
            ag_core(s, x_of, core).wait_send()
        for d in range(1, xs):
            ag_x(s, d, tp).wait_send()
            rs_x(s, d).wait_send()
        rs_core(s).wait_send()
        for b in range(bits):
            rs_z(s, b).wait_send()

    for d in range(1, lanes):
        kv_z(d, lane).wait_send()
        for m in range(3):
            lane_to = mate(d)
            sized(lane_to, lambda size, m=m, d=d, lane_to=lane_to: w_z(m, d, sp, lane_to, size).wait_send())
    for lane_of in range(lanes):
        kv_y(lane_of, side).wait_send()
        for m in range(3):
            sized(lane, lambda size, m=m, lane_of=lane_of: w_y(m, lane_of, side, size).wait_send())
        for d in range(1, xs):
            act_x(d, lane_of, tp).wait_send()
        for x_of in range(xs):
            act_core(lane_of, x_of, core).wait_send()
    for b in range(bits):
        for h in range(lanes >> (b + 1)):
            lane_of = lane % (1 << (b + 1)) + h * (1 << (b + 1))
            act_z(b, lane_of).wait_send()
    for d in range(1, xs):
        ow_x(d, tp).wait_send()
    for x_of in range(xs):
        ow_core(x_of, core).wait_send()
    for d in range(1, nt):
        att_copy(d, (tp + d) % nt, tp).wait_send()
    for p in range(GATHERED, PIECES):
        part_core(p).wait_send()
        for d in range(1, xs):
            part_x(p, d).wait_send()


VMEM_LIMIT = 60 * 1024 * 1024


def fused_plan(n, nt, rows, width, head_dim, heads, units):
    if n % SIDES or n < 2 * SIDES or nt % 2 or nt < 4 or rows % nt or units % LANE:
        return None
    lanes, xs, chunk, blocks = n // SIDES, nt // 2, rows // nt, units // LANE
    wide = -(-blocks // lanes)
    cols = width // n
    if chunk % 16 or rows % LANE or width % (n * LANE) or width % (PIECES * LANE) or head_dim % 64:
        return None
    if lanes & (lanes - 1) or (lanes - 1) * wide >= blocks:
        return None
    wu = wide * LANE
    bits = lanes.bit_length() - 1
    span = width // PIECES
    bf, f32 = jnp.bfloat16, jnp.float32
    shapes = [
        ((rows, heads * head_dim), bf),
        ((head_dim, rows), bf),
        ((1, rows), jnp.int32),
        ((1, head_dim), f32),
        ((1, head_dim), f32),
        ((1, width), f32),
        ((n, 2 * head_dim + 16, rows), bf),
        ((heads * head_dim, rows), bf),
        ((heads, 1, rows), f32),
        ((heads, 1, rows), f32),
        ((heads * head_dim, rows), f32),
        ((PIECES, 2, xs, chunk, span), bf),
        ((PIECES, xs, chunk, span), bf),
        ((PIECES, xs, chunk, span), bf),
        ((PIECES, xs, chunk, span), bf),
        ((heads * head_dim, width), bf),
        ((nt, heads * head_dim, GATHERED * span), bf),
        ((nt, chunk, heads * head_dim), bf),
        ((nt, chunk, heads * head_dim), bf),
        ((chunk, width), bf),
        ((chunk, width), f32),
        ((lanes, nt, chunk, width), bf),
        ((n, cols, wu), bf),
        ((n, cols, wu), bf),
        ((n, wu, cols), bf),
        ((lanes, rows, wu), f32),
        ((2, xs, lanes, chunk, wu), bf),
        ((n, xs, lanes, chunk, cols), f32),
        ((n, xs, lanes, chunk, cols), bf),
        ((n, xs, lanes, chunk, cols), bf),
        ((n, lanes, chunk, cols), f32),
        ((n, xs, lanes, chunk, cols), bf),
        ((n, xs, lanes, chunk, cols), bf),
        ((bits, n, lanes // 2, chunk, cols), f32),
        ((n, lanes - 1, chunk, cols), bf),
        ((n, lanes - 1, chunk, cols), bf),
    ]
    size = 0
    for shape, kind in shapes:
        count = 1
        for extent in shape:
            count *= extent
        size += count * jnp.dtype(kind).itemsize
    if size > VMEM_LIMIT * 3 // 4:
        return None
    sems = [(lanes,), (lanes,), (n,), (3,), (3, lanes), (3, lanes), (3, n), (9,)]
    sems += [(PIECES,), (PIECES,), (PIECES, xs), (PIECES, xs), (xs,), (xs,), (nt,), (nt,), (nt,)]
    sems += [(bits, lanes), (xs, lanes), (lanes, xs), (lanes, nt)]
    sems += [(n,), (n,), (n, xs), (n, xs), (n, bits), (n, bits), (n, xs), (n, xs), (n, nt)]
    return wide, [pltpu.VMEM(*s) for s in shapes] + [pltpu.SemaphoreType.DMA(s) for s in sems]


def fused_layer(
    n, nt, plan, tokens_in, queries, keys, values, doc_ids, query_gain, key_norm_scale,
    out_weight, norm_gain, gate_weight, up_weight, down_weight,
):
    wide, scratch = plan
    rows, width = tokens_in.shape
    head_dim = query_gain.shape[0]
    places = lax.axis_index("sp") * rows + jnp.arange(rows, dtype=jnp.int32)
    half = head_dim // 2
    freqs = THETA ** (-2.0 * jnp.arange(half // 2, dtype=jnp.float32) / half)
    angles = [
        freqs[:, None] * spot.astype(jnp.float32)[None, :] for spot in (places // GRID, places % GRID)
    ]
    tables = [f(a) for a in angles for f in (jnp.cos, jnp.sin)]
    hbm = pl.BlockSpec(memory_space=pl.ANY)
    out = pl.pallas_call(
        functools.partial(fused_kernel, n, nt, wide),
        out_shape=jax.ShapeDtypeStruct((nt, rows // nt, width), jnp.bfloat16),
        in_specs=[hbm] * 12 + [VM] * 4,
        out_specs=VM,
        scratch_shapes=scratch,
        compiler_params=pltpu.CompilerParams(
            collective_id=3, has_side_effects=True, vmem_limit_bytes=VMEM_LIMIT
        ),
        name="fused_layer",
    )(
        queries, keys.T, values.T, doc_ids.reshape(1, rows), query_gain.reshape(1, head_dim),
        key_norm_scale.reshape(1, head_dim), norm_gain.reshape(1, width), tokens_in, out_weight,
        gate_weight, up_weight, down_weight, *tables,
    )
    return out.reshape(rows, width)


def per_device(
    n,
    nt,
    tokens_in,
    queries,
    keys,
    values,
    doc_ids,
    query_gain,
    key_norm_scale,
    out_weight,
    norm_gain,
    gate_weight,
    up_weight,
    down_weight,
):
    tok_rows = tokens_in.shape[0]
    head_dim = query_gain.shape[0]
    local_heads = queries.shape[1] // head_dim
    plan = None
    if keys.shape[1] == head_dim:
        plan = fused_plan(
            n, nt, tok_rows, tokens_in.shape[1], head_dim, local_heads, gate_weight.shape[1]
        )
    if plan is not None:
        return fused_layer(
            n, nt, plan, tokens_in, queries, keys, values, doc_ids, query_gain, key_norm_scale,
            out_weight, norm_gain, gate_weight, up_weight, down_weight,
        )
    places = lax.axis_index("sp") * tok_rows + jnp.arange(tok_rows, dtype=jnp.int32)
    lattice_row = (places // GRID).astype(jnp.float32)
    lattice_column = (places % GRID).astype(jnp.float32)
    q_local = normalized_rotated(queries, query_gain, local_heads, lattice_row, lattice_column)
    q_rows = q_local.transpose(1, 0, 2).reshape(local_heads * tok_rows, head_dim)
    lanes = [[2 * j + side for j in range(n // 2)] for side in range(2)]
    gate_up_all = lax.all_gather(
        pair_share(n, [gate_weight, up_weight], 1, 0), "sp", axis_index_groups=lanes, axis=0, tiled=True
    )
    down_all = lax.all_gather(
        pair_share(n, [down_weight], 0, 1), "sp", axis_index_groups=lanes, axis=1, tiled=True
    )
    turned = normalized_rotated(keys, key_norm_scale, 1, lattice_row, lattice_column)
    packed = jnp.concatenate([turned.reshape(tok_rows, head_dim), values], axis=1)
    kv_all, doc_all = gather_sp(n, packed, doc_ids.reshape(1, tok_rows))
    row_docs = jnp.tile(doc_ids, local_heads)
    first_doc = doc_ids[0]
    last_doc = doc_ids[-1]
    scale = head_dim ** (-0.5)
    total_rows = local_heads * tok_rows

    def absorb_block(state, key_block, value_block, doc_block):

        def absorb(current):
            running_max, running_sum, running_acc = current
            scores = (
                jnp.einsum("qd,kd->qk", q_rows, key_block, preferred_element_type=jnp.float32)
                * scale
            )
            same = row_docs[:, None] == doc_block[None, :]
            scores = jnp.where(same, scores, NEG)
            new_max = jnp.maximum(running_max, jnp.max(scores, axis=1))
            weights = jnp.where(same, jnp.exp(scores - new_max[:, None]), 0.0)
            shrink = jnp.exp(running_max - new_max)
            new_sum = running_sum * shrink + jnp.sum(weights, axis=1)
            new_acc = running_acc * shrink[:, None] + jnp.dot(
                weights.astype(jnp.bfloat16), value_block, preferred_element_type=jnp.float32
            )
            return (new_max, new_sum, new_acc)

        touches = (doc_block[0] <= last_doc) & (doc_block[-1] >= first_doc)
        return lax.cond(touches, absorb, lambda current: current, state)

    initial = (
        jnp.full((total_rows,), NEG, jnp.float32),
        jnp.zeros((total_rows,), jnp.float32),
        jnp.zeros((total_rows, head_dim), jnp.float32),
    )
    carry = initial
    shards = n
    joined = 1
    while joined * 2 <= shards and shards % (joined * 2) == 0 and (joined * 2 * tok_rows <= 1024):
        joined = joined * 2
    blocks = shards // joined
    span_rows = joined * tok_rows
    key_blocks = kv_all[..., :head_dim].reshape(blocks, span_rows, head_dim)
    value_blocks = kv_all[..., head_dim:].reshape(blocks, span_rows, head_dim)
    doc_blocks = doc_all.reshape(blocks, span_rows)

    def visit(state, inputs):
        key_block, value_block, doc_block = inputs
        return (absorb_block(state, key_block, value_block, doc_block), None)

    carry, unused = lax.scan(visit, carry, (key_blocks, value_blocks, doc_blocks))
    attended = (carry[2] / carry[1][:, None]).astype(jnp.bfloat16)
    attended = (
        attended.reshape(local_heads, tok_rows, head_dim)
        .transpose(1, 0, 2)
        .reshape(tok_rows, local_heads * head_dim)
    )
    partial_value = jnp.dot(attended, out_weight, preferred_element_type=jnp.float32)
    normed, resid = mid_stage(nt, partial_value.astype(jnp.bfloat16), tokens_in, norm_gain)
    normed = normed.reshape(2 * tok_rows, -1)
    both = jnp.dot(normed, gate_up_all, preferred_element_type=jnp.float32)
    units = both.shape[1] // 2
    hidden = (jax.nn.silu(both[:, :units]) * both[:, units:]).astype(jnp.bfloat16)
    fed_part = jnp.dot(hidden, down_all, preferred_element_type=jnp.float32)
    out = last_stage(nt, fed_part.astype(jnp.bfloat16), resid)
    return out.reshape(tok_rows, -1)


def solution(mesh):
    return jax.shard_map(
        functools.partial(per_device, mesh.shape["sp"], mesh.shape["tp"]),
        mesh=mesh,
        in_specs=(
            P("sp", None),
            P("sp", "tp"),
            P("sp", "tp"),
            P("sp", "tp"),
            P("sp"),
            P(),
            P(),
            P("tp", None),
            P(),
            P("sp", "tp"),
            P("sp", "tp"),
            P("tp", "sp"),
        ),
        out_specs=P("sp", None),
        check_vma=False,
    )
```

```python
import functools

import jax
import jax.numpy as jnp
from jax import lax
from jax.experimental import pallas as pl
from jax.experimental.pallas import tpu as pltpu
from jax.sharding import PartitionSpec as P

GRID = 64


EPS = 1e-06
THETA = 10000.0
NEG = -1e30


def rotate_half(block, angle):
    half_dim = block.shape[-1] // 2
    cosine = jnp.cos(angle)[:, None, :]
    sine = jnp.sin(angle)[:, None, :]
    first = block[..., :half_dim]
    second = block[..., half_dim:]
    return jnp.concatenate(
        [first * cosine - second * sine, second * cosine + first * sine], axis=-1
    )


def normalized_rotated(values_in, gain, heads, lattice_row, lattice_column):
    full = values_in.astype(jnp.float32).reshape(values_in.shape[0], heads, -1)
    full = full * lax.rsqrt(jnp.mean(full * full, axis=-1, keepdims=True) + EPS) * gain
    half_dim = full.shape[-1] // 2
    freqs = THETA ** (-2.0 * jnp.arange(half_dim // 2, dtype=jnp.float32) / half_dim)
    by_row = rotate_half(full[..., :half_dim], lattice_row[:, None] * freqs[None, :])
    by_col = rotate_half(full[..., half_dim:], lattice_column[:, None] * freqs[None, :])
    return jnp.concatenate([by_row, by_col], axis=-1).astype(jnp.bfloat16)


MESH = pl.DeviceIdType.MESH
VM = pl.BlockSpec(memory_space=pltpu.VMEM)


def params(cid):
    return pltpu.CompilerParams(
        collective_id=cid, has_side_effects=True, vmem_limit_bytes=56 * 1024 * 1024
    )


def greet(count, where):
    barrier = pltpu.get_barrier_semaphore()

    @pl.loop(1, count)
    def _(step):
        pl.semaphore_signal(barrier, inc=1, device_id=where(step), device_id_type=MESH)

    pl.semaphore_wait(barrier, count - 1)


def gather_kernel(n, kv_ref, doc_ref, kv_out, doc_out, send, recv, doc_send, doc_recv):
    me = lax.axis_index("sp")

    def where(step):
        return {"sp": lax.rem(me + step, n)}

    def copies(step, slot):
        return (
            pltpu.make_async_remote_copy(
                kv_ref, kv_out.at[slot], send.at[step], recv.at[step], where(step), MESH
            ),
            pltpu.make_async_remote_copy(
                doc_ref, doc_out.at[slot], doc_send.at[step], doc_recv.at[step], where(step), MESH
            ),
        )

    greet(n, where)

    @pl.loop(1, n)
    def _(step):
        for copy in copies(step, me):
            copy.start()

    kv_out[me] = kv_ref[...]
    doc_out[me] = doc_ref[...]

    @pl.loop(1, n)
    def _(step):
        for copy in copies(step, lax.rem(me + n - step, n)):
            copy.wait_recv()
            copy.wait_send()


def gather_sp(n, packed, docs):
    return pl.pallas_call(
        functools.partial(gather_kernel, n),
        out_shape=(
            jax.ShapeDtypeStruct((n,) + packed.shape, packed.dtype),
            jax.ShapeDtypeStruct((n,) + docs.shape, docs.dtype),
        ),
        in_specs=[VM, VM],
        out_specs=(VM, VM),
        scratch_shapes=[pltpu.SemaphoreType.DMA((n,))] * 4,
        compiler_params=params(0),
        name="gather_sp",
    )(packed, docs)


def mid_kernel(
    nt, partial_ref, tokens_ref, gain_ref, normed_out, resid_out, landing, send, recv, send2, recv2
):
    sp, tp = lax.axis_index("sp"), lax.axis_index("tp")
    side = lax.rem(sp, 2)
    base = sp - side
    group = 2 * nt
    me = side * nt + tp
    rows = resid_out.shape[0]

    def where(step):
        other = lax.rem(me + step, group)
        return {"sp": base + other // nt, "tp": lax.rem(other, nt)}

    def part(step):
        peer = lax.rem(tp + step, nt)
        return pltpu.make_async_remote_copy(
            partial_ref.at[peer],
            landing.at[step],
            send.at[step],
            recv.at[step],
            {"sp": sp, "tp": peer},
            MESH,
        )

    def spread(step, slot):
        return pltpu.make_async_remote_copy(
            normed_out.at[slot], normed_out.at[slot], send2.at[step], recv2.at[step], where(step), MESH
        )

    greet(group, where)
    for step in range(1, nt):
        part(step).start()
    for step in range(1, nt):
        part(step).wait_recv()
    chunk = 16

    @pl.loop(0, rows // chunk)
    def _(i):
        at = pl.ds(pl.multiple_of(i * chunk, chunk), chunk)
        mixed = partial_ref[tp, at].astype(jnp.float32)
        for step in range(1, nt):
            mixed = mixed + landing[step, at].astype(jnp.float32)
        resid = tokens_ref[tp, at].astype(jnp.float32) + mixed
        resid_out[at] = resid
        power = jnp.mean(resid * resid, axis=-1, keepdims=True)
        normed_out[me, at] = (resid * lax.rsqrt(power + EPS) * gain_ref[...]).astype(jnp.bfloat16)

    for step in range(1, group):
        spread(step, me).start()
    for step in range(1, group):
        copy = spread(step, lax.rem(me + group - step, group))
        copy.wait_recv()
        copy.wait_send()
    for step in range(1, nt):
        part(step).wait_send()


def mid_stage(nt, part, tokens, gain):
    rows, width = part.shape[0] // nt, part.shape[1]
    return pl.pallas_call(
        functools.partial(mid_kernel, nt),
        out_shape=(
            jax.ShapeDtypeStruct((2 * nt, rows, width), jnp.bfloat16),
            jax.ShapeDtypeStruct((rows, width), jnp.float32),
        ),
        in_specs=[VM, VM, VM],
        out_specs=(VM, VM),
        scratch_shapes=[pltpu.VMEM((nt, rows, width), jnp.bfloat16)]
        + [pltpu.SemaphoreType.DMA((nt,))] * 2
        + [pltpu.SemaphoreType.DMA((2 * nt,))] * 2,
        compiler_params=params(1),
        name="mid_stage",
    )(part.reshape(nt, rows, width), tokens.reshape(nt, rows, width), gain.reshape(1, width))


def last_kernel(nt, fed_ref, resid_ref, out_ref, landing, send, recv, send2, recv2):
    sp, tp = lax.axis_index("sp"), lax.axis_index("tp")
    side = lax.rem(sp, 2)
    base = sp - side
    group = 2 * nt
    me = side * nt + tp
    rows = resid_ref.shape[0]

    def where(step):
        other = lax.rem(me + step, group)
        return {"sp": base + other // nt, "tp": lax.rem(other, nt)}

    def part(step):
        return pltpu.make_async_remote_copy(
            fed_ref.at[lax.rem(me + step, group)],
            landing.at[step],
            send.at[step],
            recv.at[step],
            where(step),
            MESH,
        )

    def spread(step, slot):
        return pltpu.make_async_remote_copy(
            out_ref.at[slot],
            out_ref.at[slot],
            send2.at[step],
            recv2.at[step],
            {"sp": sp, "tp": lax.rem(tp + step, nt)},
            MESH,
        )

    greet(group, where)
    for step in range(1, group):
        part(step).start()
    for step in range(1, group):
        part(step).wait_recv()
    chunk = 16

    @pl.loop(0, rows // chunk)
    def _(i):
        at = pl.ds(pl.multiple_of(i * chunk, chunk), chunk)
        fed = fed_ref[me, at].astype(jnp.float32)
        for step in range(1, group):
            fed = fed + landing[step, at].astype(jnp.float32)
        out_ref[tp, at] = (resid_ref[at] + fed).astype(jnp.bfloat16)

    for step in range(1, nt):
        spread(step, tp).start()
    for step in range(1, nt):
        copy = spread(step, lax.rem(tp + nt - step, nt))
        copy.wait_recv()
        copy.wait_send()
    for step in range(1, group):
        part(step).wait_send()


def last_stage(nt, fed, resid):
    rows, width = resid.shape
    return pl.pallas_call(
        functools.partial(last_kernel, nt),
        out_shape=jax.ShapeDtypeStruct((nt, rows, width), jnp.bfloat16),
        in_specs=[VM, VM],
        out_specs=VM,
        scratch_shapes=[pltpu.VMEM((2 * nt, rows, width), jnp.bfloat16)]
        + [pltpu.SemaphoreType.DMA((2 * nt,))] * 2
        + [pltpu.SemaphoreType.DMA((nt,))] * 2,
        compiler_params=params(2),
        name="last_stage",
    )(fed.reshape(2 * nt, rows, width), resid)


def pair_share(n, arrays, axis, joins):
    side = lax.rem(lax.axis_index("sp"), 2)
    own, away = [], []
    for array in arrays:
        half = array.shape[axis] // 2
        own.append(lax.dynamic_slice_in_dim(array, side * half, half, axis))
        away.append(lax.dynamic_slice_in_dim(array, (1 - side) * half, half, axis))
    own = jnp.concatenate(own, axis=axis)
    away = jnp.concatenate(away, axis=axis)
    came = lax.ppermute(away, "sp", [(i, i ^ 1) for i in range(n)])
    first = jnp.where(side == 0, own, came)
    second = jnp.where(side == 0, came, own)
    return jnp.concatenate([first, second], axis=joins)


SIDES = 2
LANE = 128
PIECES = 4
GATHERED = 2


def turned(block, gain, table):
    power = jnp.mean(block * block, axis=0, keepdims=True)
    full = block * lax.rsqrt(power + EPS) * gain
    half = block.shape[0] // 2
    quarter = half // 2
    pieces = []
    for part in range(2):
        first = full[part * half : part * half + quarter]
        second = full[part * half + quarter : (part + 1) * half]
        cosine, sine = table[2 * part], table[2 * part + 1]
        pieces += [first * cosine - second * sine, second * cosine + first * sine]
    return jnp.concatenate(pieces, axis=0)


def identity(size):
    down = lax.broadcasted_iota(jnp.int32, (size, size), 0)
    across = lax.broadcasted_iota(jnp.int32, (size, size), 1)
    return (down == across).astype(jnp.bfloat16)


def flipped(array):
    return lax.dot_general(
        identity(array.shape[1]), array, (((1,), (1,)), ((), ())), preferred_element_type=jnp.float32
    )


def upright_row(row):
    size = row.shape[1]
    down = lax.broadcasted_iota(jnp.int32, (size, size), 0)
    across = lax.broadcasted_iota(jnp.int32, (size, size), 1)
    return jnp.sum(jnp.where(down == across, row, 0.0), axis=1, keepdims=True)


def fused_kernel(
    n,
    nt,
    wide,
    q_in,
    k_in,
    v_in,
    doc_in,
    q_gain_in,
    k_gain_in,
    norm_gain_in,
    tokens,
    out_weight,
    gate,
    up,
    down,
    *rest,
):
    tables, (out, scratch) = rest[:4], (rest[4], rest[5:])
    (
        q_raw,
        k_raw,
        doc_ref,
        q_gain_ref,
        k_gain_ref,
        norm_gain,
        kv,
        q_ref,
        top,
        total,
        acc,
        part,
        part_in,
        px_out,
        px_in,
        ow,
        ow_all,
        att_out,
        att,
        tok,
        resid,
        act,
        gw,
        uw,
        dw,
        gated,
        hid,
        keep,
        core_out,
        core_in,
        x_keep,
        x_out,
        x_in,
        z_keep,
        z_out,
        z_in,
        kv_zs,
        kv_ys,
        kv_r,
        w_own,
        w_zs,
        w_ys,
        w_r,
        misc,
        pc_s,
        pc_r,
        px_s,
        px_r,
        ow_xs,
        ow_cs,
        ow_r,
        att_s,
        att_r,
        act_zs,
        act_xs,
        act_cs,
        act_r,
        rs_cs,
        rs_cr,
        rs_xs,
        rs_xr,
        rs_zs,
        rs_zr,
        ag_xs,
        ag_cs,
        ag_r,
    ) = scratch
    sp, tp = lax.axis_index("sp"), lax.axis_index("tp")
    lanes, xs = n // SIDES, nt // 2
    bits = lanes.bit_length() - 1
    lane, side = sp // SIDES, sp % SIDES
    xi, core = tp // 2, tp % 2
    rows = q_in.shape[0]
    head_dim = k_in.shape[0]
    heads = q_in.shape[1] // head_dim
    chunk = rows // nt
    blocks = gate.shape[1] // LANE
    width = wide * LANE
    last = blocks - (lanes - 1) * wide
    kv_docs = head_dim
    table = tuple(ref[...] for ref in tables)

    def at_sp(lane_to, side_to):
        return {"sp": lane_to * SIDES + side_to, "tp": tp}

    def at_tp(x_to, core_to):
        return {"sp": sp, "tp": x_to * 2 + core_to}

    def remote(src, dst, send, recv, where):
        return pltpu.make_async_remote_copy(src, dst, send, recv, where, MESH)

    def lane_at(d):
        return (lane + d) % lanes

    def x_at(d):
        return (xi + d) % xs

    def bit_of(value, b):
        return (value // (1 << b)) % 2

    def partner(b):
        return lane + (1 - 2 * bit_of(lane, b)) * (1 << b)

    def mate(e):
        return lane + sum((e >> b) % 2 * (1 - 2 * bit_of(lane, b)) * (1 << b) for b in range(bits))

    def mated(i):
        total_of = 0
        for b in range(bits):
            total_of = total_of + (bit_of(lane, b) + bit_of(i, b)) % 2 * (1 << b)
        return total_of

    def low_bit(e):
        return (e & -e).bit_length() - 1

    other_side = 1 - side
    other_core = 1 - core

    barrier = pltpu.get_barrier_semaphore()
    for d in range(1, lanes):
        pl.semaphore_signal(barrier, inc=1, device_id=at_sp(lane_at(d), side), device_id_type=MESH)
    pl.semaphore_signal(barrier, inc=1, device_id=at_sp(lane, other_side), device_id_type=MESH)
    for d in range(1, nt):
        pl.semaphore_signal(
            barrier, inc=1, device_id={"sp": sp, "tp": (tp + d) % nt}, device_id_type=MESH
        )

    def rank(lane_to):
        return lane_to + core * (lanes - 1 - 2 * lane_to)

    def sized(lane_to, action):
        if last == wide:
            action(width)
            return
        few = rank(lane_to) // (lanes - 1)

        @pl.when(few == 1)
        def _():
            action(last * LANE)

        @pl.when(few == 0)
        def _():
            action(width)

    def weight_block(m, lane_to, size):
        at = pl.ds(pl.multiple_of(rank(lane_to) * width, LANE), size)
        if m == 0:
            return gate.at[:, at]
        if m == 1:
            return up.at[:, at]
        return down.at[at, :]

    def landing(m, slot, size):
        if m == 0:
            return gw.at[slot, :, 0:size]
        if m == 1:
            return uw.at[slot, :, 0:size]
        return dw.at[slot, 0:size, :]

    def w_local(m, size):
        return pltpu.make_async_copy(weight_block(m, lane, size), landing(m, sp, size), w_own.at[m])

    ow_copy = pltpu.make_async_copy(out_weight, ow, misc.at[0])
    tok_copy = pltpu.make_async_copy(
        tokens.at[pl.ds(pl.multiple_of(tp * chunk, chunk), chunk)], tok, misc.at[1]
    )
    kv_vals = kv.shape[1] - head_dim
    small = [
        pltpu.make_async_copy(k_in, k_raw, misc.at[2]),
        pltpu.make_async_copy(doc_in, doc_ref, misc.at[3]),
        pltpu.make_async_copy(k_gain_in, k_gain_ref, misc.at[4]),
        pltpu.make_async_copy(v_in, kv.at[sp, kv_vals:, :], misc.at[5]),
        pltpu.make_async_copy(q_in, q_raw, misc.at[6]),
        pltpu.make_async_copy(q_gain_in, q_gain_ref, misc.at[7]),
        pltpu.make_async_copy(norm_gain_in, norm_gain, misc.at[8]),
    ]
    for copy in small:
        copy.start()
    for m in range(3):
        sized(lane, lambda size, m=m: w_local(m, size).start())
    ow_copy.start()
    tok_copy.start()

    for copy in small[:4]:
        copy.wait()
    k_full = turned(k_raw[...].astype(jnp.float32), upright_row(k_gain_ref[...]), table)
    kv[sp, 0:head_dim, :] = k_full.astype(jnp.bfloat16)
    q_doc = doc_ref[...].astype(jnp.float32)
    kv[sp, kv_docs:kv_vals, :] = jnp.broadcast_to(q_doc, (kv_vals - kv_docs, rows)).astype(jnp.bfloat16)

    pl.semaphore_wait(barrier, lanes - 1 + 1 + nt - 1)

    def kv_z(e, lane_of):
        slot = lane_of * SIDES + side
        return remote(kv.at[slot], kv.at[slot], kv_zs.at[e], kv_r.at[slot], at_sp(mate(e), side))

    def kv_y(lane_of, side_of):
        slot = lane_of * SIDES + side_of
        return remote(
            kv.at[slot], kv.at[slot], kv_ys.at[lane_of], kv_r.at[slot], at_sp(lane, other_side)
        )

    for e in range(1, lanes):
        kv_z(e, lane).start()
    kv_y(lane, side).start()

    span = ow.shape[1] // PIECES
    gathered = GATHERED * span
    ow_here = out_weight.at[:, 0:gathered]

    def ow_x(d, slot):
        return remote(ow_here, ow_all.at[slot], ow_xs.at[d], ow_r.at[slot], at_tp(x_at(d), core))

    def ow_core(x_of, core_of):
        slot = x_of * 2 + core_of
        return remote(
            ow_all.at[slot], ow_all.at[slot], ow_cs.at[x_of], ow_r.at[slot], at_tp(xi, other_core)
        )

    for d in range(1, xs):
        ow_x(d, tp).start()
    remote(ow_here, ow_all.at[tp], ow_cs.at[xi], ow_r.at[tp], at_tp(xi, other_core)).start()

    def w_z(m, e, slot, lane_to, size):
        return remote(
            weight_block(m, lane_to, size),
            landing(m, slot, size),
            w_zs.at[m, e],
            w_r.at[m, slot],
            at_sp(mate(e), side),
        )

    def w_y(m, lane_of, side_of, size):
        slot = lane_of * SIDES + side_of
        return remote(
            landing(m, slot, size),
            landing(m, slot, size),
            w_ys.at[m, lane_of],
            w_r.at[m, slot],
            at_sp(lane, other_side),
        )

    def send_weight(m, e):
        lane_to = mate(e)
        sized(lane_to, lambda size: w_z(m, e, sp, lane_to, size).start())

    def share_weight(m):
        def own(size):
            w_local(m, size).wait()
            w_y(m, lane, side, size).start()

        sized(lane, own)

    def forward_weight(m, lane_of):
        sized(lane, lambda size: w_z(m, 1, lane_of * SIDES + side, lane, size).wait_recv())
        sized(lane, lambda size: w_y(m, lane_of, side, size).start())

    def w_shared(m, lane_of):
        sized(lane, lambda size: w_y(m, lane_of, other_side, size).wait_recv())

    for e in range(1, lanes):
        send_weight(0, e)
    share_weight(0)

    scale = head_dim ** (-0.5)
    for copy in small[4:]:
        copy.wait()
    standing_q = flipped(q_raw[...])
    q_gain = upright_row(q_gain_ref[...])
    for h in range(heads):
        at = slice(h * head_dim, (h + 1) * head_dim)
        query = turned(standing_q[at, :], q_gain, table)
        q_ref[at, :] = (query.astype(jnp.bfloat16).astype(jnp.float32) * scale).astype(jnp.bfloat16)
    top[...] = jnp.full(top.shape, NEG, jnp.float32)
    total[...] = jnp.zeros(total.shape, jnp.float32)
    acc[...] = jnp.zeros(acc.shape, jnp.float32)

    def absorb(slot):
        upright = lax.dot_general(
            identity(rows),
            kv[slot, 0:kv_vals, :],
            (((1,), (1,)), ((), ())),
            preferred_element_type=jnp.float32,
        )
        key = upright[:, 0:head_dim].astype(jnp.bfloat16)
        same = upright[:, head_dim : head_dim + 1] == q_doc
        value = kv[slot, kv_vals:, :]
        for h in range(heads):
            at = slice(h * head_dim, (h + 1) * head_dim)
            scores = jnp.dot(key, q_ref[at, :], preferred_element_type=jnp.float32)
            scores = jnp.where(same, scores, NEG)
            before = top[h]
            now = jnp.maximum(before, jnp.max(scores, axis=0, keepdims=True))
            weights = jnp.exp(scores - now)
            shrink = jnp.exp(before - now)
            top[h] = now
            total[h] = total[h] * shrink + jnp.sum(weights, axis=0, keepdims=True)
            acc[at, :] = acc[at, :] * shrink + jnp.dot(
                value, weights.astype(jnp.bfloat16), preferred_element_type=jnp.float32
            )

    @pl.loop(0, SIDES)
    def _(k):
        side_of = (side + k) % SIDES

        @pl.when(k > 0)
        def _():
            kv_y(lane, other_side).wait_recv()

        absorb(lane * SIDES + side_of)

    @pl.loop(0, SIDES * (lanes - 1))
    def _(k):
        lane_of = mated(k % (lanes - 1) + 1)
        side_of = (side + k // (lanes - 1)) % SIDES
        slot = lane_of * SIDES + side_of

        @pl.when(k < lanes - 1)
        def _():
            kv_z(1, lane_of).wait_recv()
            kv_y(lane_of, side).start()

        @pl.when(k >= lanes - 1)
        def _():
            kv_y(lane_of, other_side).wait_recv()

        absorb(slot)

    send_weight(1, 1)
    share_weight(1)
    pieces = []
    for h in range(heads):
        at = slice(h * head_dim, (h + 1) * head_dim)
        pieces.append((acc[at, :] / total[h]).astype(jnp.bfloat16))
    attended = flipped(jnp.concatenate(pieces, axis=0)).astype(jnp.bfloat16)

    def att_copy(d, peer, slot):
        return remote(
            att_out.at[peer], att.at[slot], att_s.at[d], att_r.at[slot], {"sp": sp, "tp": peer}
        )

    for i in range(nt):
        att_out[i] = attended[i * chunk : (i + 1) * chunk]
    for d in range(1, nt):
        att_copy(d, (tp + d) % nt, tp).start()

    def part_core(p):
        return remote(part.at[p, other_core], part_in.at[p], pc_s.at[p], pc_r.at[p], at_tp(xi, other_core))

    def part_x(p, d):
        return remote(px_out.at[p, d], px_in.at[p, d], px_s.at[p, d], px_r.at[p, d], at_tp(x_at(d), core))

    ow_copy.wait()
    for p in range(GATHERED, PIECES):
        product = jnp.dot(
            attended, ow[:, p * span : (p + 1) * span], preferred_element_type=jnp.float32
        ).astype(jnp.bfloat16)
        for x_of in range(xs):
            for core_of in range(2):
                start = (x_of * 2 + core_of) * chunk
                part[p, core_of, x_of] = product[start : start + chunk]
        part_core(p).start()
    for d in range(1, xs):
        x_of = x_at(xs - d)
        ow_x(d, x_of * 2 + core).wait_recv()
        ow_core(x_of, core).start()
    tok_copy.wait()
    early = slice(0, gathered)

    def project(rows_of, weight):
        product = jnp.dot(rows_of, weight, preferred_element_type=jnp.float32)
        return product.astype(jnp.bfloat16).astype(jnp.float32)

    resid[:, early] = tok[:, early].astype(jnp.float32) + project(att_out[tp], ow[:, early])
    for p in range(GATHERED, PIECES):
        at = slice(p * span, (p + 1) * span)
        part_core(p).wait_recv()
        for d in range(1, xs):
            x_to = x_at(d)
            px_out[p, d] = (
                part[p, core, x_to].astype(jnp.float32) + part_in[p, x_to].astype(jnp.float32)
            ).astype(jnp.bfloat16)
            part_x(p, d).start()
        resid[:, at] = (
            tok[:, at].astype(jnp.float32)
            + part[p, core, xi].astype(jnp.float32)
            + part_in[p, xi].astype(jnp.float32)
        )

    def add_rows(slot):
        att_copy(1, tp, slot).wait_recv()
        resid[:, early] += project(att[slot], ow_all[slot])

    ow_core(xi, other_core).wait_recv()
    add_rows(xi * 2 + other_core)
    for d in range(1, xs):
        add_rows(x_at(xs - d) * 2 + core)
    for d in range(1, xs):
        ow_core(x_at(xs - d), other_core).wait_recv()
        add_rows(x_at(xs - d) * 2 + other_core)
    for p in range(GATHERED, PIECES):
        at = slice(p * span, (p + 1) * span)
        for d in range(1, xs):
            part_x(p, d).wait_recv()
            resid[:, at] += px_in[p, d].astype(jnp.float32)

    whole = resid[...]
    power = jnp.mean(whole * whole, axis=-1, keepdims=True)
    act[lane, tp] = (whole * lax.rsqrt(power + EPS) * norm_gain[...]).astype(jnp.bfloat16)

    def act_z(b, lane_of):
        return remote(
            act.at[lane_of, tp],
            act.at[lane_of, tp],
            act_zs.at[b, lane_of],
            act_r.at[lane_of, tp],
            at_sp(partner(b), side),
        )

    def act_x(d, lane_of, slot):
        return remote(
            act.at[lane_of, slot],
            act.at[lane_of, slot],
            act_xs.at[d, lane_of],
            act_r.at[lane_of, slot],
            at_tp(x_at(d), core),
        )

    def act_core(lane_of, x_of, core_of):
        slot = x_of * 2 + core_of
        return remote(
            act.at[lane_of, slot],
            act.at[lane_of, slot],
            act_cs.at[lane_of, x_of],
            act_r.at[lane_of, slot],
            at_tp(xi, other_core),
        )

    def act_out(lane_of):
        for d in range(1, xs):
            act_x(d, lane_of, tp).start()
        act_core(lane_of, xi, core).start()

    def act_from_x(lane_of):
        for d in range(1, xs):
            x_of = x_at(xs - d)
            act_x(d, lane_of, x_of * 2 + core).wait_recv()
            act_core(lane_of, x_of, core).start()

    def act_arrived(e):
        step = low_bit(e)
        act_z(step, mate(e)).wait_recv()
        for lower in reversed(range(step)):
            act_z(lower, mate(e)).start()
        act_out(mate(e))

    for b in reversed(range(bits)):
        act_z(b, lane).start()
    act_out(lane)
    for e in range(2, lanes - 1):
        send_weight(1, e)
    for e in range(1, lanes):
        forward_weight(0, mate(e))
    act_from_x(lane)
    for e in range(1, lanes - 1):
        act_arrived(e)
    send_weight(1, lanes - 1)
    share_weight(2)
    forward_weight(1, mate(1))

    few_here = rank(lane) // (lanes - 1)
    unit = lax.broadcasted_iota(jnp.int32, (nt * chunk, width), 1)
    mine = unit < (wide - few_here * (wide - last)) * LANE
    if last < wide:

        @pl.when(few_here == 1)
        def _():
            dw[:, last * LANE :, :] = jnp.zeros((n, width - last * LANE, dw.shape[2]), dw.dtype)

    def depth(ref):
        return ref[...].reshape(ref.shape[0] * ref.shape[1], ref.shape[2])

    for d in range(lanes):
        w_shared(0, lane_at(d))

    @pl.loop(0, lanes)
    def _(i):
        lane_of = mated(i)
        for e in range(1, lanes):

            @pl.when(i == e)
            def _(e=e):
                if e == lanes - 2:
                    act_arrived(e + 1)
                    for f in range(1, lanes):
                        send_weight(2, f)
                if e > 1:
                    forward_weight(1, mate(e))
                act_from_x(mate(e))

        for x_of in range(xs):
            act_core(lane_of, x_of, other_core).wait_recv()
        inputs = act[lane_of].reshape(nt * chunk, act.shape[-1])
        gated[lane_of] = jnp.dot(inputs, depth(gw), preferred_element_type=jnp.float32)

    for d in range(lanes):
        w_shared(1, lane_at(d))

    @pl.loop(0, lanes)
    def _(lane_of):
        inputs = act[lane_of].reshape(nt * chunk, act.shape[-1])
        lifted = jnp.dot(inputs, depth(uw), preferred_element_type=jnp.float32)
        gates = gated[lane_of]
        hidden = jnp.where(mine, gates * lax.logistic(gates) * lifted, 0.0).astype(jnp.bfloat16)
        for x_of in range(xs):
            for core_of in range(2):
                start = (x_of * 2 + core_of) * chunk
                hid[core_of, x_of, lane_of] = hidden[start : start + chunk]

    for e in range(1, lanes // 2):
        forward_weight(2, mate(e))

    cols = dw.shape[2]
    share = xs * lanes * chunk
    starts = [lanes - (lanes >> b) for b in range(bits)]

    def rs_core(s):
        return remote(core_out.at[s], core_in.at[s], rs_cs.at[s], rs_cr.at[s], at_tp(xi, other_core))

    def rs_x(s, d):
        return remote(x_out.at[s, d], x_in.at[s, d], rs_xs.at[s, d], rs_xr.at[s, d], at_tp(x_at(d), core))

    def rs_z(s, b):
        piece = pl.ds(starts[b], lanes >> (b + 1))
        return remote(
            z_out.at[s, piece], z_in.at[s, piece], rs_zs.at[s, b], rs_zr.at[s, b], at_sp(partner(b), side)
        )

    def columns(s):
        return pl.ds(pl.multiple_of(s * cols, cols), cols)

    def ag_x(s, d, slot):
        piece = out.at[slot, :, columns(s)]
        return remote(piece, piece, ag_xs.at[s, d], ag_r.at[s, slot], at_tp(x_at(d), core))

    def ag_core(s, x_of, core_of):
        slot = x_of * 2 + core_of
        piece = out.at[slot, :, columns(s)]
        return remote(piece, piece, ag_cs.at[s, x_of], ag_r.at[s, slot], at_tp(xi, other_core))

    half = lanes // 2
    upper = lane // half

    def half_slot(k):
        turn = k % lanes
        lane_of = (upper + k // lanes) % 2 * half + turn % half
        return lane_of * SIDES + (side + turn // half) % SIDES

    def slot_of(i):
        turn = i // 2
        lane_of = i % 2 * half + turn % half
        return lane_of * SIDES + (side + turn // half) % SIDES

    def multiply(k):
        s = half_slot(k)

        @pl.when((k >= lanes - 1) & (k < lanes - 1 + half))
        def _():
            forward_weight(2, (upper + 1) % 2 * half + k - (lanes - 1))

        @pl.when(k % lanes >= half)
        def _():
            w_shared(2, s // SIDES)

        away = hid[other_core].reshape(share, width)
        core_out[s] = (
            jnp.dot(away, dw[s], preferred_element_type=jnp.float32)
            .astype(jnp.bfloat16)
            .reshape(xs, lanes, chunk, cols)
        )
        rs_core(s).start()
        near = hid[core].reshape(share, width)
        keep[s] = jnp.dot(near, dw[s], preferred_element_type=jnp.float32).reshape(xs, lanes, chunk, cols)

    def reduce_core(k):
        s = half_slot(k)
        rs_core(s).wait_recv()
        for d in range(1, xs):
            x_to = x_at(d)
            x_out[s, d] = (keep[s, x_to] + core_in[s, x_to].astype(jnp.float32)).astype(jnp.bfloat16)
            rs_x(s, d).start()
        x_keep[s] = keep[s, xi] + core_in[s, xi].astype(jnp.float32)

    def reduce_lanes(b, k):
        s = half_slot(k) if b < bits - 1 else slot_of(k)
        if b == 0:
            for d in range(1, xs):
                rs_x(s, d).wait_recv()
        else:
            rs_z(s, b - 1).wait_recv()

        def summed(h):
            if b == 0:
                value = x_keep[s, h]
                for d in range(1, xs):
                    value = value + x_in[s, d, h].astype(jnp.float32)
                return value
            return z_keep[b - 1, s, h] + z_in[s, starts[b - 1] + h].astype(jnp.float32)

        if b == bits:
            out[tp, :, columns(s)] = (resid[:, columns(s)] + summed(0)).astype(jnp.bfloat16)
            for d in range(1, xs):
                ag_x(s, d, tp).start()
            ag_core(s, xi, core).start()
            return
        mine_here = bit_of(lane, b)
        count = lanes >> (b + 1)
        for h in range(count):
            z_out[s, starts[b] + h] = summed(1 - mine_here + 2 * h).astype(jnp.bfloat16)
        rs_z(s, b).start()
        for h in range(count):
            z_keep[b, s, h] = summed(mine_here + 2 * h)

    def spread(k):
        s = slot_of(k)
        for d in range(1, xs):
            x_of = x_at(xs - d)
            ag_x(s, d, x_of * 2 + core).wait_recv()
            ag_core(s, x_of, core).start()

    def by_two(b):
        def both(j):
            for i in range(2):
                reduce_lanes(b, 2 * j + i)

        return both

    lag = 4
    stages = [(0, n, multiply), (1, n, reduce_core)]
    for b in range(bits - 1):
        stages.append((lag, n, functools.partial(reduce_lanes, b)))
        lag += 2
    lag += lanes - 1 if bits > 1 else lanes
    for b in (bits - 1, bits):
        stages.append((lag, n // 2, by_two(b)))
        lag += 2

    @pl.loop(0, stages[-1][0] + n // 2)
    def _(k):
        for lag, count, action in stages:

            @pl.when((k >= lag) & (k < count + lag))
            def _(lag=lag, action=action):
                action(k - lag)

    pl.loop(0, n)(spread)

    @pl.loop(0, n)
    def _(s):
        for x_of in range(xs):
            ag_core(s, x_of, other_core).wait_recv()
            ag_core(s, x_of, core).wait_send()
        for d in range(1, xs):
            ag_x(s, d, tp).wait_send()
            rs_x(s, d).wait_send()
        rs_core(s).wait_send()
        for b in range(bits):
            rs_z(s, b).wait_send()

    for d in range(1, lanes):
        kv_z(d, lane).wait_send()
        for m in range(3):
            lane_to = mate(d)
            sized(lane_to, lambda size, m=m, d=d, lane_to=lane_to: w_z(m, d, sp, lane_to, size).wait_send())
    for lane_of in range(lanes):
        kv_y(lane_of, side).wait_send()
        for m in range(3):
            sized(lane, lambda size, m=m, lane_of=lane_of: w_y(m, lane_of, side, size).wait_send())
        for d in range(1, xs):
            act_x(d, lane_of, tp).wait_send()
        for x_of in range(xs):
            act_core(lane_of, x_of, core).wait_send()
    for b in range(bits):
        for h in range(lanes >> (b + 1)):
            lane_of = lane % (1 << (b + 1)) + h * (1 << (b + 1))
            act_z(b, lane_of).wait_send()
    for d in range(1, xs):
        ow_x(d, tp).wait_send()
    for x_of in range(xs):
        ow_core(x_of, core).wait_send()
    for d in range(1, nt):
        att_copy(d, (tp + d) % nt, tp).wait_send()
    for p in range(GATHERED, PIECES):
        part_core(p).wait_send()
        for d in range(1, xs):
            part_x(p, d).wait_send()


VMEM_LIMIT = 60 * 1024 * 1024


def fused_plan(n, nt, rows, width, head_dim, heads, units):
    if n % SIDES or n < 2 * SIDES or nt % 2 or nt < 4 or rows % nt or units % LANE:
        return None
    lanes, xs, chunk, blocks = n // SIDES, nt // 2, rows // nt, units // LANE
    wide = -(-blocks // lanes)
    cols = width // n
    if chunk % 16 or rows % LANE or width % (n * LANE) or width % (PIECES * LANE) or head_dim % 64:
        return None
    if lanes & (lanes - 1) or (lanes - 1) * wide >= blocks:
        return None
    wu = wide * LANE
    bits = lanes.bit_length() - 1
    span = width // PIECES
    bf, f32 = jnp.bfloat16, jnp.float32
    shapes = [
        ((rows, heads * head_dim), bf),
        ((head_dim, rows), bf),
        ((1, rows), jnp.int32),
        ((1, head_dim), f32),
        ((1, head_dim), f32),
        ((1, width), f32),
        ((n, 2 * head_dim + 16, rows), bf),
        ((heads * head_dim, rows), bf),
        ((heads, 1, rows), f32),
        ((heads, 1, rows), f32),
        ((heads * head_dim, rows), f32),
        ((PIECES, 2, xs, chunk, span), bf),
        ((PIECES, xs, chunk, span), bf),
        ((PIECES, xs, chunk, span), bf),
        ((PIECES, xs, chunk, span), bf),
        ((heads * head_dim, width), bf),
        ((nt, heads * head_dim, GATHERED * span), bf),
        ((nt, chunk, heads * head_dim), bf),
        ((nt, chunk, heads * head_dim), bf),
        ((chunk, width), bf),
        ((chunk, width), f32),
        ((lanes, nt, chunk, width), bf),
        ((n, cols, wu), bf),
        ((n, cols, wu), bf),
        ((n, wu, cols), bf),
        ((lanes, rows, wu), f32),
        ((2, xs, lanes, chunk, wu), bf),
        ((n, xs, lanes, chunk, cols), f32),
        ((n, xs, lanes, chunk, cols), bf),
        ((n, xs, lanes, chunk, cols), bf),
        ((n, lanes, chunk, cols), f32),
        ((n, xs, lanes, chunk, cols), bf),
        ((n, xs, lanes, chunk, cols), bf),
        ((bits, n, lanes // 2, chunk, cols), f32),
        ((n, lanes - 1, chunk, cols), bf),
        ((n, lanes - 1, chunk, cols), bf),
    ]
    size = 0
    for shape, kind in shapes:
        count = 1
        for extent in shape:
            count *= extent
        size += count * jnp.dtype(kind).itemsize
    if size > VMEM_LIMIT * 3 // 4:
        return None
    sems = [(lanes,), (lanes,), (n,), (3,), (3, lanes), (3, lanes), (3, n), (9,)]
    sems += [(PIECES,), (PIECES,), (PIECES, xs), (PIECES, xs), (xs,), (xs,), (nt,), (nt,), (nt,)]
    sems += [(bits, lanes), (xs, lanes), (lanes, xs), (lanes, nt)]
    sems += [(n,), (n,), (n, xs), (n, xs), (n, bits), (n, bits), (n, xs), (n, xs), (n, nt)]
    return wide, [pltpu.VMEM(*s) for s in shapes] + [pltpu.SemaphoreType.DMA(s) for s in sems]


def fused_layer(
    n, nt, plan, tokens_in, queries, keys, values, doc_ids, query_gain, key_norm_scale,
    out_weight, norm_gain, gate_weight, up_weight, down_weight,
):
    wide, scratch = plan
    rows, width = tokens_in.shape
    head_dim = query_gain.shape[0]
    places = lax.axis_index("sp") * rows + jnp.arange(rows, dtype=jnp.int32)
    half = head_dim // 2
    freqs = THETA ** (-2.0 * jnp.arange(half // 2, dtype=jnp.float32) / half)
    angles = [
        freqs[:, None] * spot.astype(jnp.float32)[None, :] for spot in (places // GRID, places % GRID)
    ]
    tables = [f(a) for a in angles for f in (jnp.cos, jnp.sin)]
    hbm = pl.BlockSpec(memory_space=pl.ANY)
    out = pl.pallas_call(
        functools.partial(fused_kernel, n, nt, wide),
        out_shape=jax.ShapeDtypeStruct((nt, rows // nt, width), jnp.bfloat16),
        in_specs=[hbm] * 12 + [VM] * 4,
        out_specs=VM,
        scratch_shapes=scratch,
        compiler_params=pltpu.CompilerParams(
            collective_id=3, has_side_effects=True, vmem_limit_bytes=VMEM_LIMIT
        ),
        name="fused_layer",
    )(
        queries, keys.T, values.T, doc_ids.reshape(1, rows), query_gain.reshape(1, head_dim),
        key_norm_scale.reshape(1, head_dim), norm_gain.reshape(1, width), tokens_in, out_weight,
        gate_weight, up_weight, down_weight, *tables,
    )
    return out.reshape(rows, width)


def per_device(
    n,
    nt,
    tokens_in,
    queries,
    keys,
    values,
    doc_ids,
    query_gain,
    key_norm_scale,
    out_weight,
    norm_gain,
    gate_weight,
    up_weight,
    down_weight,
):
    tok_rows = tokens_in.shape[0]
    head_dim = query_gain.shape[0]
    local_heads = queries.shape[1] // head_dim
    plan = None
    if keys.shape[1] == head_dim:
        plan = fused_plan(
            n, nt, tok_rows, tokens_in.shape[1], head_dim, local_heads, gate_weight.shape[1]
        )
    if plan is not None:
        return fused_layer(
            n, nt, plan, tokens_in, queries, keys, values, doc_ids, query_gain, key_norm_scale,
            out_weight, norm_gain, gate_weight, up_weight, down_weight,
        )
    places = lax.axis_index("sp") * tok_rows + jnp.arange(tok_rows, dtype=jnp.int32)
    lattice_row = (places // GRID).astype(jnp.float32)
    lattice_column = (places % GRID).astype(jnp.float32)
    q_local = normalized_rotated(queries, query_gain, local_heads, lattice_row, lattice_column)
    q_rows = q_local.transpose(1, 0, 2).reshape(local_heads * tok_rows, head_dim)
    lanes = [[2 * j + side for j in range(n // 2)] for side in range(2)]
    gate_up_all = lax.all_gather(
        pair_share(n, [gate_weight, up_weight], 1, 0), "sp", axis_index_groups=lanes, axis=0, tiled=True
    )
    down_all = lax.all_gather(
        pair_share(n, [down_weight], 0, 1), "sp", axis_index_groups=lanes, axis=1, tiled=True
    )
    turned = normalized_rotated(keys, key_norm_scale, 1, lattice_row, lattice_column)
    packed = jnp.concatenate([turned.reshape(tok_rows, head_dim), values], axis=1)
    kv_all, doc_all = gather_sp(n, packed, doc_ids.reshape(1, tok_rows))
    row_docs = jnp.tile(doc_ids, local_heads)
    first_doc = doc_ids[0]
    last_doc = doc_ids[-1]
    scale = head_dim ** (-0.5)
    total_rows = local_heads * tok_rows

    def absorb_block(state, key_block, value_block, doc_block):

        def absorb(current):
            running_max, running_sum, running_acc = current
            scores = (
                jnp.einsum("qd,kd->qk", q_rows, key_block, preferred_element_type=jnp.float32)
                * scale
            )
            same = row_docs[:, None] == doc_block[None, :]
            scores = jnp.where(same, scores, NEG)
            new_max = jnp.maximum(running_max, jnp.max(scores, axis=1))
            weights = jnp.where(same, jnp.exp(scores - new_max[:, None]), 0.0)
            shrink = jnp.exp(running_max - new_max)
            new_sum = running_sum * shrink + jnp.sum(weights, axis=1)
            new_acc = running_acc * shrink[:, None] + jnp.dot(
                weights.astype(jnp.bfloat16), value_block, preferred_element_type=jnp.float32
            )
            return (new_max, new_sum, new_acc)

        touches = (doc_block[0] <= last_doc) & (doc_block[-1] >= first_doc)
        return lax.cond(touches, absorb, lambda current: current, state)

    initial = (
        jnp.full((total_rows,), NEG, jnp.float32),
        jnp.zeros((total_rows,), jnp.float32),
        jnp.zeros((total_rows, head_dim), jnp.float32),
    )
    carry = initial
    shards = n
    joined = 1
    while joined * 2 <= shards and shards % (joined * 2) == 0 and (joined * 2 * tok_rows <= 1024):
        joined = joined * 2
    blocks = shards // joined
    span_rows = joined * tok_rows
    key_blocks = kv_all[..., :head_dim].reshape(blocks, span_rows, head_dim)
    value_blocks = kv_all[..., head_dim:].reshape(blocks, span_rows, head_dim)
    doc_blocks = doc_all.reshape(blocks, span_rows)

    def visit(state, inputs):
        key_block, value_block, doc_block = inputs
        return (absorb_block(state, key_block, value_block, doc_block), None)

    carry, unused = lax.scan(visit, carry, (key_blocks, value_blocks, doc_blocks))
    attended = (carry[2] / carry[1][:, None]).astype(jnp.bfloat16)
    attended = (
        attended.reshape(local_heads, tok_rows, head_dim)
        .transpose(1, 0, 2)
        .reshape(tok_rows, local_heads * head_dim)
    )
    partial_value = jnp.dot(attended, out_weight, preferred_element_type=jnp.float32)
    normed, resid = mid_stage(nt, partial_value.astype(jnp.bfloat16), tokens_in, norm_gain)
    normed = normed.reshape(2 * tok_rows, -1)
    both = jnp.dot(normed, gate_up_all, preferred_element_type=jnp.float32)
    units = both.shape[1] // 2
    hidden = (jax.nn.silu(both[:, :units]) * both[:, units:]).astype(jnp.bfloat16)
    fed_part = jnp.dot(hidden, down_all, preferred_element_type=jnp.float32)
    out = last_stage(nt, fed_part.astype(jnp.bfloat16), resid)
    return out.reshape(tok_rows, -1)


def solution(mesh):
    return jax.shard_map(
        functools.partial(per_device, mesh.shape["sp"], mesh.shape["tp"]),
        mesh=mesh,
        in_specs=(
            P("sp", None),
            P("sp", "tp"),
            P("sp", "tp"),
            P("sp", "tp"),
            P("sp"),
            P(),
            P(),
            P("tp", None),
            P(),
            P("sp", "tp"),
            P("sp", "tp"),
            P("tp", "sp"),
        ),
        out_specs=P("sp", None),
        check_vma=False,
    )
```
